256 devices in a mesh: sp: 64 (over z, y, core), tp: 4 (over x).
Axes of the slice: x: 4, y: 4, z: 8, core: 2. Of those that a mesh axis runs over, the one named last changes fastest.
Arguments:
- stream_in: bfloat16 [49152, 2048], P(('sp', 'tp')), may hold values from -6 to 6
- query_wide: bfloat16 [49152, 512], P('sp', 'tp'), may hold values from -6 to 6
- key_wide: bfloat16 [49152, 512], P('sp', 'tp'), may hold values from -6 to 6
- value_wide: bfloat16 [49152, 512], P('sp', 'tp'), may hold values from -6 to 6
- gate_wide: bfloat16 [49152, 512], P('sp', 'tp'), may hold values from -6 to 6
- decay_wide: float32 [4, 49152], P('tp', 'sp'), may hold values from -2.3 to 0, as said below
- query_narrow: bfloat16 [49152, 512], P('sp', 'tp'), may hold values from -6 to 6
- key_narrow: bfloat16 [49152, 512], P('sp', 'tp'), may hold values from -6 to 6
- value_narrow: bfloat16 [49152, 512], P('sp', 'tp'), may hold values from -6 to 6
- gate_narrow: bfloat16 [49152, 512], P('sp', 'tp'), may hold values from -6 to 6
- decay_narrow: float32 [8, 49152], P('tp', 'sp'), may hold values from -2.3 to 0, as said below
- output_wide: bfloat16 [512, 2048], P('tp'), may hold values from -0.25 to 0.25
- output_narrow: bfloat16 [512, 2048], P('tp'), may hold values from -0.25 to 0.25
- norm_gain: bfloat16 [2048], replicated, may hold values from 0.099609375 to 1.8984375
- up_weight: bfloat16 [2048, 8192], P('sp', 'tp'), may hold values from -0.125 to 0.125
- down_weight: bfloat16 [8192, 2048], P('tp', 'sp'), may hold values from -0.0625 to 0.0625
Outputs:
- layer_out: bfloat16 [49152, 2048], P(('sp', 'tp'))
The draws below stay inside these ranges and needn't reach their ends.
Inputs may be any that keep to these rules, and one draw needn't show every extreme that they name: `decay_wide`: each entry is the logarithm of one head's retention factor at one position. `decay_narrow`: each entry is the logarithm of one head's retention factor at one position.
All inputs are finite; a program needn't handle non-finite values.
Results may differ from the reference program's by a relative error of at most 0.02.
Values may be sent and summed in bfloat16 or wider, within the bound.
A program may use at most 128 MiB of HBM per device.

```python
import math
import jax
import jax.numpy as jnp
from jax import lax

D = 2048
FF = 8192
HEADS_W = 4
HEADS_N = 8
HDW = 128
HDN = 64
BLOCK = 128
TOK_DEV = 768
RW = 512
RN = 512
TOKEN_POSITIONS = 49152


spike_count = 3


def log_decay_table(key, count_of_heads, slow_share):
    random_subkey_list = jax.random.split(key, 6)
    slow_heads = jax.random.uniform(random_subkey_list[0], (count_of_heads,), jnp.float32) < slow_share
    slow_rate = jax.random.uniform(random_subkey_list[1], (count_of_heads,), jnp.float32, 0.15, 0.4) * math.log(10.0) / TOKEN_POSITIONS
    fast_rate = 1.0 / jax.random.uniform(random_subkey_list[2], (count_of_heads,), jnp.float32, 30.0, 100.0)
    decay_rate = jnp.where(slow_heads, slow_rate, fast_rate)
    stretch = jnp.exp(jax.random.uniform(random_subkey_list[3], (TOKEN_POSITIONS // TOK_DEV,), jnp.float32, -math.log(2.0), math.log(2.0)))
    stretch = jnp.repeat(stretch, TOK_DEV)
    logarithm_base = -decay_rate[:, None] * stretch[None, :]
    spike_locations = jax.random.randint(random_subkey_list[4], (spike_count,), 0, TOKEN_POSITIONS)
    spike_labels = (jnp.arange(TOKEN_POSITIONS)[None, :] == spike_locations[:, None]).astype(jnp.float32)
    spike_removals = jax.random.uniform(random_subkey_list[5], (count_of_heads, spike_count), jnp.float32, math.log(0.5), math.log(0.8))
    return logarithm_base + jnp.dot(spike_removals, spike_labels)


def draw_decay_wide(key, part):
    share = 0.5
    return log_decay_table(jax.random.fold_in(key, 11), HEADS_W, share)


def draw_decay_narrow(key, part):
    share = 0.5
    return log_decay_table(jax.random.fold_in(key, 23), HEADS_N, share)


def steps_of(own_key, extent, shards, least, largest):
    def one(position, blocks):
        draws = jax.random.uniform(jax.random.fold_in(jax.random.fold_in(own_key, 6), position), (blocks,), jnp.float32, least / len(shards), largest / len(shards))
        return jnp.repeat(jnp.exp(draws), extent[position] // blocks).reshape((-1,) + (1,) * (len(extent) - position - 1))

    level = one(*shards[0])
    for cut in shards[1:]:
        level = level * one(*cut)
    return level


def scatter_about(key, extent, scale, most, pieces=(), kind=jnp.bfloat16):
    loudness = steps_of(key, extent, pieces, -0.22, 0.18) if pieces else 1.0
    drawn = jax.random.normal(key, extent, jnp.float32) * scale * loudness
    return jnp.minimum(jnp.maximum(drawn, -most), most).astype(kind)


def setup_inputs(seed: int = 0) -> dict:
    splits = jax.random.split(jax.random.key(seed), 17)
    return {
        "stream_in": scatter_about(splits[0], (TOKEN_POSITIONS, D), 1.0, 6.0, ((0, 256),)),
        "query_wide": scatter_about(splits[1], (TOKEN_POSITIONS, RW), 1.0, 6.0, ((0, 64), (1, 4))),
        "key_wide": scatter_about(splits[2], (TOKEN_POSITIONS, RW), 1.0, 6.0, ((0, 64), (1, 4))),
        "value_wide": scatter_about(splits[3], (TOKEN_POSITIONS, RW), 1.0, 6.0, ((0, 64), (1, 4))),
        "gate_wide": scatter_about(splits[4], (TOKEN_POSITIONS, RW), 1.0, 6.0, ((0, 64), (1, 4))),
        "decay_wide": draw_decay_wide(jax.random.fold_in(splits[16], 71), 0),
        "query_narrow": scatter_about(splits[6], (TOKEN_POSITIONS, RN), 1.0, 6.0, ((0, 64), (1, 4))),
        "key_narrow": scatter_about(splits[7], (TOKEN_POSITIONS, RN), 1.0, 6.0, ((0, 64), (1, 4))),
        "value_narrow": scatter_about(splits[8], (TOKEN_POSITIONS, RN), 1.0, 6.0, ((0, 64), (1, 4))),
        "gate_narrow": scatter_about(splits[9], (TOKEN_POSITIONS, RN), 1.0, 6.0, ((0, 64), (1, 4))),
        "decay_narrow": draw_decay_narrow(jax.random.fold_in(splits[16], 71), 0),
        "output_wide": scatter_about(splits[11], (RW, D), RW ** -0.5, 0.25, ((0, 4),)),
        "output_narrow": scatter_about(splits[12], (RN, D), RN ** -0.5, 0.25, ((0, 4),)),
        "norm_gain": jnp.clip(1.0 + 0.18 * jax.random.normal(splits[13], (D,), jnp.float32), 0.099609375, 1.8984375).astype(jnp.bfloat16),
        "up_weight": scatter_about(splits[14], (D, FF), D ** -0.5, 0.125, ((0, 64), (1, 4))),
        "down_weight": scatter_about(splits[15], (FF, D), FF ** -0.5, 0.0625, ((0, 4), (1, 64))),
    }


head_eps = 1e-05
norm_eps = 1e-06
rope_base = 10000.0

def rotate(values, places):
    half = values.shape[-1] // 2
    inverse = rope_base ** (-jnp.arange(half, dtype=jnp.float32) / half)
    angles = places[:, None] * inverse[None, :]
    cosine = jnp.cos(angles)[:, None, :]
    sine = jnp.sin(angles)[:, None, :]
    front = values[..., :half]
    back = values[..., half:]
    return jnp.concatenate([front * cosine - back * sine, back * cosine + front * sine], axis=-1)

def block_step(carried, inputs):
    query, keys, values, log_rate = inputs
    running = jnp.cumsum(log_rate, axis=0)
    spread = running[:, None, :] - running[None, :, :]
    length = log_rate.shape[0]
    lower = (jnp.arange(length)[:, None] >= jnp.arange(length)[None, :])[:, :, None]
    factor = jnp.where(lower, jnp.exp(jnp.minimum(spread, 0.0)), 0.0)
    scores = jnp.einsum('thd,shd->tsh', query, keys) * factor
    within = jnp.einsum('tsh,she->the', scores, values)
    across = jnp.einsum('thd,hde->the', query, carried) * jnp.exp(running)[:, :, None]
    tail_decay = jnp.exp(running[-1][None, :] - running)
    updated = jnp.exp(running[-1])[:, None, None] * carried + jnp.einsum('shd,she->hde', keys * tail_decay[:, :, None], values)
    return (updated, within + across)

def retain(query, keys, values, log_rate):
    length, count_of_heads, width = query.shape
    blocks = length // BLOCK

    def shaped(array):
        return array.reshape(blocks, BLOCK, count_of_heads, width)
    rates = log_rate.T.reshape(blocks, BLOCK, count_of_heads)
    carried = jnp.zeros((count_of_heads, width, width), jnp.float32)
    final_state, outputs = lax.scan(block_step, carried, (shaped(query), shaped(keys), shaped(values), rates))
    return outputs.reshape(length, count_of_heads, width)

def head_norm(values):
    centre = values - lax.optimization_barrier(jnp.mean(values, axis=-1, keepdims=True))
    spread = lax.optimization_barrier(jnp.mean(centre * centre, axis=-1, keepdims=True))
    return centre * lax.rsqrt(spread + head_eps)

def group(query, keys, values, gate, log_rate, width, places):
    length = query.shape[0]
    count_of_heads = query.shape[1] // width

    def split(array):
        return array.astype(jnp.float32).reshape(length, count_of_heads, width)
    query_rot = rotate(split(query), places)
    keys_rot = rotate(split(keys), places) * width ** (-0.5)
    normed = head_norm(retain(query_rot, keys_rot, split(values), log_rate)).reshape(length, count_of_heads * width)
    return (jax.nn.silu(gate.astype(jnp.float32)) * normed).astype(jnp.bfloat16)

def reference(stream_in, query_wide, key_wide, value_wide, gate_wide, decay_wide, query_narrow, key_narrow, value_narrow, gate_narrow, decay_narrow, output_wide, output_narrow, norm_gain, up_weight, down_weight):
    places = jnp.arange(TOKEN_POSITIONS, dtype=jnp.float32)
    mixed_wide = group(query_wide, key_wide, value_wide, gate_wide, decay_wide, HDW, places)
    mixed_narrow = group(query_narrow, key_narrow, value_narrow, gate_narrow, decay_narrow, HDN, places)
    mixed_sum = jnp.dot(mixed_wide, output_wide, preferred_element_type=jnp.float32) + jnp.dot(mixed_narrow, output_narrow, preferred_element_type=jnp.float32)
    middle = (stream_in.astype(jnp.float32) + mixed_sum).astype(jnp.bfloat16)
    middle_f = middle.astype(jnp.float32)
    normed_rows = (middle_f * lax.rsqrt(lax.optimization_barrier(jnp.mean(middle_f * middle_f, axis=-1, keepdims=True)) + norm_eps) * norm_gain.astype(jnp.float32)).astype(jnp.bfloat16)
    up_sum = jnp.dot(normed_rows, up_weight, preferred_element_type=jnp.float32)
    hidden = jnp.square(jax.nn.relu(up_sum)).astype(jnp.bfloat16)
    down_sum = jnp.dot(hidden, down_weight, preferred_element_type=jnp.float32)
    return (middle_f + down_sum).astype(jnp.bfloat16)
```

```python
import functools

import jax
import jax.numpy as jnp
import numpy as np
from jax import lax
from jax.experimental import pallas as pl
from jax.experimental.pallas import tpu as pltpu
from jax.sharding import Mesh
from jax.sharding import PartitionSpec as P

HDW = 128
HDN = 64
BLOCK = 128
head_eps = 1e-05
norm_eps = 1e-06
rope_base = 10000.0
MESH = pl.DeviceIdType.MESH
F32 = jnp.float32
BF16 = jnp.bfloat16


def rope_tables(steps, stride):
    tables = []
    for width in (HDW, HDN):
        half = width // 2
        inverse = rope_base ** (-np.arange(half, dtype=np.float64) / half)
        lanes = np.tile(inverse, 128 // half)
        angles = (stride * np.arange(steps, dtype=np.float64))[:, None] * lanes[None, :]
        tables += [np.cos(angles), np.sin(angles)]
    return np.stack(tables).astype(np.float32)


def remote(src, dst, send_sem, recv_sem, device):
    return pltpu.make_async_remote_copy(
        src_ref=src, dst_ref=dst, send_sem=send_sem, recv_sem=recv_sem, device_id=device, device_id_type=MESH
    )


def turn(cos_a, sin_a, cos_b, sin_b):
    return cos_a * cos_b - sin_a * sin_b, sin_a * cos_b + cos_a * sin_b


def dot(a, b):
    return jnp.dot(a, b, preferred_element_type=F32)


def dot_t(a, b):
    return lax.dot_general(a, b, (((1,), (1,)), ((), ())), preferred_element_type=F32)


def tdot(a, b):
    return lax.dot_general(a, b, (((0,), (0,)), ((), ())), preferred_element_type=F32)


def kernel(
    sizes,
    stream, qw, kw, vw, gw, dw, qn, kn, vn, gn, dn, gain, tt, tb, ts, wo, up, down,
    out,
    stream_all, qe_w, qe_n, o_w, o_n, decays, msg, in1, pre1, tot2, in2, msg3, in3,
    mixed, middle, normed, hidden, send2, send1, sendm, own, relay_l, relay_r, got_l, got_r,
    st_s, st_r, s1_s, s1_r, s2_s, s2_r, s3_s, s3_r, mx_s, mx_r, rs_s, rs_r,
):
    nz, ny, nc, nx = sizes
    z, y, c, x = (lax.axis_index(a) for a in ("z", "y", "c", "x"))
    xr, xl, xo = lax.rem(x + 1, nx), lax.rem(x + nx - 1, nx), lax.rem(x + 2, nx)
    plane = ny * nc
    me = y * nc + c
    sp = z * plane + me
    tok = qw.shape[0]
    blocks = tok // BLOCK
    rows = stream.shape[0]
    half_rows = rows // 2
    right, left = {"x": xr}, {"x": xl}

    def at_plane(j):
        return {"y": j // nc, "c": lax.rem(j, nc)}

    barrier = pltpu.get_barrier_semaphore()
    peers = [right, left]
    peers += [at_plane(lax.rem(me + d, plane)) for d in range(1, plane)]
    peers += [{"z": lax.rem(z + d, nz)} for d in range(1, nz)]
    for peer in peers:
        pl.semaphore_signal(barrier, inc=1, device_id=peer, device_id_type=MESH)
    pl.semaphore_wait(barrier, len(peers))

    to_r = remote(stream, stream_all.at[x], st_s.at[0], st_r.at[0], right)
    to_l = remote(stream, stream_all.at[x], st_s.at[1], st_r.at[1], left)
    to_r.start()
    to_l.start()
    stream_all[pl.ds(x, 1)] = stream[...][None]

    lane = lax.broadcasted_iota(jnp.int32, (1, 128), 1)
    low = lane < HDN
    base = []
    for g in (0, 2):
        row = [ts[g + i, pl.ds(sp, 1), :] for i in (0, 1)]
        base.append(turn(row[0], row[1], tb[g], tb[g + 1]))
    sign_w = jnp.where(lane < HDW // 2, -1.0, 1.0)
    front_n = lax.rem(lane, HDN) < HDN // 2
    sign_n = jnp.where(front_n, -1.0, 1.0)

    decays[...] = jnp.zeros_like(decays)
    for b in range(blocks):
        cut = pl.ds(b * BLOCK, BLOCK)
        decays[pl.ds(3 * b, 1), :] = dw[:, cut]
        decays[pl.ds(3 * b + 1, 2), :] = dn[:, cut]
    running = decays[0:32, :]
    shift = 1
    while shift < BLOCK:
        running = running + jnp.where(lane >= shift, pltpu.roll(running, shift, 1), 0.0)
        shift *= 2
    decays[0:32, :] = running
    columns = jnp.transpose(decays[...])

    at_t = lax.broadcasted_iota(jnp.int32, (BLOCK, BLOCK), 0)
    at_s = lax.broadcasted_iota(jnp.int32, (BLOCK, BLOCK), 1)
    lower = at_t >= at_s
    same_head = (at_t < HDN) == (at_s < HDN)

    def spread(r):
        steps = jnp.minimum(columns[:, r : r + 1] - decays[pl.ds(r, 1), :], 0.0)
        return jnp.where(lower, jnp.exp(steps), 0.0)

    state_w = jnp.zeros((128, 128), F32)
    state_n = jnp.zeros((128, 128), F32)
    gone = [jnp.zeros((1, 1), F32)] * 3
    for b in range(blocks):
        cut = pl.ds(b * BLOCK, BLOCK)
        r = 3 * b
        now = [columns[:, r + h : r + h + 1] for h in range(3)]
        last = [columns[BLOCK - 1 : BLOCK, r + h : r + h + 1] for h in range(3)]
        cos, sin = turn(base[0][0][b : b + 1], base[0][1][b : b + 1], tt[0], tt[1])
        sin = sin * sign_w
        q = qw[cut, :].astype(F32)
        k = kw[cut, :].astype(F32)
        v = vw[cut, :]
        q = q * cos + pltpu.roll(q, HDW // 2, 1) * sin
        k = (k * cos + pltpu.roll(k, HDW // 2, 1) * sin) * HDW**-0.5
        scores = dot_t(q.astype(BF16), k.astype(BF16)) * spread(r)
        out_b = dot(scores.astype(BF16), v)
        if b:
            out_b += dot((q * jnp.exp(now[0])).astype(BF16), state_w.astype(BF16))
        o_w[cut, :] = out_b
        qe_w[cut, :] = (q * jnp.exp(now[0] + gone[0])).astype(BF16)
        tail = k * jnp.exp(last[0] - now[0])
        state_w = jnp.exp(last[0]) * state_w + tdot(tail.astype(BF16), v)
        cos, sin = turn(base[1][0][b : b + 1], base[1][1][b : b + 1], tt[2], tt[3])
        sin = sin * sign_n
        q = qn[cut, :].astype(F32)
        k = kn[cut, :].astype(F32)
        v = vn[cut, :]

        def other(a):
            return jnp.where(front_n, pltpu.roll(a, 128 - HDN // 2, 1), pltpu.roll(a, HDN // 2, 1))

        q = q * cos + other(q) * sin
        k = (k * cos + other(k) * sin) * HDN**-0.5
        kb = k.astype(BF16)
        probs = []
        for h, mask in enumerate((low, jnp.logical_not(low))):
            qh = jnp.where(mask, q, 0.0).astype(BF16)
            probs.append((dot_t(qh, kb) * spread(r + 1 + h)).astype(BF16))
        v_f = v.astype(F32)
        v2 = jnp.concatenate(
            [jnp.where(low, v_f, 0.0).astype(BF16), jnp.where(low, 0.0, v_f).astype(BF16)], axis=0
        )
        out_b = dot(jnp.concatenate(probs, axis=1), v2)
        if b:
            seen = jnp.where(low, jnp.exp(now[1]), jnp.exp(now[2]))
            out_b += dot((q * seen).astype(BF16), state_n.astype(BF16))
        o_n[cut, :] = out_b
        seen = jnp.where(low, jnp.exp(now[1] + gone[1]), jnp.exp(now[2] + gone[2]))
        qe_n[cut, :] = (q * seen).astype(BF16)
        tail = k * jnp.where(low, jnp.exp(last[1] - now[1]), jnp.exp(last[2] - now[2]))
        keep = jnp.where(low, jnp.exp(last[1]), jnp.exp(last[2]))
        state_n = keep * state_n + jnp.where(same_head, tdot(tail.astype(BF16), v), 0.0)
        gone = [g + t for g, t in zip(gone, last)]

    total_w = jnp.exp(gone[0]) + jnp.zeros((1, 128), F32)
    total_n = jnp.where(low, jnp.exp(gone[1]), jnp.exp(gone[2]))
    packed_n = jnp.where(low, state_n[:HDN], state_n[HDN:])
    sw, sn = 128 // plane, HDN // plane
    for j in range(plane):
        msg[j, 0:sw, :] = state_w[sw * j : sw * (j + 1)]
        msg[j, sw : sw + sn, :] = packed_n[sn * j : sn * (j + 1)]
        msg[j, sw + sn : sw + sn + 1, :] = total_w
        msg[j, sw + sn + 1 : sw + sn + 2, :] = total_n
    ns = sw + sn

    def stage1(d):
        to = lax.rem(me + d, plane)
        return remote(msg.at[to], in1.at[me], s1_s.at[d], s1_r.at[d], at_plane(to))

    for d in range(1, plane):
        stage1(d).start()
    in1[pl.ds(me, 1)] = msg[pl.ds(me, 1)]

    to_r.wait_recv()
    on_r = remote(
        stream_all.at[xl, pl.ds(0, half_rows)], stream_all.at[xl, pl.ds(0, half_rows)],
        st_s.at[2], st_r.at[2], right,
    )
    on_r.start()
    to_l.wait_recv()
    on_l = remote(
        stream_all.at[xr, pl.ds(half_rows, half_rows)], stream_all.at[xr, pl.ds(half_rows, half_rows)],
        st_s.at[3], st_r.at[3], left,
    )
    on_l.start()

    for d in range(1, plane):
        stage1(d).wait_recv()
    wide_row = lax.broadcasted_iota(jnp.int32, (ns, 128), 0) < sw

    def factor(pair):
        return jnp.where(wide_row, pair[0], pair[1])

    def rates(ref, j):
        return ref[j, ns : ns + 1, :], ref[j, ns + 1 : ns + 2, :]

    held = jnp.zeros((ns, 128), F32)
    rate = (jnp.ones((1, 128), F32), jnp.ones((1, 128), F32))
    for j in range(plane):
        pre1[j, 0:ns, :] = held
        pre1[j, ns : ns + 1, :] = rate[0]
        pre1[j, ns + 1 : ns + 2, :] = rate[1]
        mine = rates(in1, j)
        held = held * factor(mine) + in1[j, 0:ns, :]
        rate = (rate[0] * mine[0], rate[1] * mine[1])
    tot2[0:ns, :] = held
    tot2[ns : ns + 1, :] = rate[0]
    tot2[ns + 1 : ns + 2, :] = rate[1]

    def stage2(d):
        return remote(tot2, in2.at[z], s2_s.at[d], s2_r.at[d], {"z": lax.rem(z + d, nz)})

    for d in range(1, nz):
        stage2(d).start()
    in2[pl.ds(z, 1)] = tot2[...][None]
    for d in range(1, nz):
        stage2(d).wait_recv()
    held = jnp.zeros((ns, 128), F32)
    for k in range(nz):
        later = held * factor(rates(in2, k)) + in2[k, 0:ns, :]
        held = jnp.where(k < z, later, held)
    for j in range(plane):
        msg3[j] = held * factor(rates(pre1, j)) + pre1[j, 0:ns, :]

    def stage3(d):
        to = lax.rem(me + d, plane)
        return remote(msg3.at[to], in3.at[me], s3_s.at[d], s3_r.at[d], at_plane(to))

    for d in range(1, plane):
        stage3(d).start()
    in3[pl.ds(me, 1)] = msg3[pl.ds(me, 1)]
    for d in range(1, plane):
        stage3(d).wait_recv()
    arrived = in3[...]
    enter_w = arrived[:, 0:sw, :].reshape(128, 128).astype(BF16)
    enter_p = arrived[:, sw:ns, :].reshape(HDN, 128)
    enter_n = jnp.concatenate(
        [jnp.where(low, enter_p, 0.0), jnp.where(low, 0.0, enter_p)], axis=0
    ).astype(BF16)

    def mixed_to(i, side):
        return remote(
            mixed.at[x, i], mixed.at[x, i], mx_s.at[side, i], mx_r.at[side, i], (right, left)[side]
        )

    def gated(o, gate):
        return (o * jax.nn.silu(gate.astype(F32))).astype(BF16)

    for i in range(nx):
        cut = pl.ds(i * rows, rows)
        o = o_w[cut, :] + dot(qe_w[cut, :], enter_w)
        o = o - jnp.mean(o, axis=-1, keepdims=True)
        o = o * lax.rsqrt(jnp.mean(o * o, axis=-1, keepdims=True) + head_eps)
        mixed[x, i, :, 0:128] = gated(o, gw[cut, :])
        o = o_n[cut, :] + dot(qe_n[cut, :], enter_n)

        def by_head(a):
            first = jnp.sum(jnp.where(low, a, 0.0), axis=-1, keepdims=True)
            second = jnp.sum(jnp.where(low, 0.0, a), axis=-1, keepdims=True)
            return jnp.where(low, first, second) * (1.0 / HDN)

        o = o - by_head(o)
        o = o * lax.rsqrt(by_head(o * o) + head_eps)
        mixed[x, i, :, 128:256] = gated(o, gn[cut, :])
        mixed_to(i, 0).start()
        mixed_to(i, 1).start()

    def mixed_on(i, side):
        src, start = ((xl, 0), (xr, half_rows))[side]
        piece = mixed.at[src, i, pl.ds(start, half_rows)]
        return remote(piece, piece, mx_s.at[2 + side, i], mx_r.at[2 + side, i], (right, left)[side])

    def pass_on(i, _):
        for side in (0, 1):
            mixed_to(i, side).wait_recv()
            mixed_on(i, side).start()
        return 0

    lax.fori_loop(0, nx, pass_on, 0)
    on_r.wait_recv()
    on_l.wait_recv()

    width = stream.shape[1]
    tile = 512
    tiles = width // tile

    def rows_in(i, _):
        mixed_on(i, 0).wait_recv()
        mixed_on(i, 1).wait_recv()

        def project(n, squares):
            at = pl.ds(pl.multiple_of(n * tile, tile), tile)
            total = stream_all[i, :, at].astype(F32)
            for j in range(nx):
                total += dot(mixed[j, i], wo[j, :, at])
            total = total.astype(BF16)
            middle[i, :, at] = total
            total = total.astype(F32)
            return squares + jnp.sum(total * total, axis=-1, keepdims=True)

        squares = lax.fori_loop(0, tiles, project, jnp.zeros((rows, 1), F32))
        scale = lax.rsqrt(squares * (1.0 / width) + norm_eps)
        normed[...] = (middle[i].astype(F32) * scale * gain[...].astype(F32)).astype(BF16)

        def rise(n, _):
            at = pl.ds(pl.multiple_of(n * tile, tile), tile)
            h = jnp.maximum(dot(normed[...], up[:, at]), 0.0)
            hidden[i, :, at] = (h * h).astype(BF16)
            return 0

        lax.fori_loop(0, tiles, rise, 0)
        return 0

    lax.fori_loop(0, nx, rows_in, 0)

    side_tiles = tiles // 2

    def fall(i, side, into):
        def one(n, _):
            at = pl.ds(pl.multiple_of(n * tile, tile), tile)
            part = dot_t(hidden[i], down[pl.ds(pl.multiple_of((side * side_tiles + n) * tile, tile), tile), :])
            into[side, :, at] = part.astype(into.dtype)
            return 0

        lax.fori_loop(0, side_tiles, one, 0)

    far = [
        remote(send2.at[0], relay_l, rs_s.at[0], rs_r.at[0], right),
        remote(send2.at[1], relay_r, rs_s.at[1], rs_r.at[1], left),
    ]
    near_r = [remote(send1.at[s], got_l.at[s], rs_s.at[2 + s], rs_r.at[2 + s], right) for s in (0, 1)]
    near_l = [remote(sendm.at[s], got_r.at[s], rs_s.at[4 + s], rs_r.at[4 + s], left) for s in (0, 1)]
    fall(xo, 0, send2)
    far[0].start()
    fall(xo, 1, send2)
    far[1].start()
    fall(xr, 1, send1)
    near_r[1].start()
    fall(xl, 0, sendm)
    near_l[0].start()
    fall(xr, 0, own)
    fall(xl, 1, own)
    far[0].wait_recv()
    send1[0] = (own[0] + relay_l[...].astype(F32)).astype(BF16)
    near_r[0].start()
    far[1].wait_recv()
    sendm[1] = (own[1] + relay_r[...].astype(F32)).astype(BF16)
    near_l[1].start()
    fall(x, 0, own)
    fall(x, 1, own)
    span = width // 2
    for s, first, second in ((1, near_r, near_l), (0, near_l, near_r)):
        first[s].wait_recv()
        second[s].wait_recv()
        at = slice(s * span, (s + 1) * span)
        total = own[s] + got_l[s].astype(F32) + got_r[s].astype(F32)
        out[:, at] = (middle[x, :, at].astype(F32) + total).astype(BF16)

    for copy in (to_r, to_l, on_r, on_l, *far, *near_r, *near_l):
        copy.wait_send()
    for d in range(1, plane):
        stage1(d).wait_send()
        stage3(d).wait_send()
    for d in range(1, nz):
        stage2(d).wait_send()
    for i in range(nx):
        for side in (0, 1):
            mixed_to(i, side).wait_send()
            mixed_on(i, side).wait_send()


def on_device(
    sizes,
    stream_in, query_wide, key_wide, value_wide, gate_wide, decay_wide,
    query_narrow, key_narrow, value_narrow, gate_narrow, decay_narrow,
    output_wide, output_narrow, norm_gain, up_weight, down_weight,
):
    nz, ny, nc, nx = sizes
    tok = query_wide.shape[0]
    rows, width = stream_in.shape
    plane = ny * nc
    sp_axes = ("z", "y", "c")
    both = jnp.concatenate([up_weight, down_weight.T], axis=1)
    both = lax.all_gather(both, sp_axes, axis=0, tiled=True)
    hid = up_weight.shape[1]
    up, down = both[:, :hid], both[:, hid:]
    wo = lax.all_gather(jnp.concatenate([output_wide, output_narrow], axis=0), "x")
    ns = (128 + HDN) // plane
    dma = pltpu.SemaphoreType.DMA
    vm = pltpu.VMEM
    scratch = [
        vm((nx, rows, width), BF16),
        vm((tok, 128), BF16), vm((tok, 128), BF16), vm((tok, 128), F32), vm((tok, 128), F32),
        vm((128, 128), F32),
        vm((plane, ns + 8, 128), F32), vm((plane, ns + 8, 128), F32), vm((plane, ns + 8, 128), F32),
        vm((ns + 8, 128), F32), vm((nz, ns + 8, 128), F32),
        vm((plane, ns, 128), F32), vm((plane, ns, 128), F32),
        vm((nx, nx, rows, 256), BF16),
        vm((nx, rows, width), BF16), vm((rows, width), BF16), vm((nx, rows, hid), BF16),
        vm((2, rows, width // 2), BF16), vm((2, rows, width // 2), BF16), vm((2, rows, width // 2), BF16),
        vm((2, rows, width // 2), F32),
        vm((rows, width // 2), BF16), vm((rows, width // 2), BF16),
        vm((2, rows, width // 2), BF16), vm((2, rows, width // 2), BF16),
        dma((4,)), dma((4,)),
        dma((plane,)), dma((plane,)), dma((nz,)), dma((nz,)), dma((plane,)), dma((plane,)),
        dma((4, nx)), dma((4, nx)), dma((6,)), dma((6,)),
    ]
    vmem = pl.BlockSpec(memory_space=pltpu.VMEM)
    return pl.pallas_call(
        functools.partial(kernel, sizes),
        out_shape=jax.ShapeDtypeStruct((rows, width), BF16),
        in_specs=[vmem] * 18,
        out_specs=vmem,
        scratch_shapes=scratch,
        compiler_params=pltpu.CompilerParams(
            collective_id=0, has_side_effects=True, vmem_limit_bytes=60 * 1024 * 1024
        ),
    )(
        stream_in, query_wide, key_wide, value_wide, gate_wide, decay_wide,
        query_narrow, key_narrow, value_narrow, gate_narrow, decay_narrow,
        norm_gain[None], jnp.asarray(rope_tables(BLOCK, 1)), jnp.asarray(rope_tables(8, BLOCK)),
        jnp.asarray(rope_tables(nz * plane, tok)), wo, up, down,
    )


def solution(mesh):
    sizes = (8, 4, 2, mesh.shape["tp"])
    split = Mesh(mesh.devices.reshape(sizes), ("z", "y", "c", "x"))
    sp = ("z", "y", "c")
    rows, heads = P(sp, "x"), P("x", sp)
    in_specs = (
        P((*sp, "x"), None), rows, rows, rows, rows, heads, rows, rows, rows, rows, heads,
        P("x", None), P("x", None), P(), rows, heads,
    )
    return jax.shard_map(
        functools.partial(on_device, sizes), mesh=split, in_specs=in_specs,
        out_specs=P((*sp, "x"), None), check_vma=False,
    )
```

```python
import functools

import jax
import jax.numpy as jnp
import numpy as np
from jax import lax
from jax.experimental import pallas as pl
from jax.experimental.pallas import tpu as pltpu
from jax.sharding import Mesh
from jax.sharding import PartitionSpec as P

HDW = 128
HDN = 64
BLOCK = 128
head_eps = 1e-05
norm_eps = 1e-06
rope_base = 10000.0
MESH = pl.DeviceIdType.MESH
F32 = jnp.float32
BF16 = jnp.bfloat16


def rope_tables(steps, stride):
    tables = []
    for width in (HDW, HDN):
        half = width // 2
        inverse = rope_base ** (-np.arange(half, dtype=np.float64) / half)
        lanes = np.tile(inverse, 128 // half)
        angles = (stride * np.arange(steps, dtype=np.float64))[:, None] * lanes[None, :]
        tables += [np.cos(angles), np.sin(angles)]
    return np.stack(tables).astype(np.float32)


def remote(src, dst, send_sem, recv_sem, device):
    return pltpu.make_async_remote_copy(
        src_ref=src, dst_ref=dst, send_sem=send_sem, recv_sem=recv_sem, device_id=device, device_id_type=MESH
    )


def turn(cos_a, sin_a, cos_b, sin_b):
    return cos_a * cos_b - sin_a * sin_b, sin_a * cos_b + cos_a * sin_b


def dot(a, b):
    return jnp.dot(a, b, preferred_element_type=F32)


def dot_t(a, b):
    return lax.dot_general(a, b, (((1,), (1,)), ((), ())), preferred_element_type=F32)


def tdot(a, b):
    return lax.dot_general(a, b, (((0,), (0,)), ((), ())), preferred_element_type=F32)


def kernel(
    sizes,
    stream, qw, kw, vw, gw, dw, qn, kn, vn, gn, dn, gain, tt, tb, ts, ow, on, up_own, down_own,
    out,
    up, down, wo,
    stream_all, qe_w, qe_n, o_w, o_n, decays, msg, in1, pre1, tot2, in2, msg3, in3,
    mixed, middle, normed, hidden, send2, send1, sendm, own, relay_l, relay_r, got_l, got_r,
    st_s, st_r, s1_s, s1_r, s2_s, s2_r, s3_s, s3_r, mx_s, mx_r, rs_s, rs_r,
    in_s, wo_s, wo_r, uz_s, uz_r, uy_s, uy_r, ur_s, ur_r, dy_s, dy_r, dz_s, dz_r, core_s, core_r,
):
    nz, ny, nc, nx = sizes
    z, y, c, x = (lax.axis_index(a) for a in ("z", "y", "c", "x"))
    xr, xl, xo = lax.rem(x + 1, nx), lax.rem(x + nx - 1, nx), lax.rem(x + 2, nx)
    plane = ny * nc
    me = y * nc + c
    sp = z * plane + me
    tok = qw.shape[0]
    blocks = tok // BLOCK
    rows = stream.shape[0]
    width = stream.shape[1]
    half_rows = rows // 2
    right, left = {"x": xr}, {"x": xl}

    def at_plane(j):
        return {"y": j // nc, "c": lax.rem(j, nc)}

    loads = [
        pltpu.make_async_copy(up_own, up.at[z, y, c], in_s.at[0]),
        pltpu.make_async_copy(down_own, down.at[z, y, c], in_s.at[1]),
        pltpu.make_async_copy(ow, wo.at[x, 0], in_s.at[2]),
        pltpu.make_async_copy(on, wo.at[x, 1], in_s.at[3]),
        pltpu.make_async_copy(stream, stream_all.at[x], in_s.at[4]),
    ]
    for load in loads:
        load.start()

    barrier = pltpu.get_barrier_semaphore()
    peers = [right, left]
    peers += [at_plane(lax.rem(me + d, plane)) for d in range(1, plane)]
    peers += [{"z": lax.rem(z + d, nz)} for d in range(1, nz)]
    for peer in peers:
        pl.semaphore_signal(barrier, inc=1, device_id=peer, device_id_type=MESH)
    pl.semaphore_wait(barrier, len(peers))

    sent = []

    def go(copy):
        copy.start()
        sent.append(copy)

    def same(ref, send_sem, recv_sem, device):
        return remote(ref, ref, send_sem, recv_sem, device)

    z_to = ({"z": lax.rem(z + 1, nz)}, {"z": lax.rem(z + nz - 1, nz)})
    y_to = ({"y": lax.rem(y + 1, ny)}, {"y": lax.rem(y + ny - 1, ny)})
    x_to = (right, left)
    partner = {"c": 1 - c}
    fwd = (1, -1)

    def at_z(k):
        return lax.rem(z + nz + k, nz)

    def at_y(k):
        return lax.rem(y + ny + k, ny)

    def at_x(k):
        return lax.rem(x + nx + k, nx)

    part = up.shape[3]
    halves = (pl.ds(0, part // 2), pl.ds(part // 2, part // 2))

    def uz(step, side):
        ref = up.at[at_z(-fwd[side] * (step - 1)), y, c]
        if step == nz // 2:
            ref = ref.at[halves[side]]
        return same(ref, uz_s.at[side, step - 1], uz_r.at[side, step - 1], z_to[side])

    def uz_in(step, side):
        ref = up.at[at_z(-fwd[side] * step), y, c]
        if step == nz // 2:
            ref = ref.at[halves[side]]
        return same(ref, uz_s.at[side, step - 1], uz_r.at[side, step - 1], z_to[side])

    def uy(off, side):
        return same(up.at[at_z(off), y, c], uy_s.at[side, off % nz], uy_r.at[side, off % nz], y_to[side])

    def uy_in(off, side):
        ref = up.at[at_z(off), at_y(-fwd[side]), c]
        return same(ref, uy_s.at[side, off % nz], uy_r.at[side, off % nz], y_to[side])

    relayed = ((0, 1, 2, 3), (4, -1, -2, -3))

    def ur(i, side):
        ref = up.at[at_z(relayed[side][i]), at_y(-fwd[side]), c]
        return same(ref, ur_s.at[side, i], ur_r.at[side, i], y_to[side])

    def ur_in(i, side):
        ref = up.at[at_z(relayed[side][i]), at_y(2), c]
        return same(ref, ur_s.at[side, i], ur_r.at[side, i], y_to[side])

    def u_core(i):
        ref = up.at[:, at_y((0, 1, -1, 2)[i]), c]
        return same(ref, core_s.at[i], core_r.at[i], partner)

    def u_core_in(i):
        ref = up.at[:, at_y((0, 1, -1, 2)[i]), 1 - c]
        return same(ref, core_s.at[i], core_r.at[i], partner)

    def u_own():
        for side in (0, 1):
            go(uz(1, side))
        for side in (0, 1):
            go(uy(0, side))

    def u_step(step):
        for side in (0, 1):
            uz_in(step, side).wait_recv()
            if step < nz // 2:
                go(uz(step + 1, side))
        offs = (-step, step) if step < nz // 2 else (step,)
        for off in offs:
            for side in (0, 1):
                go(uy(off, side))
        if step == nz // 2:
            go(u_core(0))

    def u_relay(*which):
        for i, side in which:
            uy_in(relayed[side][i], side).wait_recv()
            go(ur(i, side))

    def u_rest():
        for side in (0, 1):
            for off in relayed[1 - side]:
                uy_in(off, side).wait_recv()
        go(u_core(1))
        go(u_core(2))

    def u_last():
        for side in (0, 1):
            for i in range(nz // 2):
                ur_in(i, side).wait_recv()
        go(u_core(3))

    def u_done():
        for i in range(ny):
            u_core_in(i).wait_recv()

    def dy(step, side):
        ref = down.at[z, at_y(-fwd[side] * (step - 1)), c]
        if step == 2:
            ref = ref.at[halves[side]]
        return same(ref, dy_s.at[side, step - 1], dy_r.at[side, step - 1], y_to[side])

    def dy_in(step, side):
        ref = down.at[z, at_y(-fwd[side] * step), c]
        if step == 2:
            ref = ref.at[halves[side]]
        return same(ref, dy_s.at[side, step - 1], dy_r.at[side, step - 1], y_to[side])

    columns_y = (0, 1, -1, 2)
    last_by = ((0, 1), (2, 3))

    def dz(step, side, g):
        ref = down.at[at_z(-fwd[side] * (step - 1)), at_y(columns_y[g]), c]
        return same(ref, dz_s.at[side, step - 1, g], dz_r.at[side, step - 1, g], z_to[side])

    def dz_in(step, side, g):
        ref = down.at[at_z(-fwd[side] * step), at_y(columns_y[g]), c]
        return same(ref, dz_s.at[side, step - 1, g], dz_r.at[side, step - 1, g], z_to[side])

    def d_core(k):
        return same(down.at[at_z(k), :, c], core_s.at[4 + k % nz], core_r.at[4 + k % nz], partner)

    def d_core_in(k):
        return same(down.at[at_z(k), :, 1 - c], core_s.at[4 + k % nz], core_r.at[4 + k % nz], partner)

    def d_own():
        for side in (0, 1):
            go(dy(1, side))

    def d_turn():
        for side in (0, 1):
            dy_in(1, side).wait_recv()
            go(dy(2, side))

    def d_column():
        for side in (0, 1):
            dy_in(2, side).wait_recv()
        go(d_core(0))

    def d_send(*gs):
        for side in (0, 1):
            for g in gs:
                go(dz(1, side, g))

    def d_step(step, *gs):
        for g in gs:
            for side in (0, 1):
                if step < nz // 2:
                    dz_in(step, side, g).wait_recv()
                    if step + 1 < nz // 2 or g in last_by[side]:
                        go(dz(step + 1, side, g))
                elif g in last_by[side]:
                    dz_in(step, side, g).wait_recv()

    def d_cores(step):
        go(d_core(step))
        if step < nz // 2:
            go(d_core(-step))

    def d_done():
        for k in range(nz):
            d_core_in(k).wait_recv()

    deep = wo.shape[2]
    wo_halves = (pl.ds(0, deep // 2), pl.ds(deep // 2, deep // 2))

    def wx(step, side):
        ref = wo.at[at_x(-fwd[side] * (step - 1)), c]
        if step == 2:
            ref = ref.at[wo_halves[side]]
        return same(ref, wo_s.at[side, step - 1], wo_r.at[side, step - 1], x_to[side])

    def wx_in(step, side):
        ref = wo.at[at_x(-fwd[side] * step), c]
        if step == 2:
            ref = ref.at[wo_halves[side]]
        return same(ref, wo_s.at[side, step - 1], wo_r.at[side, step - 1], x_to[side])

    def w_core(i):
        return same(wo.at[at_x(i + 1), c], core_s.at[12 + i], core_r.at[12 + i], partner)

    def w_core_in(i):
        return same(wo.at[at_x(i + 1), 1 - c], core_s.at[12 + i], core_r.at[12 + i], partner)

    def w_turn():
        for side in (0, 1):
            wx_in(1, side).wait_recv()
            go(wx(2, side))
        go(w_core(0))
        go(w_core(2))

    def w_last():
        for side in (0, 1):
            wx_in(2, side).wait_recv()
        go(w_core(1))

    def w_done():
        for i in range(nx - 1):
            w_core_in(i).wait_recv()

    for load in loads:
        load.wait()
    u_own()
    d_own()
    for side in (0, 1):
        go(wx(1, side))

    to_r = same(stream_all.at[x], st_s.at[0], st_r.at[0], right)
    to_l = same(stream_all.at[x], st_s.at[1], st_r.at[1], left)
    to_r.start()
    to_l.start()

    lane = lax.broadcasted_iota(jnp.int32, (1, 128), 1)
    low = lane < HDN
    base = []
    for g in (0, 2):
        row = [ts[g + i, pl.ds(sp, 1), :] for i in (0, 1)]
        base.append(turn(row[0], row[1], tb[g], tb[g + 1]))
    sign_w = jnp.where(lane < HDW // 2, -1.0, 1.0)
    front_n = lax.rem(lane, HDN) < HDN // 2
    sign_n = jnp.where(front_n, -1.0, 1.0)

    decays[...] = jnp.zeros_like(decays)
    for b in range(blocks):
        cut = pl.ds(b * BLOCK, BLOCK)
        decays[pl.ds(3 * b, 1), :] = dw[:, cut]
        decays[pl.ds(3 * b + 1, 2), :] = dn[:, cut]
    running = decays[0:32, :]
    shift = 1
    while shift < BLOCK:
        running = running + jnp.where(lane >= shift, pltpu.roll(running, shift, 1), 0.0)
        shift *= 2
    decays[0:32, :] = running
    columns = jnp.transpose(decays[...])

    at_t = lax.broadcasted_iota(jnp.int32, (BLOCK, BLOCK), 0)
    at_s = lax.broadcasted_iota(jnp.int32, (BLOCK, BLOCK), 1)
    lower = at_t >= at_s
    same_head = (at_t < HDN) == (at_s < HDN)

    def spread(r):
        steps = jnp.minimum(columns[:, r : r + 1] - decays[pl.ds(r, 1), :], 0.0)
        return jnp.where(lower, jnp.exp(steps), 0.0)

    def tick(b):
        if b == 0:
            d_turn()
            d_send(0)
        elif b == 1:
            u_step(1)
            d_column()
        elif b == 2:
            u_relay((0, 0))
            d_send(1, 2)
        elif b == 3:
            u_step(2)
            w_turn()
        elif b == 4:
            u_relay((1, 0), (1, 1))
            d_send(3)
        elif b == 5:
            u_step(3)

    state_w = jnp.zeros((128, 128), F32)
    state_n = jnp.zeros((128, 128), F32)
    gone = [jnp.zeros((1, 1), F32)] * 3
    for b in range(blocks):
        cut = pl.ds(b * BLOCK, BLOCK)
        r = 3 * b
        now = [columns[:, r + h : r + h + 1] for h in range(3)]
        last = [columns[BLOCK - 1 : BLOCK, r + h : r + h + 1] for h in range(3)]
        cos, sin = turn(base[0][0][b : b + 1], base[0][1][b : b + 1], tt[0], tt[1])
        sin = sin * sign_w
        q = qw[cut, :].astype(F32)
        k = kw[cut, :].astype(F32)
        v = vw[cut, :]
        q = q * cos + pltpu.roll(q, HDW // 2, 1) * sin
        k = (k * cos + pltpu.roll(k, HDW // 2, 1) * sin) * HDW**-0.5
        scores = dot_t(q.astype(BF16), k.astype(BF16)) * spread(r)
        out_b = dot(scores.astype(BF16), v)
        if b:
            out_b += dot((q * jnp.exp(now[0])).astype(BF16), state_w.astype(BF16))
        o_w[cut, :] = out_b
        qe_w[cut, :] = (q * jnp.exp(now[0] + gone[0])).astype(BF16)
        tail = k * jnp.exp(last[0] - now[0])
        state_w = jnp.exp(last[0]) * state_w + tdot(tail.astype(BF16), v)
        cos, sin = turn(base[1][0][b : b + 1], base[1][1][b : b + 1], tt[2], tt[3])
        sin = sin * sign_n
        q = qn[cut, :].astype(F32)
        k = kn[cut, :].astype(F32)
        v = vn[cut, :]

        def other(a):
            return jnp.where(front_n, pltpu.roll(a, 128 - HDN // 2, 1), pltpu.roll(a, HDN // 2, 1))

        q = q * cos + other(q) * sin
        k = (k * cos + other(k) * sin) * HDN**-0.5
        kb = k.astype(BF16)
        probs = []
        for h, mask in enumerate((low, jnp.logical_not(low))):
            qh = jnp.where(mask, q, 0.0).astype(BF16)
            probs.append((dot_t(qh, kb) * spread(r + 1 + h)).astype(BF16))
        v_f = v.astype(F32)
        v2 = jnp.concatenate(
            [jnp.where(low, v_f, 0.0).astype(BF16), jnp.where(low, 0.0, v_f).astype(BF16)], axis=0
        )
        out_b = dot(jnp.concatenate(probs, axis=1), v2)
        if b:
            seen = jnp.where(low, jnp.exp(now[1]), jnp.exp(now[2]))
            out_b += dot((q * seen).astype(BF16), state_n.astype(BF16))
        o_n[cut, :] = out_b
        seen = jnp.where(low, jnp.exp(now[1] + gone[1]), jnp.exp(now[2] + gone[2]))
        qe_n[cut, :] = (q * seen).astype(BF16)
        tail = k * jnp.where(low, jnp.exp(last[1] - now[1]), jnp.exp(last[2] - now[2]))
        keep = jnp.where(low, jnp.exp(last[1]), jnp.exp(last[2]))
        state_n = keep * state_n + jnp.where(same_head, tdot(tail.astype(BF16), v), 0.0)
        gone = [g + t for g, t in zip(gone, last)]
        tick(b)

    total_w = jnp.exp(gone[0]) + jnp.zeros((1, 128), F32)
    total_n = jnp.where(low, jnp.exp(gone[1]), jnp.exp(gone[2]))
    packed_n = jnp.where(low, state_n[:HDN], state_n[HDN:])
    sw, sn = 128 // plane, HDN // plane
    for j in range(plane):
        msg[j, 0:sw, :] = state_w[sw * j : sw * (j + 1)]
        msg[j, sw : sw + sn, :] = packed_n[sn * j : sn * (j + 1)]
        msg[j, sw + sn : sw + sn + 1, :] = total_w
        msg[j, sw + sn + 1 : sw + sn + 2, :] = total_n
    ns = sw + sn

    def stage1(d):
        to = lax.rem(me + d, plane)
        return remote(msg.at[to], in1.at[me], s1_s.at[d], s1_r.at[d], at_plane(to))

    for d in range(1, plane):
        stage1(d).start()
    in1[pl.ds(me, 1)] = msg[pl.ds(me, 1)]

    on_r = same(stream_all.at[xl, pl.ds(0, half_rows)], st_s.at[2], st_r.at[2], right)
    on_l = same(stream_all.at[xr, pl.ds(half_rows, half_rows)], st_s.at[3], st_r.at[3], left)

    d_step(1, 0)
    for d in range(1, plane):
        stage1(d).wait_recv()
    wide_row = lax.broadcasted_iota(jnp.int32, (ns, 128), 0) < sw

    def factor(pair):
        return jnp.where(wide_row, pair[0], pair[1])

    def rates(ref, j):
        return ref[j, ns : ns + 1, :], ref[j, ns + 1 : ns + 2, :]

    held = jnp.zeros((ns, 128), F32)
    rate = (jnp.ones((1, 128), F32), jnp.ones((1, 128), F32))
    for j in range(plane):
        pre1[j, 0:ns, :] = held
        pre1[j, ns : ns + 1, :] = rate[0]
        pre1[j, ns + 1 : ns + 2, :] = rate[1]
        mine = rates(in1, j)
        held = held * factor(mine) + in1[j, 0:ns, :]
        rate = (rate[0] * mine[0], rate[1] * mine[1])
    tot2[0:ns, :] = held
    tot2[ns : ns + 1, :] = rate[0]
    tot2[ns + 1 : ns + 2, :] = rate[1]

    def stage2(d):
        return remote(tot2, in2.at[z], s2_s.at[d], s2_r.at[d], {"z": lax.rem(z + d, nz)})

    for d in range(1, nz):
        stage2(d).start()
    u_relay((2, 0), (2, 1))
    u_step(4)
    in2[pl.ds(z, 1)] = tot2[...][None]
    for d in range(1, nz):
        stage2(d).wait_recv()
    held = jnp.zeros((ns, 128), F32)
    for k in range(nz):
        later = held * factor(rates(in2, k)) + in2[k, 0:ns, :]
        held = jnp.where(k < z, later, held)
    for j in range(plane):
        msg3[j] = held * factor(rates(pre1, j)) + pre1[j, 0:ns, :]

    def stage3(d):
        to = lax.rem(me + d, plane)
        return remote(msg3.at[to], in3.at[me], s3_s.at[d], s3_r.at[d], at_plane(to))

    for d in range(1, plane):
        stage3(d).start()
    in3[pl.ds(me, 1)] = msg3[pl.ds(me, 1)]
    d_step(1, 1, 2)
    for d in range(1, plane):
        stage3(d).wait_recv()
    arrived = in3[...]
    enter_w = arrived[:, 0:sw, :].reshape(128, 128).astype(BF16)
    enter_p = arrived[:, sw:ns, :].reshape(HDN, 128)
    enter_n = jnp.concatenate(
        [jnp.where(low, enter_p, 0.0), jnp.where(low, 0.0, enter_p)], axis=0
    ).astype(BF16)

    u_relay((3, 0), (3, 1), (0, 1))
    d_step(2, 0)
    d_step(1, 3)
    d_cores(1)

    def mixed_to(i, side):
        return remote(
            mixed.at[x, i], mixed.at[x, i], mx_s.at[side, i], mx_r.at[side, i], (right, left)[side]
        )

    def gated(o, gate):
        return (o * jax.nn.silu(gate.astype(F32))).astype(BF16)

    for i in range(nx):
        cut = pl.ds(i * rows, rows)
        o = o_w[cut, :] + dot(qe_w[cut, :], enter_w)
        o = o - jnp.mean(o, axis=-1, keepdims=True)
        o = o * lax.rsqrt(jnp.mean(o * o, axis=-1, keepdims=True) + head_eps)
        mixed[x, i, :, 0:128] = gated(o, gw[cut, :])
        o = o_n[cut, :] + dot(qe_n[cut, :], enter_n)

        def by_head(a):
            first = jnp.sum(jnp.where(low, a, 0.0), axis=-1, keepdims=True)
            second = jnp.sum(jnp.where(low, 0.0, a), axis=-1, keepdims=True)
            return jnp.where(low, first, second) * (1.0 / HDN)

        o = o - by_head(o)
        o = o * lax.rsqrt(by_head(o * o) + head_eps)
        mixed[x, i, :, 128:256] = gated(o, gn[cut, :])
        mixed_to(i, 0).start()
        mixed_to(i, 1).start()

    def mixed_on(i, side):
        src, start = ((xl, 0), (xr, half_rows))[side]
        piece = mixed.at[src, i, pl.ds(start, half_rows)]
        return remote(piece, piece, mx_s.at[2 + side, i], mx_r.at[2 + side, i], (right, left)[side])

    to_r.wait_recv()
    on_r.start()
    to_l.wait_recv()
    on_l.start()
    d_step(2, 1, 2)
    u_rest()
    w_last()
    d_step(3, 0)
    d_step(2, 3)
    d_cores(2)
    u_last()

    def pass_on(i, _):
        for side in (0, 1):
            mixed_to(i, side).wait_recv()
            mixed_on(i, side).start()
        return 0

    lax.fori_loop(0, nx, pass_on, 0)
    on_r.wait_recv()
    on_l.wait_recv()
    w_done()
    d_step(3, 1, 2)

    tile = 512
    tiles = width // tile

    def rows_in(i, _):
        mixed_on(i, 0).wait_recv()
        mixed_on(i, 1).wait_recv()

        def project(n, squares):
            at = pl.ds(pl.multiple_of(n * tile, tile), tile)
            total = stream_all[i, :, at].astype(F32)
            for j in range(nx):
                total += dot(mixed[j, i], wo[j, :, :, at].reshape(2 * deep, tile))
            total = total.astype(BF16)
            middle[i, :, at] = total
            total = total.astype(F32)
            return squares + jnp.sum(total * total, axis=-1, keepdims=True)

        squares = lax.fori_loop(0, tiles, project, jnp.zeros((rows, 1), F32))
        scale = lax.rsqrt(squares * (1.0 / width) + norm_eps)
        normed[i] = (middle[i].astype(F32) * scale * gain[...].astype(F32)).astype(BF16)
        return 0

    lax.fori_loop(0, nx, rows_in, 0)
    d_step(3, 3)
    d_cores(3)
    u_done()

    def rise(n, _):
        at = pl.ds(pl.multiple_of(n * tile, tile), tile)

        def one(i, _):
            h = jnp.maximum(dot(normed[i], up[:, :, :, :, at].reshape(width, tile)), 0.0)
            hidden[i, :, at] = (h * h).astype(BF16)
            return 0

        return lax.fori_loop(0, nx, one, 0)

    lax.fori_loop(0, tiles, rise, 0)
    d_step(4, 0, 1, 2, 3)
    d_cores(4)
    d_done()

    side_tiles = tiles // 2
    per_tile = nz // tiles

    def fall(i, side, into):
        def one(n, _):
            at = pl.ds(pl.multiple_of(n * tile, tile), tile)
            of_z = pl.ds((side * side_tiles + n) * per_tile, per_tile)
            part = dot_t(hidden[i], down[of_z].reshape(tile, width))
            into[side, :, at] = part.astype(into.dtype)
            return 0

        lax.fori_loop(0, side_tiles, one, 0)

    far = [
        remote(send2.at[0], relay_l, rs_s.at[0], rs_r.at[0], right),
        remote(send2.at[1], relay_r, rs_s.at[1], rs_r.at[1], left),
    ]
    near_r = [remote(send1.at[s], got_l.at[s], rs_s.at[2 + s], rs_r.at[2 + s], right) for s in (0, 1)]
    near_l = [remote(sendm.at[s], got_r.at[s], rs_s.at[4 + s], rs_r.at[4 + s], left) for s in (0, 1)]
    fall(xo, 0, send2)
    far[0].start()
    fall(xo, 1, send2)
    far[1].start()
    fall(xr, 1, send1)
    near_r[1].start()
    fall(xl, 0, sendm)
    near_l[0].start()
    fall(xr, 0, own)
    fall(xl, 1, own)
    far[0].wait_recv()
    send1[0] = (own[0] + relay_l[...].astype(F32)).astype(BF16)
    near_r[0].start()
    far[1].wait_recv()
    sendm[1] = (own[1] + relay_r[...].astype(F32)).astype(BF16)
    near_l[1].start()
    fall(x, 0, own)
    fall(x, 1, own)
    span = width // 2
    for s, first, second in ((1, near_r, near_l), (0, near_l, near_r)):
        first[s].wait_recv()
        second[s].wait_recv()
        at = slice(s * span, (s + 1) * span)
        total = own[s] + got_l[s].astype(F32) + got_r[s].astype(F32)
        out[:, at] = (middle[x, :, at].astype(F32) + total).astype(BF16)

    for copy in sent:
        copy.wait_send()
    for copy in (to_r, to_l, on_r, on_l, *far, *near_r, *near_l):
        copy.wait_send()
    for d in range(1, plane):
        stage1(d).wait_send()
        stage3(d).wait_send()
    for d in range(1, nz):
        stage2(d).wait_send()
    for i in range(nx):
        for side in (0, 1):
            mixed_to(i, side).wait_send()
            mixed_on(i, side).wait_send()


def on_device(
    sizes,
    stream_in, query_wide, key_wide, value_wide, gate_wide, decay_wide,
    query_narrow, key_narrow, value_narrow, gate_narrow, decay_narrow,
    output_wide, output_narrow, norm_gain, up_weight, down_weight,
):
    nz, ny, nc, nx = sizes
    tok = query_wide.shape[0]
    rows, width = stream_in.shape
    plane = ny * nc
    part, hid = up_weight.shape
    ns = (128 + HDN) // plane
    dma = pltpu.SemaphoreType.DMA
    vm = pltpu.VMEM
    scratch = [
        vm((nz, ny, nc, part, hid), BF16), vm((nz, ny, nc, part, hid), BF16), vm((nx, 2, *output_wide.shape), BF16),
        vm((nx, rows, width), BF16),
        vm((tok, 128), BF16), vm((tok, 128), BF16), vm((tok, 128), F32), vm((tok, 128), F32),
        vm((128, 128), F32),
        vm((plane, ns + 8, 128), F32), vm((plane, ns + 8, 128), F32), vm((plane, ns + 8, 128), F32),
        vm((ns + 8, 128), F32), vm((nz, ns + 8, 128), F32),
        vm((plane, ns, 128), F32), vm((plane, ns, 128), F32),
        vm((nx, nx, rows, 256), BF16),
        vm((nx, rows, width), BF16), vm((nx, rows, width), BF16), vm((nx, rows, hid), BF16),
        vm((2, rows, width // 2), BF16), vm((2, rows, width // 2), BF16), vm((2, rows, width // 2), BF16),
        vm((2, rows, width // 2), F32),
        vm((rows, width // 2), BF16), vm((rows, width // 2), BF16),
        vm((2, rows, width // 2), BF16), vm((2, rows, width // 2), BF16),
        dma((4,)), dma((4,)),
        dma((plane,)), dma((plane,)), dma((nz,)), dma((nz,)), dma((plane,)), dma((plane,)),
        dma((4, nx)), dma((4, nx)), dma((6,)), dma((6,)),
        dma((5,)), dma((2, 2)), dma((2, 2)), dma((2, 4)), dma((2, 4)), dma((2, nz)), dma((2, nz)),
        dma((2, 4)), dma((2, 4)), dma((2, 2)), dma((2, 2)), dma((2, 4, 4)), dma((2, 4, 4)), dma((15,)), dma((15,)),
    ]
    vmem = pl.BlockSpec(memory_space=pltpu.VMEM)
    hbm = pl.BlockSpec(memory_space=pl.ANY)
    return pl.pallas_call(
        functools.partial(kernel, sizes),
        out_shape=jax.ShapeDtypeStruct((rows, width), BF16),
        in_specs=[hbm] + [vmem] * 14 + [hbm] * 4,
        out_specs=vmem,
        scratch_shapes=scratch,
        compiler_params=pltpu.CompilerParams(
            collective_id=0, has_side_effects=True, vmem_limit_bytes=60 * 1024 * 1024
        ),
    )(
        stream_in, query_wide, key_wide, value_wide, gate_wide, decay_wide,
        query_narrow, key_narrow, value_narrow, gate_narrow, decay_narrow,
        norm_gain[None], jnp.asarray(rope_tables(BLOCK, 1)), jnp.asarray(rope_tables(8, BLOCK)),
        jnp.asarray(rope_tables(nz * plane, tok)),
        output_wide, output_narrow, up_weight, down_weight.T,
    )


def solution(mesh):
    sizes = (8, 4, 2, mesh.shape["tp"])
    split = Mesh(mesh.devices.reshape(sizes), ("z", "y", "c", "x"))
    sp = ("z", "y", "c")
    rows, heads = P(sp, "x"), P("x", sp)
    in_specs = (
        P((*sp, "x"), None), rows, rows, rows, rows, heads, rows, rows, rows, rows, heads,
        P("x", None), P("x", None), P(), rows, heads,
    )
    return jax.shard_map(
        functools.partial(on_device, sizes), mesh=split, in_specs=in_specs,
        out_specs=P((*sp, "x"), None), check_vma=False,
    )
```

```python
import functools

import jax
import jax.numpy as jnp
import numpy as np
from jax import lax
from jax.experimental import pallas as pl
from jax.experimental.pallas import tpu as pltpu
from jax.sharding import Mesh
from jax.sharding import PartitionSpec as P

HDW = 128
HDN = 64
BLOCK = 128
head_eps = 1e-05
norm_eps = 1e-06
rope_base = 10000.0
MESH = pl.DeviceIdType.MESH
F32 = jnp.float32
BF16 = jnp.bfloat16


def rope_tables(steps, stride):
    tables = []
    for width in (HDW, HDN):
        half = width // 2
        inverse = rope_base ** (-np.arange(half, dtype=np.float64) / half)
        lanes = np.tile(inverse, 128 // half)
        angles = (stride * np.arange(steps, dtype=np.float64))[:, None] * lanes[None, :]
        tables += [np.cos(angles), np.sin(angles)]
    return np.stack(tables).astype(np.float32)


def remote(src, dst, send_sem, recv_sem, device):
    return pltpu.make_async_remote_copy(
        src_ref=src, dst_ref=dst, send_sem=send_sem, recv_sem=recv_sem, device_id=device, device_id_type=MESH
    )


def turn(cos_a, sin_a, cos_b, sin_b):
    return cos_a * cos_b - sin_a * sin_b, sin_a * cos_b + cos_a * sin_b


def dot(a, b):
    return jnp.dot(a, b, preferred_element_type=F32)


def dot_t(a, b):
    return lax.dot_general(a, b, (((1,), (1,)), ((), ())), preferred_element_type=F32)


def tdot(a, b):
    return lax.dot_general(a, b, (((0,), (0,)), ((), ())), preferred_element_type=F32)


def kernel(
    sizes,
    dw, dn, gain, tt, tb, ts,
    qw_in, kw_in, vw_in, qn_in, kn_in, vn_in, gw_in, gn_in, stream_in, ow, on, up_own, down_own,
    out,
    qw, kw, vw, qn, kn, vn, gw, gn, stream,
    up, down, wo,
    qe_w, qe_n, o_w, o_n, decays, msg, in1, tot2, in2, msg3, in3,
    mixed, mix_in, middle, normed, hidden, send2, send1, sendm, own, relay_l, relay_r, got_l, got_r,
    st_s, st_r, s1_s, s1_r, s2_s, s2_r, s3_s, s3_r, mx_s, mx_r, rs_s, rs_r,
    in_s, wo_s, wo_r, uz_s, uz_r, uy_s, uy_r, ur_s, ur_r, dy_s, dy_r, dz_s, dz_r, core_s, core_r,
):
    nz, ny, nc, nx = sizes
    z, y, c, x = (lax.axis_index(a) for a in ("z", "y", "c", "x"))
    xr, xl, xo = lax.rem(x + 1, nx), lax.rem(x + nx - 1, nx), lax.rem(x + 2, nx)
    plane = ny * nc
    me = y * nc + c
    sp = z * plane + me
    tok = qw.shape[0]
    blocks = tok // BLOCK
    rows = stream.shape[0]
    width = stream.shape[1]
    half_rows, part_rows = rows // 2, rows // 4
    right, left = {"x": xr}, {"x": xl}

    def at_plane(j):
        return {"y": j // nc, "c": lax.rem(j, nc)}

    barrier = pltpu.get_barrier_semaphore()
    peers = [right, left, {"x": xo}]
    peers += [at_plane(lax.rem(me + d, plane)) for d in range(1, plane)]
    peers += [{"z": lax.rem(z + d, nz)} for d in range(1, nz)]
    for peer in peers:
        pl.semaphore_signal(barrier, inc=1, device_id=peer, device_id_type=MESH)

    pairs = [
        (qw_in, qw), (kw_in, kw), (vw_in, vw), (qn_in, qn), (kn_in, kn), (vn_in, vn),
        (up_own, up.at[z, y, c]), (ow, wo.at[x, 0]), (on, wo.at[x, 1]), (down_own, down.at[z, y, c]),
        (gw_in, gw), (gn_in, gn), (stream_in, stream),
    ]
    loads = [pltpu.make_async_copy(a, b, in_s.at[i]) for i, (a, b) in enumerate(pairs)]
    for load in loads:
        load.start()

    lane = lax.broadcasted_iota(jnp.int32, (1, 128), 1)
    low = lane < HDN
    base = []
    for g in (0, 2):
        row = [ts[g + i, pl.ds(sp, 1), :] for i in (0, 1)]
        base.append(turn(row[0], row[1], tb[g], tb[g + 1]))
    sign_w = jnp.where(lane < HDW // 2, -1.0, 1.0)
    front_n = lax.rem(lane, HDN) < HDN // 2
    sign_n = jnp.where(front_n, -1.0, 1.0)

    sent = []

    def go(copy):
        copy.start()
        sent.append(copy)

    def same(ref, send_sem, recv_sem, device):
        return remote(ref, ref, send_sem, recv_sem, device)

    z_to = ({"z": lax.rem(z + 1, nz)}, {"z": lax.rem(z + nz - 1, nz)})
    y_to = ({"y": lax.rem(y + 1, ny)}, {"y": lax.rem(y + ny - 1, ny)})
    x_to = (right, left)
    partner = {"c": 1 - c}
    fwd = (1, -1)

    def at_z(k):
        return lax.rem(z + nz + k, nz)

    def at_y(k):
        return lax.rem(y + ny + k, ny)

    def at_x(k):
        return lax.rem(x + nx + k, nx)

    part = up.shape[3]
    halves = (pl.ds(0, part // 2), pl.ds(part // 2, part // 2))

    def uz(step, side):
        ref = up.at[at_z(-fwd[side] * (step - 1)), y, c]
        if step == nz // 2:
            ref = ref.at[halves[side]]
        return same(ref, uz_s.at[side, step - 1], uz_r.at[side, step - 1], z_to[side])

    def uz_in(step, side):
        ref = up.at[at_z(-fwd[side] * step), y, c]
        if step == nz // 2:
            ref = ref.at[halves[side]]
        return same(ref, uz_s.at[side, step - 1], uz_r.at[side, step - 1], z_to[side])

    def uy(off, side):
        return same(up.at[at_z(off), y, c], uy_s.at[side, off % nz], uy_r.at[side, off % nz], y_to[side])

    def uy_in(off, side):
        ref = up.at[at_z(off), at_y(-fwd[side]), c]
        return same(ref, uy_s.at[side, off % nz], uy_r.at[side, off % nz], y_to[side])

    relayed = ((0, 1, 2, 3), (4, -1, -2, -3))

    def ur(i, side):
        ref = up.at[at_z(relayed[side][i]), at_y(-fwd[side]), c]
        return same(ref, ur_s.at[side, i], ur_r.at[side, i], y_to[side])

    def ur_in(i, side):
        ref = up.at[at_z(relayed[side][i]), at_y(2), c]
        return same(ref, ur_s.at[side, i], ur_r.at[side, i], y_to[side])

    def u_core(i):
        ref = up.at[:, at_y((0, 1, -1, 2)[i]), c]
        return same(ref, core_s.at[i], core_r.at[i], partner)

    def u_core_in(i):
        ref = up.at[:, at_y((0, 1, -1, 2)[i]), 1 - c]
        return same(ref, core_s.at[i], core_r.at[i], partner)

    def u_own():
        for side in (0, 1):
            go(uz(1, side))
        for side in (0, 1):
            go(uy(0, side))

    def u_step(step):
        for side in (0, 1):
            uz_in(step, side).wait_recv()
            if step < nz // 2:
                go(uz(step + 1, side))

    def u_turn(step):
        offs = (-step, step) if step < nz // 2 else (step,)
        for off in offs:
            for side in (0, 1):
                go(uy(off, side))
        if step == nz // 2:
            go(u_core(0))

    def u_relay(*which):
        for i, side in which:
            uy_in(relayed[side][i], side).wait_recv()
            go(ur(i, side))

    def u_rest():
        for side in (0, 1):
            for off in relayed[1 - side]:
                uy_in(off, side).wait_recv()
        go(u_core(1))
        go(u_core(2))

    def u_last():
        for side in (0, 1):
            for i in range(nz // 2):
                ur_in(i, side).wait_recv()
        go(u_core(3))

    def u_done():
        for i in range(ny):
            u_core_in(i).wait_recv()

    def dy(step, side):
        ref = down.at[z, at_y(-fwd[side] * (step - 1)), c]
        if step == 2:
            ref = ref.at[halves[side]]
        return same(ref, dy_s.at[side, step - 1], dy_r.at[side, step - 1], y_to[side])

    def dy_in(step, side):
        ref = down.at[z, at_y(-fwd[side] * step), c]
        if step == 2:
            ref = ref.at[halves[side]]
        return same(ref, dy_s.at[side, step - 1], dy_r.at[side, step - 1], y_to[side])

    columns_y = (0, 1, -1, 2)
    last_by = ((0, 1), (2, 3))

    def dz(step, side, g):
        ref = down.at[at_z(-fwd[side] * (step - 1)), at_y(columns_y[g]), c]
        return same(ref, dz_s.at[side, step - 1, g], dz_r.at[side, step - 1, g], z_to[side])

    def dz_in(step, side, g):
        ref = down.at[at_z(-fwd[side] * step), at_y(columns_y[g]), c]
        return same(ref, dz_s.at[side, step - 1, g], dz_r.at[side, step - 1, g], z_to[side])

    def d_core(k):
        return same(down.at[at_z(k), :, c], core_s.at[4 + k % nz], core_r.at[4 + k % nz], partner)

    def d_core_in(k):
        return same(down.at[at_z(k), :, 1 - c], core_s.at[4 + k % nz], core_r.at[4 + k % nz], partner)

    def d_own():
        for side in (0, 1):
            go(dy(1, side))

    def d_turn():
        for side in (0, 1):
            dy_in(1, side).wait_recv()
            go(dy(2, side))

    def d_column():
        for side in (0, 1):
            dy_in(2, side).wait_recv()
        go(d_core(0))

    def d_send(*gs):
        for side in (0, 1):
            for g in gs:
                go(dz(1, side, g))

    def d_step(step, *gs):
        for g in gs:
            for side in (0, 1):
                if step < nz // 2:
                    dz_in(step, side, g).wait_recv()
                    if step + 1 < nz // 2 or g in last_by[side]:
                        go(dz(step + 1, side, g))
                elif g in last_by[side]:
                    dz_in(step, side, g).wait_recv()

    def d_cores(step):
        go(d_core(step))
        if step < nz // 2:
            go(d_core(-step))

    def d_done():
        for k in range(nz):
            d_core_in(k).wait_recv()

    deep = wo.shape[2]
    wo_halves = (pl.ds(0, deep // 2), pl.ds(deep // 2, deep // 2))

    def wx(step, side):
        ref = wo.at[at_x(-fwd[side] if step == 2 else 0), c].at[wo_halves[1 - side if step == 1 else side]]
        return same(ref, wo_s.at[side, step], wo_r.at[side, step], x_to[side])

    def wx_in(step, side):
        ref = wo.at[at_x(-fwd[side] * (2 if step == 2 else 1)), c].at[wo_halves[1 - side if step == 1 else side]]
        return same(ref, wo_s.at[side, step], wo_r.at[side, step], x_to[side])

    def w_core(i):
        return same(wo.at[at_x(i + 1), c], core_s.at[12 + i], core_r.at[12 + i], partner)

    def w_core_in(i):
        return same(wo.at[at_x(i + 1), 1 - c], core_s.at[12 + i], core_r.at[12 + i], partner)

    def w_turn():
        for side in (0, 1):
            wx_in(0, side).wait_recv()
            go(wx(2, side))

    def w_near():
        for side in (0, 1):
            wx_in(1, side).wait_recv()
        go(w_core(0))
        go(w_core(2))

    def w_last():
        for side in (0, 1):
            wx_in(2, side).wait_recv()
        go(w_core(1))

    def w_done():
        for i in range(nx - 1):
            w_core_in(i).wait_recv()

    for load in loads[:6]:
        load.wait()

    decays[...] = jnp.zeros_like(decays)
    for b in range(blocks):
        cut = pl.ds(b * BLOCK, BLOCK)
        decays[pl.ds(3 * b, 1), :] = dw[:, cut]
        decays[pl.ds(3 * b + 1, 2), :] = dn[:, cut]
    running = decays[0:32, :]
    shift = 1
    while shift < BLOCK:
        running = running + jnp.where(lane >= shift, pltpu.roll(running, shift, 1), 0.0)
        shift *= 2
    decays[0:32, :] = running
    columns = jnp.transpose(decays[...])

    at_t = lax.broadcasted_iota(jnp.int32, (BLOCK, BLOCK), 0)
    at_s = lax.broadcasted_iota(jnp.int32, (BLOCK, BLOCK), 1)
    lower = at_t >= at_s
    same_head = (at_t < HDN) == (at_s < HDN)

    def spread(r):
        steps = jnp.minimum(columns[:, r : r + 1] - decays[pl.ds(r, 1), :], 0.0)
        return jnp.where(lower, jnp.exp(steps), 0.0)

    state_w = jnp.zeros((128, 128), F32)
    state_n = jnp.zeros((128, 128), F32)
    gone = [jnp.zeros((1, 1), F32)] * 3
    for b in range(blocks):
        cut = pl.ds(b * BLOCK, BLOCK)
        r = 3 * b
        now = [columns[:, r + h : r + h + 1] for h in range(3)]
        last = [columns[BLOCK - 1 : BLOCK, r + h : r + h + 1] for h in range(3)]
        cos, sin = turn(base[0][0][b : b + 1], base[0][1][b : b + 1], tt[0], tt[1])
        sin = sin * sign_w
        q = qw[cut, :].astype(F32)
        k = kw[cut, :].astype(F32)
        v = vw[cut, :]
        q = q * cos + pltpu.roll(q, HDW // 2, 1) * sin
        k = (k * cos + pltpu.roll(k, HDW // 2, 1) * sin) * HDW**-0.5
        scores = dot_t(q.astype(BF16), k.astype(BF16)) * spread(r)
        out_b = dot(scores.astype(BF16), v)
        if b:
            out_b += dot((q * jnp.exp(now[0])).astype(BF16), state_w.astype(BF16))
        o_w[cut, :] = out_b
        qe_w[cut, :] = (q * jnp.exp(now[0] + gone[0])).astype(BF16)
        tail = k * jnp.exp(last[0] - now[0])
        state_w = jnp.exp(last[0]) * state_w + tdot(tail.astype(BF16), v)
        cos, sin = turn(base[1][0][b : b + 1], base[1][1][b : b + 1], tt[2], tt[3])
        sin = sin * sign_n
        q = qn[cut, :].astype(F32)
        k = kn[cut, :].astype(F32)
        v = vn[cut, :]

        def other(a):
            return jnp.where(front_n, pltpu.roll(a, 128 - HDN // 2, 1), pltpu.roll(a, HDN // 2, 1))

        q = q * cos + other(q) * sin
        k = (k * cos + other(k) * sin) * HDN**-0.5
        kb = k.astype(BF16)
        probs = []
        for h, mask in enumerate((low, jnp.logical_not(low))):
            qh = jnp.where(mask, q, 0.0).astype(BF16)
            probs.append((dot_t(qh, kb) * spread(r + 1 + h)).astype(BF16))
        v_f = v.astype(F32)
        v2 = jnp.concatenate(
            [jnp.where(low, v_f, 0.0).astype(BF16), jnp.where(low, 0.0, v_f).astype(BF16)], axis=0
        )
        out_b = dot(jnp.concatenate(probs, axis=1), v2)
        if b:
            seen = jnp.where(low, jnp.exp(now[1]), jnp.exp(now[2]))
            out_b += dot((q * seen).astype(BF16), state_n.astype(BF16))
        o_n[cut, :] = out_b
        seen = jnp.where(low, jnp.exp(now[1] + gone[1]), jnp.exp(now[2] + gone[2]))
        qe_n[cut, :] = (q * seen).astype(BF16)
        tail = k * jnp.where(low, jnp.exp(last[1] - now[1]), jnp.exp(last[2] - now[2]))
        keep = jnp.where(low, jnp.exp(last[1]), jnp.exp(last[2]))
        state_n = keep * state_n + jnp.where(same_head, tdot(tail.astype(BF16), v), 0.0)
        gone = [g + t for g, t in zip(gone, last)]

    total_w = jnp.exp(gone[0]) + jnp.zeros((1, 128), F32)
    total_n = jnp.where(low, jnp.exp(gone[1]), jnp.exp(gone[2]))
    packed_n = jnp.where(low, state_n[:HDN], state_n[HDN:])
    sw, sn = 128 // plane, HDN // plane
    part_of = lax.broadcasted_iota(jnp.int32, (8, 128), 0)

    def message(state, rate_w, rate_n):
        parts = jnp.zeros((8, 128), F32)
        for r, rate in ((0, rate_w), (2, rate_n)):
            high = rate.astype(BF16).astype(F32)
            parts = jnp.where(part_of == r, high, jnp.where(part_of == r + 1, rate - high, parts))
        return jnp.concatenate([state, parts], axis=0).astype(BF16)

    for j in range(plane):
        state = [state_w[sw * j : sw * (j + 1)], packed_n[sn * j : sn * (j + 1)]]
        msg[j] = message(jnp.concatenate(state, axis=0), total_w, total_n)
    ns = sw + sn

    def stage1(d):
        to = lax.rem(me + d, plane)
        return remote(msg.at[to], in1.at[me], s1_s.at[d], s1_r.at[d], at_plane(to))

    pl.semaphore_wait(barrier, len(peers))
    for d in range(1, plane):
        stage1(d).start()
    for load in loads[6:10]:
        load.wait()
    for side in (0, 1):
        go(uz(1, side))
        go(wx(0, side))
    d_own()
    for side in (0, 1):
        go(wx(1, side))
    d_send(0)
    in1[pl.ds(me, 1)] = msg[pl.ds(me, 1)]

    for d in range(1, plane):
        stage1(d).wait_recv()
    wide_row = lax.broadcasted_iota(jnp.int32, (ns, 128), 0) < sw

    def factor(pair):
        return jnp.where(wide_row, pair[0], pair[1])

    def opened(ref, j):
        whole = ref[j].astype(F32)
        return whole[0:ns], (whole[ns : ns + 1] + whole[ns + 1 : ns + 2], whole[ns + 2 : ns + 3] + whole[ns + 3 : ns + 4])

    before = []
    held = jnp.zeros((ns, 128), F32)
    rate = (jnp.ones((1, 128), F32), jnp.ones((1, 128), F32))
    for j in range(plane):
        before.append((held, rate))
        state, mine = opened(in1, j)
        held = held * factor(mine) + state
        rate = (rate[0] * mine[0], rate[1] * mine[1])
    tot2[...] = message(held, *rate)

    def stage2(d):
        return remote(tot2, in2.at[z], s2_s.at[d], s2_r.at[d], {"z": lax.rem(z + d, nz)})

    for d in range(1, nz):
        stage2(d).start()
    for side in (0, 1):
        go(uy(0, side))
    u_step(1)
    d_turn()
    d_send(1)
    w_turn()
    in2[pl.ds(z, 1)] = tot2[...][None]
    for d in range(1, nz):
        stage2(d).wait_recv()
    held = jnp.zeros((ns, 128), F32)
    for k in range(nz):
        state, mine = opened(in2, k)
        later = held * factor(mine) + state
        held = jnp.where(k < z, later, held)
    for j in range(plane):
        state, rate = before[j]
        state = held * factor(rate) + state
        msg3[j] = jnp.concatenate([state, jnp.zeros((8, 128), F32)], axis=0).astype(BF16)

    def stage3(d):
        to = lax.rem(me + d, plane)
        return remote(msg3.at[to], in3.at[me], s3_s.at[d], s3_r.at[d], at_plane(to))

    for d in range(1, plane):
        stage3(d).start()
    in3[pl.ds(me, 1)] = msg3[pl.ds(me, 1)]
    u_turn(1)
    d_column()
    u_step(2)
    d_send(2)
    for load in loads[10:]:
        load.wait()
    for d in range(1, plane):
        stage3(d).wait_recv()
    arrived = in3[...].astype(F32)
    enter_w = arrived[:, 0:sw, :].reshape(128, 128).astype(BF16)
    enter_p = arrived[:, sw:ns, :].reshape(HDN, 128)
    enter_n = jnp.concatenate(
        [jnp.where(low, enter_p, 0.0), jnp.where(low, 0.0, enter_p)], axis=0
    ).astype(BF16)

    def mixed_to(d):
        to = lax.rem(x + d, nx)
        return remote(mixed.at[to], mix_in.at[x], mx_s.at[d], mx_r.at[d], {"x": to})

    def gated(o, gate):
        return (o * jax.nn.silu(gate.astype(F32))).astype(BF16)

    for i in range(nx):
        cut = pl.ds(i * rows, rows)
        o = o_w[cut, :] + dot(qe_w[cut, :], enter_w)
        o = o - jnp.mean(o, axis=-1, keepdims=True)
        o = o * lax.rsqrt(jnp.mean(o * o, axis=-1, keepdims=True) + head_eps)
        mixed[i, :, 0:128] = gated(o, gw[cut, :])
        o = o_n[cut, :] + dot(qe_n[cut, :], enter_n)

        def by_head(a):
            first = jnp.sum(jnp.where(low, a, 0.0), axis=-1, keepdims=True)
            second = jnp.sum(jnp.where(low, 0.0, a), axis=-1, keepdims=True)
            return jnp.where(low, first, second) * (1.0 / HDN)

        o = o - by_head(o)
        o = o * lax.rsqrt(by_head(o * o) + head_eps)
        mixed[i, :, 128:256] = gated(o, gn[cut, :])

    for d in (2, 1, 3):
        go(mixed_to(d))
    mix_in[pl.ds(x, 1)] = mixed[pl.ds(x, 1)]

    u_turn(2)
    u_relay((0, 0))
    w_near()
    u_step(3)
    u_turn(3)
    d_send(3)
    d_step(1, 0, 1)
    w_last()
    w_done()
    u_relay((1, 0), (1, 1))
    for d in (1, 3, 2):
        mixed_to(d).wait_recv()

    tile = 512
    tiles = width // tile

    def project(n, squares):
        at = pl.ds(pl.multiple_of(n * tile, tile), tile)
        total = stream[:, at].astype(F32)
        for j in range(nx):
            total += dot(mix_in[j], wo[j, :, :, at].reshape(2 * deep, tile))
        total = total.astype(BF16)
        middle[:, at] = total
        total = total.astype(F32)
        return squares + jnp.sum(total * total, axis=-1, keepdims=True)

    squares = lax.fori_loop(0, tiles, project, jnp.zeros((rows, 1), F32))
    scale = lax.rsqrt(squares * (1.0 / width) + norm_eps)
    normed[pl.ds(x, 1)] = (middle[...].astype(F32) * scale * gain[...].astype(F32).reshape(1, width)).astype(BF16)[None]

    def nx_rows(piece, side):
        start = side * half_rows if piece in (0, 3) else (1 - side) * half_rows + (piece - 1) * part_rows
        return pl.ds(start, half_rows if piece in (0, 3) else part_rows)

    def nm(piece, side):
        ref = normed.at[at_x(-fwd[side] if piece == 3 else 0), nx_rows(piece, side)]
        return same(ref, st_s.at[side, piece], st_r.at[side, piece], x_to[side])

    def nm_in(piece, side):
        ref = normed.at[at_x(-fwd[side] * (2 if piece == 3 else 1)), nx_rows(piece, side)]
        return same(ref, st_s.at[side, piece], st_r.at[side, piece], x_to[side])

    for piece in (0, 1):
        for side in (0, 1):
            go(nm(piece, side))

    d_step(1, 2)
    u_step(4)
    u_turn(4)
    u_relay((2, 1), (2, 0))
    d_step(1, 3)
    d_cores(1)
    d_step(2, 0, 1)
    u_relay((3, 1))
    d_step(2, 2)
    for side in (0, 1):
        nm_in(0, side).wait_recv()
        go(nm(3, side))
        go(nm(2, side))
    u_relay((3, 0), (0, 1))
    d_step(2, 3)
    d_cores(2)
    u_rest()
    d_step(3, 0, 1)
    u_last()
    d_step(3, 2)
    u_done()
    d_step(3, 3)
    d_cores(3)

    def rise(i):
        def one(n, _):
            at = pl.ds(pl.multiple_of(n * tile, tile), tile)
            h = jnp.maximum(dot(normed[i], up[:, :, :, :, at].reshape(width, tile)), 0.0)
            hidden[i, :, at] = (h * h).astype(BF16)
            return 0

        lax.fori_loop(0, tiles, one, 0)

    for side in (0, 1):
        nm_in(3, side).wait_recv()
    rise(xo)

    side_tiles = tiles // 2
    by_distance = (0, 1, -1, 2, -2, 3, -3, 4)
    span = width // nz

    def fall(i, side, into):
        for n in range(nz // 2):
            of_z = at_z(by_distance[side * (nz // 2) + n])
            piece = dot_t(hidden[i], down[of_z].reshape(span, width))
            into[side, :, n * span : (n + 1) * span] = piece.astype(into.dtype)

    far = [
        remote(send2.at[0], relay_l, rs_s.at[0], rs_r.at[0], right),
        remote(send2.at[1], relay_r, rs_s.at[1], rs_r.at[1], left),
    ]
    near_r = [remote(send1.at[s], got_l.at[s], rs_s.at[2 + s], rs_r.at[2 + s], right) for s in (0, 1)]
    near_l = [remote(sendm.at[s], got_r.at[s], rs_s.at[4 + s], rs_r.at[4 + s], left) for s in (0, 1)]
    for k in (0, 1, -1, 2):
        d_core_in(k).wait_recv()
    fall(xo, 0, send2)
    far[0].start()
    d_step(4, 0, 1, 2, 3)
    d_cores(4)
    for k in (-2, 3, -3, 4):
        d_core_in(k).wait_recv()
    fall(xo, 1, send2)
    far[1].start()
    for side in (0, 1):
        for piece in (1, 2):
            nm_in(piece, side).wait_recv()
    rise(xr)
    fall(xr, 1, send1)
    near_r[1].start()
    rise(xl)
    fall(xl, 0, sendm)
    near_l[0].start()
    fall(xr, 0, own)
    fall(xl, 1, own)
    far[0].wait_recv()
    send1[0] = (own[0] + relay_l[...].astype(F32)).astype(BF16)
    near_r[0].start()
    far[1].wait_recv()
    sendm[1] = (own[1] + relay_r[...].astype(F32)).astype(BF16)
    near_l[1].start()
    rise(x)
    fall(x, 0, own)
    fall(x, 1, own)
    for s, first, second in ((1, near_r, near_l), (0, near_l, near_r)):
        first[s].wait_recv()
        second[s].wait_recv()
        total = own[s] + got_l[s].astype(F32) + got_r[s].astype(F32)
        for n in range(nz // 2):
            at = pl.ds(pl.multiple_of(at_z(by_distance[s * (nz // 2) + n]) * span, span), span)
            out[:, at] = (middle[:, at].astype(F32) + total[:, n * span : (n + 1) * span]).astype(BF16)

    for copy in sent:
        copy.wait_send()
    for copy in (*far, *near_r, *near_l):
        copy.wait_send()
    for d in range(1, plane):
        stage1(d).wait_send()
        stage3(d).wait_send()
    for d in range(1, nz):
        stage2(d).wait_send()


def on_device(
    sizes,
    stream_in, query_wide, key_wide, value_wide, gate_wide, decay_wide,
    query_narrow, key_narrow, value_narrow, gate_narrow, decay_narrow,
    output_wide, output_narrow, norm_gain, up_weight, down_weight,
):
    nz, ny, nc, nx = sizes
    tok = query_wide.shape[0]
    rows, width = stream_in.shape
    plane = ny * nc
    part, hid = up_weight.shape
    ns = (128 + HDN) // plane
    dma = pltpu.SemaphoreType.DMA
    vm = pltpu.VMEM
    scratch = [
        *[vm((tok, 128), BF16)] * 8, vm((rows, width), BF16),
        vm((nz, ny, nc, part, hid), BF16), vm((nz, ny, nc, part, hid), BF16), vm((nx, 2, *output_wide.shape), BF16),
        vm((tok, 128), BF16), vm((tok, 128), BF16), vm((tok, 128), F32), vm((tok, 128), F32),
        vm((128, 128), F32),
        vm((plane, ns + 8, 128), BF16), vm((plane, ns + 8, 128), BF16),
        vm((ns + 8, 128), BF16), vm((nz, ns + 8, 128), BF16),
        vm((plane, ns + 8, 128), BF16), vm((plane, ns + 8, 128), BF16),
        vm((nx, rows, 256), BF16), vm((nx, rows, 256), BF16),
        vm((rows, width), BF16), vm((nx, rows, width), BF16), vm((nx, rows, hid), BF16),
        vm((2, rows, width // 2), BF16), vm((2, rows, width // 2), BF16), vm((2, rows, width // 2), BF16),
        vm((2, rows, width // 2), F32),
        vm((rows, width // 2), BF16), vm((rows, width // 2), BF16),
        vm((2, rows, width // 2), BF16), vm((2, rows, width // 2), BF16),
        dma((2, 4)), dma((2, 4)),
        dma((plane,)), dma((plane,)), dma((nz,)), dma((nz,)), dma((plane,)), dma((plane,)),
        dma((nx,)), dma((nx,)), dma((6,)), dma((6,)),
        dma((13,)), dma((2, 3)), dma((2, 3)), dma((2, 4)), dma((2, 4)), dma((2, nz)), dma((2, nz)),
        dma((2, 4)), dma((2, 4)), dma((2, 2)), dma((2, 2)), dma((2, 4, 4)), dma((2, 4, 4)), dma((15,)), dma((15,)),
    ]
    vmem = pl.BlockSpec(memory_space=pltpu.VMEM)
    hbm = pl.BlockSpec(memory_space=pl.ANY)
    return pl.pallas_call(
        functools.partial(kernel, sizes),
        out_shape=jax.ShapeDtypeStruct((rows, width), BF16),
        in_specs=[vmem] * 6 + [hbm] * 13,
        out_specs=vmem,
        scratch_shapes=scratch,
        compiler_params=pltpu.CompilerParams(
            collective_id=0, has_side_effects=True, vmem_limit_bytes=60 * 1024 * 1024
        ),
    )(
        decay_wide, decay_narrow, norm_gain, jnp.asarray(rope_tables(BLOCK, 1)),
        jnp.asarray(rope_tables(8, BLOCK)), jnp.asarray(rope_tables(nz * plane, tok)),
        query_wide, key_wide, value_wide, query_narrow, key_narrow, value_narrow, gate_wide, gate_narrow, stream_in,
        output_wide, output_narrow, up_weight, down_weight.T,
    )


def solution(mesh):
    sizes = (8, 4, 2, mesh.shape["tp"])
    split = Mesh(mesh.devices.reshape(sizes), ("z", "y", "c", "x"))
    sp = ("z", "y", "c")
    rows, heads = P(sp, "x"), P("x", sp)
    in_specs = (
        P((*sp, "x"), None), rows, rows, rows, rows, heads, rows, rows, rows, rows, heads,
        P("x", None), P("x", None), P(), rows, heads,
    )
    return jax.shard_map(
        functools.partial(on_device, sizes), mesh=split, in_specs=in_specs,
        out_specs=P((*sp, "x"), None), check_vma=False,
    )
```

```python
import functools

import jax
import jax.numpy as jnp
import numpy as np
from jax import lax
from jax.experimental import pallas as pl
from jax.experimental.pallas import tpu as pltpu
from jax.sharding import Mesh
from jax.sharding import PartitionSpec as P

HDW = 128
HDN = 64
BLOCK = 128
head_eps = 1e-05
norm_eps = 1e-06
rope_base = 10000.0
MESH = pl.DeviceIdType.MESH
F32 = jnp.float32
BF16 = jnp.bfloat16


def rope_tables(steps, stride):
    tables = []
    for width in (HDW, HDN):
        half = width // 2
        inverse = rope_base ** (-np.arange(half, dtype=np.float64) / half)
        lanes = np.tile(inverse, 128 // half)
        angles = (stride * np.arange(steps, dtype=np.float64))[:, None] * lanes[None, :]
        tables += [np.cos(angles), np.sin(angles)]
    return np.stack(tables).astype(np.float32)


def remote(src, dst, send_sem, recv_sem, device):
    return pltpu.make_async_remote_copy(
        src_ref=src, dst_ref=dst, send_sem=send_sem, recv_sem=recv_sem, device_id=device, device_id_type=MESH
    )


def turn(cos_a, sin_a, cos_b, sin_b):
    return cos_a * cos_b - sin_a * sin_b, sin_a * cos_b + cos_a * sin_b


def dot(a, b):
    return jnp.dot(a, b, preferred_element_type=F32)


def dot_t(a, b):
    return lax.dot_general(a, b, (((1,), (1,)), ((), ())), preferred_element_type=F32)


def tdot(a, b):
    return lax.dot_general(a, b, (((0,), (0,)), ((), ())), preferred_element_type=F32)


def kernel(
    sizes,
    dw, dn, gain, tt, tb, ts,
    qw_in, kw_in, vw_in, qn_in, kn_in, vn_in, gw_in, gn_in, stream_in, ow, on, up_own, down_own,
    out,
    qw, kw, vw, qn, kn, vn, gw, gn, stream,
    up, down, wo,
    qe_w, qe_n, o_w, o_n, decays, st_w, st_n, k_w, k_n, msg, in1, tot2, in2, msg3, in3,
    mixed, mix_in, middle, normed, hidden, send2, send1, sendm, own, hold, result, relay_l, relay_r, got_both,
    left_s, in_s, out_s, st_r, s1_r, s2_r, s3_r, mx_r, rs_r, wo_r, uz_r, uy_r, ur_r, dy_r, dz_r, core_r,
):
    nz, ny, nc, nx = sizes
    z, y, c, x = (lax.axis_index(a) for a in ("z", "y", "c", "x"))
    xr, xl, xo = lax.rem(x + 1, nx), lax.rem(x + nx - 1, nx), lax.rem(x + 2, nx)
    plane = ny * nc
    me = y * nc + c
    sp = z * plane + me
    tok = qw.shape[0]
    blocks = tok // BLOCK
    rows = stream.shape[0]
    width = stream.shape[1]
    half_rows, few = rows // 2, rows // 6
    right, left = {"x": xr}, {"x": xl}

    def at_plane(j):
        return {"y": j // nc, "c": lax.rem(j, nc)}

    barrier = pltpu.get_barrier_semaphore()
    peers = [right, left, {"x": xo}]
    peers += [at_plane(lax.rem(me + d, plane)) for d in range(1, plane)]
    peers += [{"z": lax.rem(z + d, nz)} for d in range(1, nz)]
    for peer in peers:
        pl.semaphore_signal(barrier, inc=1, device_id=peer, device_id_type=MESH)

    pairs = [
        (kw_in, kw), (vw_in, vw), (kn_in, kn), (vn_in, vn),
        (up_own, up.at[z, y, c]), (ow, wo.at[x, 0]), (on, wo.at[x, 1]), (down_own, down.at[z, y, c]),
        (qw_in, qw), (qn_in, qn), (gw_in, gw), (gn_in, gn), (stream_in, stream),
    ]
    loads = [pltpu.make_async_copy(a, b, in_s.at[i]) for i, (a, b) in enumerate(pairs)]
    for load in loads:
        load.start()

    lane = lax.broadcasted_iota(jnp.int32, (1, 128), 1)
    low = lane < HDN
    base = []
    for g in (0, 2):
        row = [ts[g + i, pl.ds(sp, 1), :] for i in (0, 1)]
        base.append(turn(row[0], row[1], tb[g], tb[g + 1]))
    sign_w = jnp.where(lane < HDW // 2, -1.0, 1.0)
    front_n = lax.rem(lane, HDN) < HDN // 2
    sign_n = jnp.where(front_n, -1.0, 1.0)

    def go(copy):
        copy.start()

    def wait_all(ref, sem):
        pltpu.make_async_copy(ref, ref, sem).wait()

    def same(ref, send_sem, recv_sem, device):
        return remote(ref, ref, send_sem, recv_sem, device)

    z_to = ({"z": lax.rem(z + 1, nz)}, {"z": lax.rem(z + nz - 1, nz)})
    y_to = ({"y": lax.rem(y + 1, ny)}, {"y": lax.rem(y + ny - 1, ny)})
    x_to = (right, left)
    partner = {"c": 1 - c}
    fwd = (1, -1)

    def at_z(k):
        return lax.rem(z + nz + k, nz)

    def at_y(k):
        return lax.rem(y + ny + k, ny)

    def at_x(k):
        return lax.rem(x + nx + k, nx)

    part = up.shape[3]
    halves = (pl.ds(0, part // 2), pl.ds(part // 2, part // 2))

    relayed = ((0, 1, 2, 3), (4, -1, -2, -3))

    def uz(step, side):
        ref = up.at[at_z(-fwd[side] * (step - 1)), y, c]
        if step == nz // 2:
            ref = ref.at[halves[side]]
        return same(ref, left_s.at[0], uz_r.at[side, step - 1], z_to[side])

    def uz_in(step, side):
        ref = up.at[at_z(-fwd[side] * step), y, c]
        if step == nz // 2:
            ref = ref.at[halves[side]]
        return same(ref, left_s.at[0], uz_r.at[side, step - 1], z_to[side])

    def uy(off, side):
        return same(up.at[at_z(off), y, c], left_s.at[1], uy_r.at[side, relayed[side].index(off) if off in relayed[side] else 4], y_to[side])

    def uy_in(off, side):
        ref = up.at[at_z(off), at_y(-fwd[side]), c]
        return same(ref, left_s.at[1], uy_r.at[side, relayed[side].index(off) if off in relayed[side] else 4], y_to[side])


    def ur(i, side):
        ref = up.at[at_z(relayed[side][i]), at_y(-fwd[side]), c]
        return same(ref, left_s.at[2], ur_r, y_to[side])

    def u_core(i):
        ref = up.at[:, at_y((0, 1, -1, 2)[i]), c]
        return same(ref, left_s.at[6], core_r.at[0], partner)

    def u_step(step):
        for side in (0, 1):
            uz_in(step, side).wait_recv()
            if step < nz // 2:
                go(uz(step + 1, side))

    def u_turn(step):
        offs = (-step, step) if step < nz // 2 else (step,)
        for off in offs:
            for side in (0, 1):
                go(uy(off, side))
        if step == nz // 2:
            go(u_core(0))

    def u_relay(*which):
        for i, side in which:
            uy_in(relayed[side][i], side).wait_recv()
            go(ur(i, side))

    def u_rest():
        for side in (0, 1):
            wait_all(up.at[pl.ds(0, 4), 0, 0], uy_r.at[side, 4])
        go(u_core(1))
        go(u_core(2))

    def u_last():
        wait_all(up.at[:, 0, 0], ur_r)
        go(u_core(3))

    def u_done():
        wait_all(up.at[:, :, 0], core_r.at[0])

    by_distance = (0, 1, -1, 2, -2, 3, -3, 4)
    early = 5

    def dy(step, side):
        ref = down.at[z, at_y(-fwd[side] * (step - 1)), c]
        if step == 2:
            ref = ref.at[halves[side]]
        return same(ref, left_s.at[3], dy_r.at[side, step - 1], y_to[side])

    def dy_in(step, side):
        ref = down.at[z, at_y(-fwd[side] * step), c]
        if step == 2:
            ref = ref.at[halves[side]]
        return same(ref, left_s.at[3], dy_r.at[side, step - 1], y_to[side])

    columns_y = (0, 1, -1, 2)
    last_by = ((0, 3), (2, 1))

    def dz(step, side, g):
        ref = down.at[at_z(-fwd[side] * (step - 1)), at_y(columns_y[g]), c]
        return same(ref, left_s.at[4], dz_r.at[side, step - 1, g], z_to[side])

    def dz_in(step, side, g):
        ref = down.at[at_z(-fwd[side] * step), at_y(columns_y[g]), c]
        return same(ref, left_s.at[4], dz_r.at[side, step - 1, g], z_to[side])

    def d_core(k):
        return same(down.at[at_z(k), :, c], left_s.at[6], core_r.at[2 if k in by_distance[:early] else 3], partner)

    def d_own():
        for side in (0, 1):
            go(dy(1, side))

    def d_turn():
        for side in (0, 1):
            dy_in(1, side).wait_recv()
            go(dy(2, side))

    def d_column():
        for side in (0, 1):
            dy_in(2, side).wait_recv()
        go(d_core(0))

    def d_send(*gs):
        for side in (0, 1):
            for g in gs:
                go(dz(1, side, g))

    def d_step(step, *gs):
        for g in gs:
            for side in (0, 1):
                if step < nz // 2:
                    dz_in(step, side, g).wait_recv()
                    if step + 1 < nz // 2 or g in last_by[side]:
                        go(dz(step + 1, side, g))
                elif g in last_by[side]:
                    dz_in(step, side, g).wait_recv()

    def d_cores(step):
        go(d_core(step))
        if step < nz // 2:
            go(d_core(-step))

    deep = wo.shape[2]
    wo_halves = (pl.ds(0, deep // 2), pl.ds(deep // 2, deep // 2))

    def wx(step, side):
        ref = wo.at[at_x(-fwd[side] if step == 2 else 0), c].at[wo_halves[1 - side if step == 1 else side]]
        return same(ref, left_s.at[5], wo_r.at[side, step], x_to[side])

    def wx_in(step, side):
        ref = wo.at[at_x(-fwd[side] * (2 if step == 2 else 1)), c].at[wo_halves[1 - side if step == 1 else side]]
        return same(ref, left_s.at[5], wo_r.at[side, step], x_to[side])

    def w_core(i):
        return same(wo.at[at_x(i + 1), c], left_s.at[5], core_r.at[1], partner)

    def w_turn():
        for side in (0, 1):
            wx_in(0, side).wait_recv()
            go(wx(2, side))

    def w_near():
        for side in (0, 1):
            wx_in(1, side).wait_recv()
        go(w_core(0))
        go(w_core(2))

    def w_last():
        for side in (0, 1):
            wx_in(2, side).wait_recv()
        go(w_core(1))

    def w_done():
        wait_all(wo.at[pl.ds(0, nx - 1), 0], core_r.at[1])

    for load in loads[:4]:
        load.wait()

    decays[...] = jnp.zeros_like(decays)
    for b in range(blocks):
        cut = pl.ds(b * BLOCK, BLOCK)
        decays[pl.ds(3 * b, 1), :] = dw[:, cut]
        decays[pl.ds(3 * b + 1, 2), :] = dn[:, cut]
    running = decays[0:32, :]
    shift = 1
    while shift < BLOCK:
        running = running + jnp.where(lane >= shift, pltpu.roll(running, shift, 1), 0.0)
        shift *= 2
    decays[0:32, :] = running
    columns = jnp.transpose(decays[...])

    at_t = lax.broadcasted_iota(jnp.int32, (BLOCK, BLOCK), 0)
    at_s = lax.broadcasted_iota(jnp.int32, (BLOCK, BLOCK), 1)
    lower = at_t >= at_s
    same_head = (at_t < HDN) == (at_s < HDN)

    def spread(r):
        steps = jnp.minimum(columns[:, r : r + 1] - decays[pl.ds(r, 1), :], 0.0)
        return jnp.where(lower, jnp.exp(steps), 0.0)

    def angles(b):
        cos_w, sin_w = turn(base[0][0][b : b + 1], base[0][1][b : b + 1], tt[0], tt[1])
        cos_n, sin_n = turn(base[1][0][b : b + 1], base[1][1][b : b + 1], tt[2], tt[3])
        return cos_w, sin_w * sign_w, cos_n, sin_n * sign_n

    def rotate_w(a, cos, sin):
        return a * cos + pltpu.roll(a, HDW // 2, 1) * sin

    def rotate_n(a, cos, sin):
        other = jnp.where(front_n, pltpu.roll(a, 128 - HDN // 2, 1), pltpu.roll(a, HDN // 2, 1))
        return a * cos + other * sin

    def ends(b):
        r = 3 * b
        now = [columns[:, r + h : r + h + 1] for h in range(3)]
        return now, [columns[BLOCK - 1 : BLOCK, r + h : r + h + 1] for h in range(3)]

    state_w = jnp.zeros((128, 128), F32)
    state_n = jnp.zeros((128, 128), F32)
    gone = [jnp.zeros((1, 1), F32)] * 3
    before_block = []
    for b in range(blocks):
        cut = pl.ds(b * BLOCK, BLOCK)
        now, last = ends(b)
        cos_w, sin_w, cos_n, sin_n = angles(b)
        st_w[b] = state_w.astype(BF16)
        st_n[b] = state_n.astype(BF16)
        before_block.append(gone)
        k = rotate_w(kw[cut, :].astype(F32), cos_w, sin_w) * HDW**-0.5
        k_w[cut, :] = k.astype(BF16)
        tail = k * jnp.exp(last[0] - now[0])
        state_w = jnp.exp(last[0]) * state_w + tdot(tail.astype(BF16), vw[cut, :])
        k = rotate_n(kn[cut, :].astype(F32), cos_n, sin_n) * HDN**-0.5
        k_n[cut, :] = k.astype(BF16)
        tail = k * jnp.where(low, jnp.exp(last[1] - now[1]), jnp.exp(last[2] - now[2]))
        keep = jnp.where(low, jnp.exp(last[1]), jnp.exp(last[2]))
        state_n = keep * state_n + jnp.where(same_head, tdot(tail.astype(BF16), vn[cut, :]), 0.0)
        gone = [g + t for g, t in zip(gone, last)]

    def outputs(b):
        cut = pl.ds(b * BLOCK, BLOCK)
        r = 3 * b
        now, last = ends(b)
        cos_w, sin_w, cos_n, sin_n = angles(b)
        gone = before_block[b]
        q = rotate_w(qw[cut, :].astype(F32), cos_w, sin_w)
        scores = dot_t(q.astype(BF16), k_w[cut, :]) * spread(r)
        out_b = dot(scores.astype(BF16), vw[cut, :])
        if b:
            out_b += dot((q * jnp.exp(now[0])).astype(BF16), st_w[b])
        o_w[cut, :] = out_b
        qe_w[cut, :] = (q * jnp.exp(now[0] + gone[0])).astype(BF16)
        q = rotate_n(qn[cut, :].astype(F32), cos_n, sin_n)
        probs = []
        for h, mask in enumerate((low, jnp.logical_not(low))):
            qh = jnp.where(mask, q, 0.0).astype(BF16)
            probs.append((dot_t(qh, k_n[cut, :]) * spread(r + 1 + h)).astype(BF16))
        v_f = vn[cut, :].astype(F32)
        v2 = jnp.concatenate(
            [jnp.where(low, v_f, 0.0).astype(BF16), jnp.where(low, 0.0, v_f).astype(BF16)], axis=0
        )
        out_b = dot(jnp.concatenate(probs, axis=1), v2)
        if b:
            seen = jnp.where(low, jnp.exp(now[1]), jnp.exp(now[2]))
            out_b += dot((q * seen).astype(BF16), st_n[b])
        o_n[cut, :] = out_b
        seen = jnp.where(low, jnp.exp(now[1] + gone[1]), jnp.exp(now[2] + gone[2]))
        qe_n[cut, :] = (q * seen).astype(BF16)

    total_w = jnp.exp(gone[0]) + jnp.zeros((1, 128), F32)
    total_n = jnp.where(low, jnp.exp(gone[1]), jnp.exp(gone[2]))
    packed_n = jnp.where(low, state_n[:HDN], state_n[HDN:])
    sw, sn = 128 // plane, HDN // plane
    part_of = lax.broadcasted_iota(jnp.int32, (8, 128), 0)

    def message(state, rate_w, rate_n):
        parts = jnp.zeros((8, 128), F32)
        for r, rate in ((0, rate_w), (2, rate_n)):
            high = rate.astype(BF16).astype(F32)
            parts = jnp.where(part_of == r, high, jnp.where(part_of == r + 1, rate - high, parts))
        return jnp.concatenate([state, parts], axis=0).astype(BF16)

    for j in range(plane):
        state = [state_w[sw * j : sw * (j + 1)], packed_n[sn * j : sn * (j + 1)]]
        msg[j] = message(jnp.concatenate(state, axis=0), total_w, total_n)
    ns = sw + sn

    def stage1(d):
        to = lax.rem(me + d, plane)
        return remote(msg.at[to], in1.at[me], left_s.at[10], s1_r, at_plane(to))

    pl.semaphore_wait(barrier, len(peers))
    for d in range(1, plane):
        stage1(d).start()
    for load in loads[4:10]:
        load.wait()
    for side in (0, 1):
        go(uz(1, side))
        go(wx(0, side))
    d_own()
    for side in (0, 1):
        go(wx(1, side))
    in1[pl.ds(me, 1)] = msg[pl.ds(me, 1)]
    for b in range(blocks // 2):
        outputs(b)

    wait_all(msg.at[pl.ds(0, plane - 1)], s1_r)
    wide_row = lax.broadcasted_iota(jnp.int32, (ns, 128), 0) < sw

    def factor(pair):
        return jnp.where(wide_row, pair[0], pair[1])

    def opened(ref, j):
        whole = ref[j].astype(F32)
        return whole[0:ns], (whole[ns : ns + 1] + whole[ns + 1 : ns + 2], whole[ns + 2 : ns + 3] + whole[ns + 3 : ns + 4])

    before = []
    held = jnp.zeros((ns, 128), F32)
    rate = (jnp.ones((1, 128), F32), jnp.ones((1, 128), F32))
    for j in range(plane):
        before.append((held, rate))
        state, mine = opened(in1, j)
        held = held * factor(mine) + state
        rate = (rate[0] * mine[0], rate[1] * mine[1])
    tot2[...] = message(held, *rate)

    def stage2(d):
        return remote(tot2, in2.at[z], left_s.at[11], s2_r, {"z": lax.rem(z + d, nz)})

    for d in range(1, nz):
        stage2(d).start()
    for side in (0, 1):
        go(uy(0, side))
    d_send(0)
    for b in range(blocks // 2, blocks):
        outputs(b)
    u_step(1)
    d_turn()
    d_send(1)
    w_turn()
    in2[pl.ds(z, 1)] = tot2[...][None]
    wait_all(in2.at[pl.ds(0, nz - 1)], s2_r)
    held = jnp.zeros((ns, 128), F32)
    for k in range(nz):
        state, mine = opened(in2, k)
        later = held * factor(mine) + state
        held = jnp.where(k < z, later, held)
    for j in range(plane):
        state, rate = before[j]
        state = held * factor(rate) + state
        msg3[j] = jnp.concatenate([state, jnp.zeros((8, 128), F32)], axis=0).astype(BF16)

    def stage3(d):
        to = lax.rem(me + d, plane)
        return remote(msg3.at[to], in3.at[me], left_s.at[12], s3_r, at_plane(to))

    for d in range(1, plane):
        stage3(d).start()
    in3[pl.ds(me, 1)] = msg3[pl.ds(me, 1)]
    u_turn(1)
    u_relay((0, 0))
    d_column()
    w_near()
    u_step(2)
    u_turn(2)
    d_send(2)
    for load in loads[10:]:
        load.wait()
    wait_all(msg.at[pl.ds(0, plane - 1)], s3_r)
    arrived = in3[...].astype(F32)
    enter_w = arrived[:, 0:sw, :].reshape(128, 128).astype(BF16)
    enter_p = arrived[:, sw:ns, :].reshape(HDN, 128)
    enter_n = jnp.concatenate(
        [jnp.where(low, enter_p, 0.0), jnp.where(low, 0.0, enter_p)], axis=0
    ).astype(BF16)

    def mixed_to(d):
        to = lax.rem(x + d, nx)
        return remote(mixed.at[to], mix_in.at[x], left_s.at[7], mx_r, {"x": to})

    def gated(o, gate):
        return (o * jax.nn.silu(gate.astype(F32))).astype(BF16)

    for d in (2, 1, 3, 0):
        i = lax.rem(x + d, nx)
        cut = pl.ds(pl.multiple_of(i * rows, rows), rows)
        o = o_w[cut, :] + dot(qe_w[cut, :], enter_w)
        o = o - jnp.mean(o, axis=-1, keepdims=True)
        o = o * lax.rsqrt(jnp.mean(o * o, axis=-1, keepdims=True) + head_eps)
        mixed[i, :, 0:128] = gated(o, gw[cut, :])
        o = o_n[cut, :] + dot(qe_n[cut, :], enter_n)

        def by_head(a):
            first = jnp.sum(jnp.where(low, a, 0.0), axis=-1, keepdims=True)
            second = jnp.sum(jnp.where(low, 0.0, a), axis=-1, keepdims=True)
            return jnp.where(low, first, second) * (1.0 / HDN)

        o = o - by_head(o)
        o = o * lax.rsqrt(by_head(o * o) + head_eps)
        mixed[i, :, 128:256] = gated(o, gn[cut, :])
        if d:
            go(mixed_to(d))

    mix_in[pl.ds(x, 1)] = mixed[pl.ds(x, 1)]

    u_relay((1, 1))
    w_last()
    u_step(3)
    u_turn(3)
    d_send(3)
    d_step(1, 0, 1)
    u_relay((1, 0))
    w_done()
    wait_all(mixed.at[pl.ds(0, nx - 1)], mx_r)

    tile = 512
    tiles = width // tile

    def project(n, squares):
        at = pl.ds(pl.multiple_of(n * tile, tile), tile)
        total = stream[:, at].astype(F32)
        for j in range(nx):
            total += dot(mix_in[j], wo[j, :, :, at].reshape(2 * deep, tile))
        total = total.astype(BF16)
        middle[:, at] = total
        total = total.astype(F32)
        return squares + jnp.sum(total * total, axis=-1, keepdims=True)

    squares = lax.fori_loop(0, tiles, project, jnp.zeros((rows, 1), F32))
    scale = lax.rsqrt(squares * (1.0 / width) + norm_eps)
    normed[pl.ds(x, 1)] = (middle[...].astype(F32) * scale * gain[...].astype(F32).reshape(1, width)).astype(BF16)[None]

    def nx_rows(piece, side):
        if piece in (0, 3):
            return pl.ds(side * half_rows, half_rows)
        start = (1 - side) * half_rows
        return pl.ds(start, few) if piece == 1 else pl.ds(start + few, half_rows - few)

    def nm(piece, side):
        ref = normed.at[at_x(-fwd[side] if piece == 3 else 0), nx_rows(piece, side)]
        return same(ref, left_s.at[8], st_r.at[side, piece], x_to[side])

    def nm_in(piece, side):
        ref = normed.at[at_x(-fwd[side] * (2 if piece == 3 else 1)), nx_rows(piece, side)]
        return same(ref, left_s.at[8], st_r.at[side, piece], x_to[side])

    for piece in (0, 1):
        for side in (0, 1):
            go(nm(piece, side))

    u_relay((2, 1))
    d_step(1, 2)
    u_step(4)
    u_turn(4)
    d_step(1, 3)
    d_cores(1)
    u_relay((2, 0))
    d_step(2, 0)
    u_relay((3, 1))
    d_step(2, 1)
    u_relay((3, 0))
    d_step(2, 2)
    for side in (0, 1):
        nm_in(0, side).wait_recv()
        go(nm(3, side))
        go(nm(2, side))
    u_relay((0, 1))
    d_step(2, 3)
    d_cores(2)
    u_rest()
    d_step(3, 0, 1)
    u_last()
    d_step(3, 2)
    u_done()

    def rise(i):
        def one(n, _):
            at = pl.ds(pl.multiple_of(n * tile, tile), tile)
            h = jnp.maximum(dot(normed[i], up[:, :, :, :, at].reshape(width, tile)), 0.0)
            hidden[i, :, at] = (h * h).astype(BF16)
            return 0

        lax.fori_loop(0, tiles, one, 0)

    for side in (0, 1):
        nm_in(3, side).wait_recv()
    rise(xo)
    d_step(3, 3)
    d_cores(3)

    span = width // nz
    blocks_of = (by_distance[:early], by_distance[early:])
    lanes_of = (pl.ds(0, early * span), pl.ds(early * span, width - early * span))

    first, second = slice(0, half_rows), slice(half_rows, rows)

    def fall(i, half, put):
        for n, k in enumerate(blocks_of[half]):
            at = (half * early + n) * span
            put(slice(at, at + span), dot_t(hidden[i], down[at_z(k)].reshape(span, width)))

    def put_far(at, piece):
        send2[:, at] = piece.astype(BF16)

    def put_right(at, piece):
        send1[second, at] = piece[second].astype(BF16)
        hold[0, :, at] = piece[first]

    def put_left(at, piece):
        sendm[first, at] = piece[first].astype(BF16)
        hold[1, :, at] = piece[second]

    def put_own(at, piece):
        own[:, at] = piece

    got_l, got_r = got_both.at[0], got_both.at[1]
    row_halves = (pl.ds(0, half_rows), pl.ds(half_rows, half_rows))

    def far(half, side):
        to = (relay_l, relay_r)[side].at[:, lanes_of[half]]
        return remote(send2.at[row_halves[side], lanes_of[half]], to, left_s.at[9], rs_r.at[2 * half + side], x_to[side])

    def near(half, side, summed):
        at = (row_halves[side if summed else 1 - side], lanes_of[half])
        source, to = ((send1, got_l), (sendm, got_r))[side]
        return remote(source.at[at], to.at[at], left_s.at[9], rs_r.at[4 + half], x_to[side])

    def add_far(half):
        at = lanes_of[half]
        far(half, 0).wait_recv()
        send1[first, at] = (hold[0, :, at] + relay_l[:, at].astype(F32)).astype(BF16)
        go(near(half, 0, 1))
        far(half, 1).wait_recv()
        sendm[second, at] = (hold[1, :, at] + relay_r[:, at].astype(F32)).astype(BF16)
        go(near(half, 1, 1))

    wait_all(down.at[pl.ds(0, early), :, 0], core_r.at[2])
    fall(xo, 0, put_far)
    for side in (0, 1):
        go(far(0, side))
    for side in (0, 1):
        for piece in (1, 2):
            nm_in(piece, side).wait_recv()
    rise(xl)
    d_step(4, 0, 1, 2, 3)
    d_cores(4)
    fall(xl, 0, put_left)
    go(near(0, 1, 0))
    wait_all(down.at[pl.ds(0, nz - early), :, 0], core_r.at[3])
    fall(xo, 1, put_far)
    for side in (0, 1):
        go(far(1, side))
    rise(xr)
    fall(xr, 0, put_right)
    go(near(0, 0, 0))
    add_far(0)
    fall(xr, 1, put_right)
    go(near(1, 0, 0))
    fall(xl, 1, put_left)
    go(near(1, 1, 0))
    add_far(1)
    rise(x)
    fall(x, 0, put_own)
    fall(x, 1, put_own)
    for half in (0, 1):
        at = lanes_of[half]
        wait_all(got_both.at[:, :, at], rs_r.at[4 + half])
        total = own[:, at] + got_l[:, at].astype(F32) + got_r[:, at].astype(F32)
        for n, k in enumerate(blocks_of[half]):
            at = pl.ds(pl.multiple_of(at_z(k) * span, span), span)
            result[:, at] = (middle[:, at].astype(F32) + total[:, n * span : (n + 1) * span]).astype(BF16)
            go(pltpu.make_async_copy(result.at[:, at], out.at[:, at], out_s))

    totals = (
        up.at[pl.ds(0, nz - 1), 0, 0], up.at[:, pl.ds(0, 2), 0], up.at[:, 0, 0], down.at[pl.ds(0, 3), 0, 0],
        down.at[pl.ds(0, nz - 1), :, 0], wo.at[pl.ds(0, 3)], up, mixed.at[pl.ds(0, nx - 1)], normed.at[pl.ds(0, 3)],
        normed.at[pl.ds(0, 3)], msg.at[pl.ds(0, plane - 1)], in2.at[pl.ds(0, nz - 1)], msg.at[pl.ds(0, plane - 1)],
    )
    for i, total in enumerate(totals):
        wait_all(total, left_s.at[i])
    wait_all(out, out_s)


def on_device(
    sizes,
    stream_in, query_wide, key_wide, value_wide, gate_wide, decay_wide,
    query_narrow, key_narrow, value_narrow, gate_narrow, decay_narrow,
    output_wide, output_narrow, norm_gain, up_weight, down_weight,
):
    nz, ny, nc, nx = sizes
    tok = query_wide.shape[0]
    rows, width = stream_in.shape
    plane = ny * nc
    part, hid = up_weight.shape
    ns = (128 + HDN) // plane
    dma = pltpu.SemaphoreType.DMA
    vm = pltpu.VMEM
    scratch = [
        *[vm((tok, 128), BF16)] * 8, vm((rows, width), BF16),
        vm((nz, ny, nc, part, hid), BF16), vm((nz, ny, nc, part, hid), BF16), vm((nx, 2, *output_wide.shape), BF16),
        vm((tok, 128), BF16), vm((tok, 128), BF16), vm((tok, 128), F32), vm((tok, 128), F32),
        vm((128, 128), F32),
        vm((tok // BLOCK, 128, 128), BF16), vm((tok // BLOCK, 128, 128), BF16), vm((tok, 128), BF16), vm((tok, 128), BF16),
        vm((plane, ns + 8, 128), BF16), vm((plane, ns + 8, 128), BF16),
        vm((ns + 8, 128), BF16), vm((nz, ns + 8, 128), BF16),
        vm((plane, ns + 8, 128), BF16), vm((plane, ns + 8, 128), BF16),
        vm((nx, rows, 256), BF16), vm((nx, rows, 256), BF16),
        vm((rows, width), BF16), vm((nx, rows, width), BF16), vm((nx, rows, hid), BF16),
        vm((rows, width), BF16), vm((rows, width), BF16), vm((rows, width), BF16),
        vm((rows, width), F32), vm((2, rows // 2, width), F32), vm((rows, width), BF16),
        vm((rows // 2, width), BF16), vm((rows // 2, width), BF16), vm((2, rows, width), BF16),
        dma((13,)), dma((13,)), dma, dma((2, 4)), dma, dma, dma, dma, dma((6,)), dma((2, 3)), dma((2, 4)), dma((2, 5)),
        dma, dma((2, 2)), dma((2, 4, 4)), dma((4,)),
    ]
    vmem = pl.BlockSpec(memory_space=pltpu.VMEM)
    hbm = pl.BlockSpec(memory_space=pl.ANY)
    return pl.pallas_call(
        functools.partial(kernel, sizes),
        out_shape=jax.ShapeDtypeStruct((rows, width), BF16),
        in_specs=[vmem] * 6 + [hbm] * 13,
        out_specs=hbm,
        scratch_shapes=scratch,
        compiler_params=pltpu.CompilerParams(
            collective_id=0, has_side_effects=True, vmem_limit_bytes=60 * 1024 * 1024
        ),
    )(
        decay_wide, decay_narrow, norm_gain, jnp.asarray(rope_tables(BLOCK, 1)),
        jnp.asarray(rope_tables(8, BLOCK)), jnp.asarray(rope_tables(nz * plane, tok)),
        query_wide, key_wide, value_wide, query_narrow, key_narrow, value_narrow, gate_wide, gate_narrow, stream_in,
        output_wide, output_narrow, up_weight, down_weight.T,
    )


def solution(mesh):
    sizes = (8, 4, 2, mesh.shape["tp"])
    split = Mesh(mesh.devices.reshape(sizes), ("z", "y", "c", "x"))
    sp = ("z", "y", "c")
    rows, heads = P(sp, "x"), P("x", sp)
    in_specs = (
        P((*sp, "x"), None), rows, rows, rows, rows, heads, rows, rows, rows, rows, heads,
        P("x", None), P("x", None), P(), rows, heads,
    )
    return jax.shard_map(
        functools.partial(on_device, sizes), mesh=split, in_specs=in_specs,
        out_specs=P((*sp, "x"), None), check_vma=False,
    )
```

```python
import functools

import jax
import jax.numpy as jnp
import numpy as np
from jax import lax
from jax.experimental import pallas as pl
from jax.experimental.pallas import tpu as pltpu
from jax.sharding import Mesh
from jax.sharding import PartitionSpec as P

HDW = 128
HDN = 64
BLOCK = 128
head_eps = 1e-05
norm_eps = 1e-06
rope_base = 10000.0
MESH = pl.DeviceIdType.MESH
F32 = jnp.float32
BF16 = jnp.bfloat16


def rope_tables(steps, stride):
    tables = []
    for width in (HDW, HDN):
        half = width // 2
        inverse = rope_base ** (-np.arange(half, dtype=np.float64) / half)
        lanes = np.tile(inverse, 128 // half)
        angles = (stride * np.arange(steps, dtype=np.float64))[:, None] * lanes[None, :]
        tables += [np.cos(angles), np.sin(angles)]
    return np.stack(tables).astype(np.float32)


def remote(src, dst, send_sem, recv_sem, device):
    return pltpu.make_async_remote_copy(
        src_ref=src, dst_ref=dst, send_sem=send_sem, recv_sem=recv_sem, device_id=device, device_id_type=MESH
    )


def turn(cos_a, sin_a, cos_b, sin_b):
    return cos_a * cos_b - sin_a * sin_b, sin_a * cos_b + cos_a * sin_b


def dot(a, b):
    return jnp.dot(a, b, preferred_element_type=F32)


def dot_t(a, b):
    return lax.dot_general(a, b, (((1,), (1,)), ((), ())), preferred_element_type=F32)


def tdot(a, b):
    return lax.dot_general(a, b, (((0,), (0,)), ((), ())), preferred_element_type=F32)


def kernel(
    sizes,
    dw, dn, gain, tt, tb, ts,
    qw_in, kw_in, vw_in, qn_in, kn_in, vn_in, gw_in, gn_in, stream_in, ow, on, up_own, down_own,
    out,
    qw, kw, vw, qn, kn, vn, gw, gn, stream,
    up, down, wo,
    qe_w, qe_n, o_w, o_n, decays, st_w, st_n, k_w, k_n, msg, in1, tot2, in2, msg3, in3,
    mixed, mix_in, middle, normed, hidden, send2, send1, sendm, own, hold, result, relay_l, relay_r, got_both,
    left_s, in_s, out_s, st_r, s1_r, s2_r, s3_r, mx_r, rs_r, wo_r, uz_r, uy_r, ur_r, dy_r, dz_r, core_r,
):
    nz, ny, nc, nx = sizes
    z, y, c, x = (lax.axis_index(a) for a in ("z", "y", "c", "x"))
    xr, xl, xo = lax.rem(x + 1, nx), lax.rem(x + nx - 1, nx), lax.rem(x + 2, nx)
    plane = ny * nc
    me = y * nc + c
    sp = z * plane + me
    tok = qw.shape[0]
    blocks = tok // BLOCK
    rows = stream.shape[0]
    width = stream.shape[1]
    half_rows, part_rows = rows // 2, rows // 4
    right, left = {"x": xr}, {"x": xl}

    def at_plane(j):
        return {"y": j // nc, "c": lax.rem(j, nc)}

    barrier = pltpu.get_barrier_semaphore()
    peers = [right, left, {"x": xo}]
    peers += [at_plane(lax.rem(me + d, plane)) for d in range(1, plane)]
    peers += [{"z": lax.rem(z + d, nz)} for d in range(1, nz)]
    for peer in peers:
        pl.semaphore_signal(barrier, inc=1, device_id=peer, device_id_type=MESH)

    pairs = [
        (kw_in, kw), (vw_in, vw), (kn_in, kn), (vn_in, vn),
        (up_own, up.at[z, y, c]), (ow, wo.at[x, 0]), (on, wo.at[x, 1]), (down_own, down.at[z, y, c]),
        (qw_in, qw), (qn_in, qn), (gw_in, gw), (gn_in, gn), (stream_in, stream),
    ]
    loads = [pltpu.make_async_copy(a, b, in_s.at[i]) for i, (a, b) in enumerate(pairs)]
    for load in loads:
        load.start()

    lane = lax.broadcasted_iota(jnp.int32, (1, 128), 1)
    low = lane < HDN
    base = []
    for g in (0, 2):
        row = [ts[g + i, pl.ds(sp, 1), :] for i in (0, 1)]
        base.append(turn(row[0], row[1], tb[g], tb[g + 1]))
    sign_w = jnp.where(lane < HDW // 2, -1.0, 1.0)
    front_n = lax.rem(lane, HDN) < HDN // 2
    sign_n = jnp.where(front_n, -1.0, 1.0)

    def go(copy):
        copy.start()

    def wait_all(ref, sem):
        pltpu.make_async_copy(ref, ref, sem).wait()

    def same(ref, send_sem, recv_sem, device):
        return remote(ref, ref, send_sem, recv_sem, device)

    z_to = ({"z": lax.rem(z + 1, nz)}, {"z": lax.rem(z + nz - 1, nz)})
    y_to = ({"y": lax.rem(y + 1, ny)}, {"y": lax.rem(y + ny - 1, ny)})
    x_to = (right, left)
    partner = {"c": 1 - c}
    fwd = (1, -1)

    def at_z(k):
        return lax.rem(z + nz + k, nz)

    def at_y(k):
        return lax.rem(y + ny + k, ny)

    def at_x(k):
        return lax.rem(x + nx + k, nx)

    part = up.shape[3]
    halves = (pl.ds(0, part // 2), pl.ds(part // 2, part // 2))

    relayed = ((0, 1, 2, 3), (4, -1, -2, -3))

    def uz(step, side):
        ref = up.at[at_z(-fwd[side] * (step - 1)), y, c]
        if step == nz // 2:
            ref = ref.at[halves[side]]
        return same(ref, left_s.at[0], uz_r.at[side, step - 1], z_to[side])

    def uz_in(step, side):
        ref = up.at[at_z(-fwd[side] * step), y, c]
        if step == nz // 2:
            ref = ref.at[halves[side]]
        return same(ref, left_s.at[0], uz_r.at[side, step - 1], z_to[side])

    def uy(off, side):
        return same(up.at[at_z(off), y, c], left_s.at[1], uy_r.at[side, relayed[side].index(off) if off in relayed[side] else 4], y_to[side])

    def uy_in(off, side):
        ref = up.at[at_z(off), at_y(-fwd[side]), c]
        return same(ref, left_s.at[1], uy_r.at[side, relayed[side].index(off) if off in relayed[side] else 4], y_to[side])


    def ur(i, side):
        ref = up.at[at_z(relayed[side][i]), at_y(-fwd[side]), c]
        return same(ref, left_s.at[2], ur_r, y_to[side])

    def u_core(i):
        ref = up.at[:, at_y((0, 1, -1, 2)[i]), c]
        return same(ref, left_s.at[6], core_r.at[0], partner)

    def u_step(step):
        for side in (0, 1):
            uz_in(step, side).wait_recv()
            if step < nz // 2:
                go(uz(step + 1, side))

    def u_turn(step):
        offs = (-step, step) if step < nz // 2 else (step,)
        for off in offs:
            for side in (0, 1):
                go(uy(off, side))
        if step == nz // 2:
            go(u_core(0))

    def u_relay(*which):
        for i, side in which:
            uy_in(relayed[side][i], side).wait_recv()
            go(ur(i, side))

    def u_rest():
        for side in (0, 1):
            wait_all(up.at[pl.ds(0, 4), 0, 0], uy_r.at[side, 4])
        go(u_core(1))
        go(u_core(2))

    def u_last():
        wait_all(up.at[:, 0, 0], ur_r)
        go(u_core(3))

    def u_done():
        wait_all(up.at[:, :, 0], core_r.at[0])

    by_distance = (0, 1, -1, 2, -2, 3, -3, 4)
    early = 5

    def dy(step, side):
        ref = down.at[z, at_y(-fwd[side] * (step - 1)), c]
        if step == 2:
            ref = ref.at[halves[side]]
        return same(ref, left_s.at[3], dy_r.at[side, step - 1], y_to[side])

    def dy_in(step, side):
        ref = down.at[z, at_y(-fwd[side] * step), c]
        if step == 2:
            ref = ref.at[halves[side]]
        return same(ref, left_s.at[3], dy_r.at[side, step - 1], y_to[side])

    columns_y = (0, 1, -1, 2)
    last_by = ((0, 3), (2, 1))

    def dz(step, side, g):
        ref = down.at[at_z(-fwd[side] * (step - 1)), at_y(columns_y[g]), c]
        return same(ref, left_s.at[4], dz_r.at[side, step - 1, g], z_to[side])

    def dz_in(step, side, g):
        ref = down.at[at_z(-fwd[side] * step), at_y(columns_y[g]), c]
        return same(ref, left_s.at[4], dz_r.at[side, step - 1, g], z_to[side])

    def d_core(k):
        return same(down.at[at_z(k), :, c], left_s.at[6], core_r.at[2 if k in by_distance[:early] else 3], partner)

    def d_own():
        for side in (0, 1):
            go(dy(1, side))

    def d_turn():
        for side in (0, 1):
            dy_in(1, side).wait_recv()
            go(dy(2, side))

    def d_column():
        for side in (0, 1):
            dy_in(2, side).wait_recv()
        go(d_core(0))

    def d_send(*gs):
        for side in (0, 1):
            for g in gs:
                go(dz(1, side, g))

    def d_step(step, *gs):
        for g in gs:
            for side in (0, 1):
                if step < nz // 2:
                    dz_in(step, side, g).wait_recv()
                    if step + 1 < nz // 2 or g in last_by[side]:
                        go(dz(step + 1, side, g))
                elif g in last_by[side]:
                    dz_in(step, side, g).wait_recv()

    def d_cores(step):
        go(d_core(step))
        if step < nz // 2:
            go(d_core(-step))

    deep = wo.shape[2]
    wo_halves = (pl.ds(0, deep // 2), pl.ds(deep // 2, deep // 2))

    def wx(step, side):
        ref = wo.at[at_x(-fwd[side] if step == 2 else 0), c].at[wo_halves[1 - side if step == 1 else side]]
        return same(ref, left_s.at[5], wo_r.at[side, step], x_to[side])

    def wx_in(step, side):
        ref = wo.at[at_x(-fwd[side] * (2 if step == 2 else 1)), c].at[wo_halves[1 - side if step == 1 else side]]
        return same(ref, left_s.at[5], wo_r.at[side, step], x_to[side])

    def w_core(i):
        return same(wo.at[at_x(i + 1), c], left_s.at[5], core_r.at[1], partner)

    def w_turn():
        for side in (0, 1):
            wx_in(0, side).wait_recv()
            go(wx(2, side))

    def w_near():
        for side in (0, 1):
            wx_in(1, side).wait_recv()
        go(w_core(0))
        go(w_core(2))

    def w_last():
        for side in (0, 1):
            wx_in(2, side).wait_recv()
        go(w_core(1))

    def w_done():
        wait_all(wo.at[pl.ds(0, nx - 1), 0], core_r.at[1])

    for load in loads[:4]:
        load.wait()

    decays[...] = jnp.zeros_like(decays)
    for b in range(blocks):
        cut = pl.ds(b * BLOCK, BLOCK)
        decays[pl.ds(3 * b, 1), :] = dw[:, cut]
        decays[pl.ds(3 * b + 1, 2), :] = dn[:, cut]
    running = decays[0:32, :]
    shift = 1
    while shift < BLOCK:
        running = running + jnp.where(lane >= shift, pltpu.roll(running, shift, 1), 0.0)
        shift *= 2
    decays[0:32, :] = running
    columns = jnp.transpose(decays[...])

    at_t = lax.broadcasted_iota(jnp.int32, (BLOCK, BLOCK), 0)
    at_s = lax.broadcasted_iota(jnp.int32, (BLOCK, BLOCK), 1)
    lower = at_t >= at_s
    same_head = (at_t < HDN) == (at_s < HDN)

    def spread(r):
        steps = jnp.minimum(columns[:, r : r + 1] - decays[pl.ds(r, 1), :], 0.0)
        return jnp.where(lower, jnp.exp(steps), 0.0)

    def angles(b):
        cos_w, sin_w = turn(base[0][0][b : b + 1], base[0][1][b : b + 1], tt[0], tt[1])
        cos_n, sin_n = turn(base[1][0][b : b + 1], base[1][1][b : b + 1], tt[2], tt[3])
        return cos_w, sin_w * sign_w, cos_n, sin_n * sign_n

    def rotate_w(a, cos, sin):
        return a * cos + pltpu.roll(a, HDW // 2, 1) * sin

    def rotate_n(a, cos, sin):
        other = jnp.where(front_n, pltpu.roll(a, 128 - HDN // 2, 1), pltpu.roll(a, HDN // 2, 1))
        return a * cos + other * sin

    def ends(b):
        r = 3 * b
        now = [columns[:, r + h : r + h + 1] for h in range(3)]
        return now, [columns[BLOCK - 1 : BLOCK, r + h : r + h + 1] for h in range(3)]

    state_w = jnp.zeros((128, 128), F32)
    state_n = jnp.zeros((128, 128), F32)
    gone = [jnp.zeros((1, 1), F32)] * 3
    before_block = []
    for b in range(blocks):
        cut = pl.ds(b * BLOCK, BLOCK)
        now, last = ends(b)
        cos_w, sin_w, cos_n, sin_n = angles(b)
        st_w[b] = state_w.astype(BF16)
        st_n[b] = state_n.astype(BF16)
        before_block.append(gone)
        k = rotate_w(kw[cut, :].astype(F32), cos_w, sin_w) * HDW**-0.5
        k_w[cut, :] = k.astype(BF16)
        tail = k * jnp.exp(last[0] - now[0])
        state_w = jnp.exp(last[0]) * state_w + tdot(tail.astype(BF16), vw[cut, :])
        k = rotate_n(kn[cut, :].astype(F32), cos_n, sin_n) * HDN**-0.5
        k_n[cut, :] = k.astype(BF16)
        tail = k * jnp.where(low, jnp.exp(last[1] - now[1]), jnp.exp(last[2] - now[2]))
        keep = jnp.where(low, jnp.exp(last[1]), jnp.exp(last[2]))
        state_n = keep * state_n + jnp.where(same_head, tdot(tail.astype(BF16), vn[cut, :]), 0.0)
        gone = [g + t for g, t in zip(gone, last)]

    def outputs(b):
        cut = pl.ds(b * BLOCK, BLOCK)
        r = 3 * b
        now, last = ends(b)
        cos_w, sin_w, cos_n, sin_n = angles(b)
        gone = before_block[b]
        q = rotate_w(qw[cut, :].astype(F32), cos_w, sin_w)
        scores = dot_t(q.astype(BF16), k_w[cut, :]) * spread(r)
        out_b = dot(scores.astype(BF16), vw[cut, :])
        if b:
            out_b += dot((q * jnp.exp(now[0])).astype(BF16), st_w[b])
        o_w[cut, :] = out_b
        qe_w[cut, :] = (q * jnp.exp(now[0] + gone[0])).astype(BF16)
        q = rotate_n(qn[cut, :].astype(F32), cos_n, sin_n)
        probs = []
        for h, mask in enumerate((low, jnp.logical_not(low))):
            qh = jnp.where(mask, q, 0.0).astype(BF16)
            probs.append((dot_t(qh, k_n[cut, :]) * spread(r + 1 + h)).astype(BF16))
        v_f = vn[cut, :].astype(F32)
        v2 = jnp.concatenate(
            [jnp.where(low, v_f, 0.0).astype(BF16), jnp.where(low, 0.0, v_f).astype(BF16)], axis=0
        )
        out_b = dot(jnp.concatenate(probs, axis=1), v2)
        if b:
            seen = jnp.where(low, jnp.exp(now[1]), jnp.exp(now[2]))
            out_b += dot((q * seen).astype(BF16), st_n[b])
        o_n[cut, :] = out_b
        seen = jnp.where(low, jnp.exp(now[1] + gone[1]), jnp.exp(now[2] + gone[2]))
        qe_n[cut, :] = (q * seen).astype(BF16)

    total_w = jnp.exp(gone[0]) + jnp.zeros((1, 128), F32)
    total_n = jnp.where(low, jnp.exp(gone[1]), jnp.exp(gone[2]))
    packed_n = jnp.where(low, state_n[:HDN], state_n[HDN:])
    sw, sn = 128 // plane, HDN // plane
    part_of = lax.broadcasted_iota(jnp.int32, (8, 128), 0)

    def message(state, rate_w, rate_n):
        parts = jnp.zeros((8, 128), F32)
        for r, rate in ((0, rate_w), (2, rate_n)):
            high = rate.astype(BF16).astype(F32)
            parts = jnp.where(part_of == r, high, jnp.where(part_of == r + 1, rate - high, parts))
        return jnp.concatenate([state, parts], axis=0).astype(BF16)

    for j in range(plane):
        state = [state_w[sw * j : sw * (j + 1)], packed_n[sn * j : sn * (j + 1)]]
        msg[j] = message(jnp.concatenate(state, axis=0), total_w, total_n)
    ns = sw + sn

    def stage1(d):
        to = lax.rem(me + d, plane)
        return remote(msg.at[to], in1.at[me], left_s.at[10], s1_r, at_plane(to))

    pl.semaphore_wait(barrier, len(peers))
    for d in range(1, plane):
        stage1(d).start()
    for load in loads[4:10]:
        load.wait()
    for side in (0, 1):
        go(uz(1, side))
        go(wx(0, side))
    d_own()
    for side in (0, 1):
        go(wx(1, side))
    in1[pl.ds(me, 1)] = msg[pl.ds(me, 1)]
    for b in range(blocks // 2):
        outputs(b)

    wait_all(msg.at[pl.ds(0, plane - 1)], s1_r)
    wide_row = lax.broadcasted_iota(jnp.int32, (ns, 128), 0) < sw

    def factor(pair):
        return jnp.where(wide_row, pair[0], pair[1])

    def opened(ref, j):
        whole = ref[j].astype(F32)
        return whole[0:ns], (whole[ns : ns + 1] + whole[ns + 1 : ns + 2], whole[ns + 2 : ns + 3] + whole[ns + 3 : ns + 4])

    before = []
    held = jnp.zeros((ns, 128), F32)
    rate = (jnp.ones((1, 128), F32), jnp.ones((1, 128), F32))
    for j in range(plane):
        before.append((held, rate))
        state, mine = opened(in1, j)
        held = held * factor(mine) + state
        rate = (rate[0] * mine[0], rate[1] * mine[1])
    tot2[...] = message(held, *rate)

    def stage2(d):
        return remote(tot2, in2.at[z], left_s.at[11], s2_r, {"z": lax.rem(z + d, nz)})

    for d in range(1, nz):
        stage2(d).start()
    for side in (0, 1):
        go(uy(0, side))
    d_send(0)
    for b in range(blocks // 2, blocks):
        outputs(b)
    u_step(1)
    d_turn()
    d_send(1)
    w_turn()
    in2[pl.ds(z, 1)] = tot2[...][None]
    wait_all(in2.at[pl.ds(0, nz - 1)], s2_r)
    held = jnp.zeros((ns, 128), F32)
    for k in range(nz):
        state, mine = opened(in2, k)
        later = held * factor(mine) + state
        held = jnp.where(k < z, later, held)
    for j in range(plane):
        state, rate = before[j]
        state = held * factor(rate) + state
        msg3[j] = jnp.concatenate([state, jnp.zeros((8, 128), F32)], axis=0).astype(BF16)

    def stage3(d):
        to = lax.rem(me + d, plane)
        return remote(msg3.at[to], in3.at[me], left_s.at[12], s3_r, at_plane(to))

    for d in range(1, plane):
        stage3(d).start()
    in3[pl.ds(me, 1)] = msg3[pl.ds(me, 1)]
    u_turn(1)
    u_relay((0, 0))
    d_column()
    w_near()
    u_step(2)
    u_turn(2)
    d_send(2)
    for load in loads[10:]:
        load.wait()
    wait_all(msg.at[pl.ds(0, plane - 1)], s3_r)
    arrived = in3[...].astype(F32)
    enter_w = arrived[:, 0:sw, :].reshape(128, 128).astype(BF16)
    enter_p = arrived[:, sw:ns, :].reshape(HDN, 128)
    enter_n = jnp.concatenate(
        [jnp.where(low, enter_p, 0.0), jnp.where(low, 0.0, enter_p)], axis=0
    ).astype(BF16)

    def mixed_to(d):
        to = lax.rem(x + d, nx)
        return remote(mixed.at[to], mix_in.at[x], left_s.at[7], mx_r, {"x": to})

    def gated(o, gate):
        return (o * jax.nn.silu(gate.astype(F32))).astype(BF16)

    for d in (2, 1, 3, 0):
        i = lax.rem(x + d, nx)
        cut = pl.ds(pl.multiple_of(i * rows, rows), rows)
        o = o_w[cut, :] + dot(qe_w[cut, :], enter_w)
        o = o - jnp.mean(o, axis=-1, keepdims=True)
        o = o * lax.rsqrt(jnp.mean(o * o, axis=-1, keepdims=True) + head_eps)
        mixed[i, :, 0:128] = gated(o, gw[cut, :])
        o = o_n[cut, :] + dot(qe_n[cut, :], enter_n)

        def by_head(a):
            first = jnp.sum(jnp.where(low, a, 0.0), axis=-1, keepdims=True)
            second = jnp.sum(jnp.where(low, 0.0, a), axis=-1, keepdims=True)
            return jnp.where(low, first, second) * (1.0 / HDN)

        o = o - by_head(o)
        o = o * lax.rsqrt(by_head(o * o) + head_eps)
        mixed[i, :, 128:256] = gated(o, gn[cut, :])
        if d:
            go(mixed_to(d))

    mix_in[pl.ds(x, 1)] = mixed[pl.ds(x, 1)]

    u_relay((1, 1))
    w_last()
    u_step(3)
    u_turn(3)
    d_send(3)
    d_step(1, 0, 1)
    u_relay((1, 0))
    w_done()
    wait_all(mixed.at[pl.ds(0, nx - 1)], mx_r)

    tile = 512
    tiles = width // tile

    def project(n, squares):
        at = pl.ds(pl.multiple_of(n * tile, tile), tile)
        total = stream[:, at].astype(F32)
        for j in range(nx):
            total += dot(mix_in[j], wo[j, :, :, at].reshape(2 * deep, tile))
        total = total.astype(BF16)
        middle[:, at] = total
        total = total.astype(F32)
        return squares + jnp.sum(total * total, axis=-1, keepdims=True)

    squares = lax.fori_loop(0, tiles, project, jnp.zeros((rows, 1), F32))
    scale = lax.rsqrt(squares * (1.0 / width) + norm_eps)
    normed[pl.ds(x, 1)] = (middle[...].astype(F32) * scale * gain[...].astype(F32).reshape(1, width)).astype(BF16)[None]

    def nx_rows(piece, side):
        if piece == 4:
            return pl.ds((1 - side) * half_rows, half_rows)
        return pl.ds(side * half_rows + piece % 2 * part_rows, part_rows)

    def nm(piece, side):
        ref = normed.at[at_x(-fwd[side] if piece in (2, 3) else 0), nx_rows(piece, side)]
        return same(ref, left_s.at[8], st_r.at[side, piece], x_to[side])

    def nm_in(piece, side):
        ref = normed.at[at_x(-fwd[side] * (2 if piece in (2, 3) else 1)), nx_rows(piece, side)]
        return same(ref, left_s.at[8], st_r.at[side, piece], x_to[side])

    def nm_on(piece):
        for side in (0, 1):
            nm_in(piece, side).wait_recv()
            go(nm(piece + 2, side))

    for piece in (0, 1):
        for side in (0, 1):
            go(nm(piece, side))

    u_relay((2, 1))
    d_step(1, 2)
    u_step(4)
    u_turn(4)
    d_step(1, 3)
    d_cores(1)
    u_relay((2, 0))
    d_step(2, 0)
    u_relay((3, 1))
    d_step(2, 1)
    nm_on(0)
    u_relay((3, 0))
    d_step(2, 2)
    nm_on(1)
    for side in (0, 1):
        go(nm(4, side))
    u_relay((0, 1))
    d_step(2, 3)
    d_cores(2)
    u_rest()
    d_step(3, 0)
    u_last()
    d_step(3, 1)
    u_done()

    near_rows = ((xl, 0, xr, 1), (xo, 0, xo, 1), (xr, 0, xl, 1), (x, 0, x, 1))
    EARLY, FAR, LATE, OWN = range(4)

    def rise(batch):
        slot_a, half_a, slot_b, half_b = near_rows[batch]

        def one(n, _):
            at = pl.ds(pl.multiple_of(n * tile, tile), tile)
            a = normed[slot_a, half_a * half_rows : (half_a + 1) * half_rows]
            b = normed[slot_b, half_b * half_rows : (half_b + 1) * half_rows]
            h = dot(jnp.concatenate([a, b], axis=0), up[:, :, :, :, at].reshape(width, tile))
            h = jnp.maximum(h, 0.0)
            hidden[batch, :, at] = (h * h).astype(BF16)
            return 0

        lax.fori_loop(0, tiles, one, 0)

    span = width // nz
    blocks_of = (by_distance[:early], by_distance[early:])
    lanes_of = (pl.ds(0, early * span), pl.ds(early * span, width - early * span))

    first, second = slice(0, half_rows), slice(half_rows, rows)

    def fall(batch, half, put):
        for n, k in enumerate(blocks_of[half]):
            at = (half * early + n) * span
            put(slice(at, at + span), dot_t(hidden[batch], down[at_z(k)].reshape(span, width)))

    def put_far(at, piece):
        send2[:, at] = piece.astype(BF16)

    def put_early(at, piece):
        sendm[first, at] = piece[first].astype(BF16)
        send1[second, at] = piece[second].astype(BF16)

    def put_late(at, piece):
        hold[0, :, at] = piece[first]
        hold[1, :, at] = piece[second]

    def put_own(at, piece):
        own[:, at] = piece

    got_l, got_r = got_both.at[0], got_both.at[1]
    row_halves = (pl.ds(0, half_rows), pl.ds(half_rows, half_rows))

    def far(half, side):
        to = (relay_l, relay_r)[side].at[:, lanes_of[half]]
        return remote(send2.at[row_halves[side], lanes_of[half]], to, left_s.at[9], rs_r.at[2 * half + side], x_to[side])

    def near(half, side, summed):
        at = (row_halves[side if summed else 1 - side], lanes_of[half])
        source, to = ((send1, got_l), (sendm, got_r))[side]
        return remote(source.at[at], to.at[at], left_s.at[9], rs_r.at[4 + half], x_to[side])

    def add_far(half):
        at = lanes_of[half]
        far(half, 0).wait_recv()
        send1[first, at] = (hold[0, :, at] + relay_l[:, at].astype(F32)).astype(BF16)
        go(near(half, 0, 1))
        far(half, 1).wait_recv()
        sendm[second, at] = (hold[1, :, at] + relay_r[:, at].astype(F32)).astype(BF16)
        go(near(half, 1, 1))

    rise(EARLY)
    d_step(3, 2)
    wait_all(down.at[pl.ds(0, early), :, 0], core_r.at[2])
    fall(EARLY, 0, put_early)
    for side in (0, 1):
        go(near(0, side, 0))
    for side in (0, 1):
        nm_in(2, side).wait_recv()
        nm_in(3, side).wait_recv()
    d_step(3, 3)
    d_cores(3)
    rise(FAR)
    fall(FAR, 0, put_far)
    for side in (0, 1):
        go(far(0, side))
    d_step(4, 0, 1, 2, 3)
    d_cores(4)
    for side in (0, 1):
        nm_in(4, side).wait_recv()
    rise(LATE)
    fall(LATE, 0, put_late)
    wait_all(down.at[pl.ds(0, nz - early), :, 0], core_r.at[3])
    fall(EARLY, 1, put_early)
    for side in (0, 1):
        go(near(1, side, 0))
    fall(FAR, 1, put_far)
    for side in (0, 1):
        go(far(1, side))
    add_far(0)
    fall(LATE, 1, put_late)
    add_far(1)
    rise(OWN)
    fall(OWN, 0, put_own)
    fall(OWN, 1, put_own)
    for half in (0, 1):
        at = lanes_of[half]
        wait_all(got_both.at[:, :, at], rs_r.at[4 + half])
        total = own[:, at] + got_l[:, at].astype(F32) + got_r[:, at].astype(F32)
        for n, k in enumerate(blocks_of[half]):
            at = pl.ds(pl.multiple_of(at_z(k) * span, span), span)
            result[:, at] = (middle[:, at].astype(F32) + total[:, n * span : (n + 1) * span]).astype(BF16)
            go(pltpu.make_async_copy(result.at[:, at], out.at[:, at], out_s))

    totals = (
        up.at[pl.ds(0, nz - 1), 0, 0], up.at[:, pl.ds(0, 2), 0], up.at[:, 0, 0], down.at[pl.ds(0, 3), 0, 0],
        down.at[pl.ds(0, nz - 1), :, 0], wo.at[pl.ds(0, 3)], up, mixed.at[pl.ds(0, nx - 1)], normed.at[pl.ds(0, 3)],
        normed.at[pl.ds(0, 3)], msg.at[pl.ds(0, plane - 1)], in2.at[pl.ds(0, nz - 1)], msg.at[pl.ds(0, plane - 1)],
    )
    for i, total in enumerate(totals):
        wait_all(total, left_s.at[i])
    wait_all(out, out_s)


def on_device(
    sizes,
    stream_in, query_wide, key_wide, value_wide, gate_wide, decay_wide,
    query_narrow, key_narrow, value_narrow, gate_narrow, decay_narrow,
    output_wide, output_narrow, norm_gain, up_weight, down_weight,
):
    nz, ny, nc, nx = sizes
    tok = query_wide.shape[0]
    rows, width = stream_in.shape
    plane = ny * nc
    part, hid = up_weight.shape
    ns = (128 + HDN) // plane
    dma = pltpu.SemaphoreType.DMA
    vm = pltpu.VMEM
    scratch = [
        *[vm((tok, 128), BF16)] * 8, vm((rows, width), BF16),
        vm((nz, ny, nc, part, hid), BF16), vm((nz, ny, nc, part, hid), BF16), vm((nx, 2, *output_wide.shape), BF16),
        vm((tok, 128), BF16), vm((tok, 128), BF16), vm((tok, 128), F32), vm((tok, 128), F32),
        vm((128, 128), F32),
        vm((tok // BLOCK, 128, 128), BF16), vm((tok // BLOCK, 128, 128), BF16), vm((tok, 128), BF16), vm((tok, 128), BF16),
        vm((plane, ns + 8, 128), BF16), vm((plane, ns + 8, 128), BF16),
        vm((ns + 8, 128), BF16), vm((nz, ns + 8, 128), BF16),
        vm((plane, ns + 8, 128), BF16), vm((plane, ns + 8, 128), BF16),
        vm((nx, rows, 256), BF16), vm((nx, rows, 256), BF16),
        vm((rows, width), BF16), vm((nx, rows, width), BF16), vm((nx, rows, hid), BF16),
        vm((rows, width), BF16), vm((rows, width), BF16), vm((rows, width), BF16),
        vm((rows, width), F32), vm((2, rows // 2, width), F32), vm((rows, width), BF16),
        vm((rows // 2, width), BF16), vm((rows // 2, width), BF16), vm((2, rows, width), BF16),
        dma((13,)), dma((13,)), dma, dma((2, 5)), dma, dma, dma, dma, dma((6,)), dma((2, 3)), dma((2, 4)), dma((2, 5)),
        dma, dma((2, 2)), dma((2, 4, 4)), dma((4,)),
    ]
    vmem = pl.BlockSpec(memory_space=pltpu.VMEM)
    hbm = pl.BlockSpec(memory_space=pl.ANY)
    return pl.pallas_call(
        functools.partial(kernel, sizes),
        out_shape=jax.ShapeDtypeStruct((rows, width), BF16),
        in_specs=[vmem] * 6 + [hbm] * 13,
        out_specs=hbm,
        scratch_shapes=scratch,
        compiler_params=pltpu.CompilerParams(
            collective_id=0, has_side_effects=True, vmem_limit_bytes=60 * 1024 * 1024
        ),
    )(
        decay_wide, decay_narrow, norm_gain, jnp.asarray(rope_tables(BLOCK, 1)),
        jnp.asarray(rope_tables(8, BLOCK)), jnp.asarray(rope_tables(nz * plane, tok)),
        query_wide, key_wide, value_wide, query_narrow, key_narrow, value_narrow, gate_wide, gate_narrow, stream_in,
        output_wide, output_narrow, up_weight, down_weight.T,
    )


def solution(mesh):
    sizes = (8, 4, 2, mesh.shape["tp"])
    split = Mesh(mesh.devices.reshape(sizes), ("z", "y", "c", "x"))
    sp = ("z", "y", "c")
    rows, heads = P(sp, "x"), P("x", sp)
    in_specs = (
        P((*sp, "x"), None), rows, rows, rows, rows, heads, rows, rows, rows, rows, heads,
        P("x", None), P("x", None), P(), rows, heads,
    )
    return jax.shard_map(
        functools.partial(on_device, sizes), mesh=split, in_specs=in_specs,
        out_specs=P((*sp, "x"), None), check_vma=False,
    )
```

```python
import functools

import jax
import jax.numpy as jnp
import numpy as np
from jax import lax
from jax.experimental import pallas as pl
from jax.experimental.pallas import tpu as pltpu
from jax.sharding import Mesh
from jax.sharding import PartitionSpec as P

HDW = 128
HDN = 64
BLOCK = 128
head_eps = 1e-05
norm_eps = 1e-06
rope_base = 10000.0
MESH = pl.DeviceIdType.MESH
F32 = jnp.float32
BF16 = jnp.bfloat16


def rope_tables(steps, stride):
    tables = []
    for width in (HDW, HDN):
        half = width // 2
        inverse = rope_base ** (-np.arange(half, dtype=np.float64) / half)
        lanes = np.tile(inverse, 128 // half)
        angles = (stride * np.arange(steps, dtype=np.float64))[:, None] * lanes[None, :]
        tables += [np.cos(angles), np.sin(angles)]
    return np.stack(tables).astype(np.float32)


def remote(src, dst, send_sem, recv_sem, device):
    return pltpu.make_async_remote_copy(
        src_ref=src, dst_ref=dst, send_sem=send_sem, recv_sem=recv_sem, device_id=device, device_id_type=MESH
    )


def turn(cos_a, sin_a, cos_b, sin_b):
    return cos_a * cos_b - sin_a * sin_b, sin_a * cos_b + cos_a * sin_b


def dot(a, b):
    return jnp.dot(a, b, preferred_element_type=F32)


def dot_t(a, b):
    return lax.dot_general(a, b, (((1,), (1,)), ((), ())), preferred_element_type=F32)


def tdot(a, b):
    return lax.dot_general(a, b, (((0,), (0,)), ((), ())), preferred_element_type=F32)


def kernel(
    sizes,
    dw, dn, gain, tt, tb, ts,
    qw_in, kw_in, vw_in, qn_in, kn_in, vn_in, gw_in, gn_in, stream_in, ow, on, up_own, down_own,
    out,
    qw, kw, vw, qn, kn, vn, gw, gn, stream,
    up, down, wo,
    qe_w, qe_n, o_w, o_n, decays, st_w, st_n, k_w, k_n, msg, in1, tot2, in2, msg3, in3,
    mixed, mix_in, middle, normed, hidden, send2, send1, sendm, own, hold, result, relay_l, relay_r, got_both,
    left_s, in_s, out_s, st_r, s1_r, s2_r, s3_r, mx_r, rs_r, wo_r, uz_r, uy_r, ur_r, dy_r, dz_r, core_r,
):
    nz, ny, nc, nx = sizes
    z, y, c, x = (lax.axis_index(a) for a in ("z", "y", "c", "x"))
    xr, xl, xo = lax.rem(x + 1, nx), lax.rem(x + nx - 1, nx), lax.rem(x + 2, nx)
    plane = ny * nc
    me = y * nc + c
    sp = z * plane + me
    tok = qw.shape[0]
    blocks = tok // BLOCK
    rows = stream.shape[0]
    width = stream.shape[1]
    half_rows, part_rows = rows // 2, rows // 4
    right, left = {"x": xr}, {"x": xl}

    def at_plane(j):
        return {"y": j // nc, "c": lax.rem(j, nc)}

    barrier = pltpu.get_barrier_semaphore()
    peers = [right, left, {"x": xo}]
    peers += [at_plane(lax.rem(me + d, plane)) for d in range(1, plane)]
    peers += [{"z": lax.rem(z + d, nz)} for d in range(1, nz)]
    for peer in peers:
        pl.semaphore_signal(barrier, inc=1, device_id=peer, device_id_type=MESH)

    pairs = [
        (kw_in, kw), (vw_in, vw), (kn_in, kn), (vn_in, vn),
        (up_own, up.at[z, y, c]), (ow, wo.at[x, 0]), (on, wo.at[x, 1]), (down_own, down.at[z, y, c]),
        (qw_in, qw), (qn_in, qn), (gw_in, gw), (gn_in, gn), (stream_in, stream),
    ]
    loads = [pltpu.make_async_copy(a, b, in_s.at[i]) for i, (a, b) in enumerate(pairs)]
    for load in loads:
        load.start()

    lane = lax.broadcasted_iota(jnp.int32, (1, 128), 1)
    low = lane < HDN
    base = []
    for g in (0, 2):
        row = [ts[g + i, pl.ds(sp, 1), :] for i in (0, 1)]
        base.append(turn(row[0], row[1], tb[g], tb[g + 1]))
    sign_w = jnp.where(lane < HDW // 2, -1.0, 1.0)
    front_n = lax.rem(lane, HDN) < HDN // 2
    sign_n = jnp.where(front_n, -1.0, 1.0)

    def go(copy):
        copy.start()

    def wait_all(ref, sem):
        pltpu.make_async_copy(ref, ref, sem).wait()

    def same(ref, send_sem, recv_sem, device):
        return remote(ref, ref, send_sem, recv_sem, device)

    z_to = ({"z": lax.rem(z + 1, nz)}, {"z": lax.rem(z + nz - 1, nz)})
    y_to = ({"y": lax.rem(y + 1, ny)}, {"y": lax.rem(y + ny - 1, ny)})
    x_to = (right, left)
    partner = {"c": 1 - c}
    fwd = (1, -1)

    def at_z(k):
        return lax.rem(z + nz + k, nz)

    def at_y(k):
        return lax.rem(y + ny + k, ny)

    def at_x(k):
        return lax.rem(x + nx + k, nx)

    part = up.shape[3]
    halves = (pl.ds(0, part // 2), pl.ds(part // 2, part // 2))

    relayed = ((0, 1, 2, 3), (4, -1, -2, -3))

    def uz(step, side):
        ref = up.at[at_z(-fwd[side] * (step - 1)), y, c]
        if step == nz // 2:
            ref = ref.at[halves[side]]
        return same(ref, left_s.at[0], uz_r.at[side, step - 1], z_to[side])

    def uz_in(step, side):
        ref = up.at[at_z(-fwd[side] * step), y, c]
        if step == nz // 2:
            ref = ref.at[halves[side]]
        return same(ref, left_s.at[0], uz_r.at[side, step - 1], z_to[side])

    def uy(off, side):
        return same(up.at[at_z(off), y, c], left_s.at[1], uy_r.at[side, relayed[side].index(off) if off in relayed[side] else 4], y_to[side])

    def uy_in(off, side):
        ref = up.at[at_z(off), at_y(-fwd[side]), c]
        return same(ref, left_s.at[1], uy_r.at[side, relayed[side].index(off) if off in relayed[side] else 4], y_to[side])


    relays = (((0, 0), (1, 1), (1, 0), (2, 1)), ((2, 0), (3, 1), (3, 0), (0, 1)))

    def ur(i, side):
        ref = up.at[at_z(relayed[side][i]), at_y(-fwd[side]), c]
        return same(ref, left_s.at[2], ur_r.at[0 if (i, side) in relays[0] else 1], y_to[side])

    def u_core(i):
        ref = up.at[:, at_y((0, 1, -1, 2)[i]), c]
        return same(ref, left_s.at[6], core_r.at[0], partner)

    def u_step(step):
        for side in (0, 1):
            uz_in(step, side).wait_recv()
            if step < nz // 2:
                go(uz(step + 1, side))

    def u_turn(step):
        offs = (-step, step) if step < nz // 2 else (step,)
        for off in offs:
            for side in (0, 1):
                go(uy(off, side))
        if step == nz // 2:
            go(u_core(0))

    def u_relay(*which):
        for i, side in which:
            uy_in(relayed[side][i], side).wait_recv()
            go(ur(i, side))

    def u_rest():
        for side in (0, 1):
            wait_all(up.at[pl.ds(0, 4), 0, 0], uy_r.at[side, 4])
        go(u_core(1))
        go(u_core(2))

    def u_last(group):
        wait_all(up.at[pl.ds(0, 4), 0, 0], ur_r.at[group])
        for i, side in relays[group]:
            go(same(up.at[at_z(relayed[side][i]), at_y(2), c], left_s.at[6], core_r.at[0], partner))

    def u_done():
        wait_all(up.at[:, :, 0], core_r.at[0])

    by_distance = (0, 1, -1, 2, -2, 3, -3, 4)
    early = 5

    def dy(step, side):
        ref = down.at[z, at_y(-fwd[side] * (step - 1)), c]
        if step == 2:
            ref = ref.at[halves[side]]
        return same(ref, left_s.at[3], dy_r.at[side, step - 1], y_to[side])

    def dy_in(step, side):
        ref = down.at[z, at_y(-fwd[side] * step), c]
        if step == 2:
            ref = ref.at[halves[side]]
        return same(ref, left_s.at[3], dy_r.at[side, step - 1], y_to[side])

    columns_y = (0, 1, -1, 2)
    last_by = ((0, 3), (2, 1))

    def dz(step, side, g):
        ref = down.at[at_z(-fwd[side] * (step - 1)), at_y(columns_y[g]), c]
        return same(ref, left_s.at[4], dz_r.at[side, step - 1, g], z_to[side])

    def dz_in(step, side, g):
        ref = down.at[at_z(-fwd[side] * step), at_y(columns_y[g]), c]
        return same(ref, left_s.at[4], dz_r.at[side, step - 1, g], z_to[side])

    def d_core(k):
        return same(down.at[at_z(k), :, c], left_s.at[6], core_r.at[2 if k in by_distance[:early] else 3], partner)

    def d_own():
        for side in (0, 1):
            go(dy(1, side))

    def d_turn():
        for side in (0, 1):
            dy_in(1, side).wait_recv()
            go(dy(2, side))

    def d_column():
        for side in (0, 1):
            dy_in(2, side).wait_recv()
        go(d_core(0))

    def d_send(*gs):
        for side in (0, 1):
            for g in gs:
                go(dz(1, side, g))

    def d_step(step, *gs):
        for g in gs:
            for side in (0, 1):
                if step < nz // 2:
                    dz_in(step, side, g).wait_recv()
                    if step + 1 < nz // 2 or g in last_by[side]:
                        go(dz(step + 1, side, g))
                elif g in last_by[side]:
                    dz_in(step, side, g).wait_recv()

    def d_cores(step):
        go(d_core(step))
        if step < nz // 2:
            go(d_core(-step))

    deep = wo.shape[2]
    wo_halves = (pl.ds(0, deep // 2), pl.ds(deep // 2, deep // 2))

    def wx(step, side):
        ref = wo.at[at_x(-fwd[side] if step == 2 else 0), c].at[wo_halves[1 - side if step == 1 else side]]
        return same(ref, left_s.at[5], wo_r.at[side, step], x_to[side])

    def wx_in(step, side):
        ref = wo.at[at_x(-fwd[side] * (2 if step == 2 else 1)), c].at[wo_halves[1 - side if step == 1 else side]]
        return same(ref, left_s.at[5], wo_r.at[side, step], x_to[side])

    def w_core(i):
        return same(wo.at[at_x(i + 1), c], left_s.at[5], core_r.at[1], partner)

    def w_turn():
        for side in (0, 1):
            wx_in(0, side).wait_recv()
            go(wx(2, side))

    def w_near():
        for side in (0, 1):
            wx_in(1, side).wait_recv()
        go(w_core(0))
        go(w_core(2))

    def w_last():
        for side in (0, 1):
            wx_in(2, side).wait_recv()
        go(w_core(1))

    def w_done():
        wait_all(wo.at[pl.ds(0, nx - 1), 0], core_r.at[1])

    for load in loads[:4]:
        load.wait()

    decays[...] = jnp.zeros_like(decays)
    for b in range(blocks):
        cut = pl.ds(b * BLOCK, BLOCK)
        decays[pl.ds(3 * b, 1), :] = dw[:, cut]
        decays[pl.ds(3 * b + 1, 2), :] = dn[:, cut]
    running = decays[0:32, :]
    shift = 1
    while shift < BLOCK:
        running = running + jnp.where(lane >= shift, pltpu.roll(running, shift, 1), 0.0)
        shift *= 2
    decays[0:32, :] = running
    columns = jnp.transpose(decays[...])

    at_t = lax.broadcasted_iota(jnp.int32, (BLOCK, BLOCK), 0)
    at_s = lax.broadcasted_iota(jnp.int32, (BLOCK, BLOCK), 1)
    lower = at_t >= at_s
    same_head = (at_t < HDN) == (at_s < HDN)

    def spread(r):
        steps = jnp.minimum(columns[:, r : r + 1] - decays[pl.ds(r, 1), :], 0.0)
        return jnp.where(lower, jnp.exp(steps), 0.0)

    def angles(b):
        cos_w, sin_w = turn(base[0][0][b : b + 1], base[0][1][b : b + 1], tt[0], tt[1])
        cos_n, sin_n = turn(base[1][0][b : b + 1], base[1][1][b : b + 1], tt[2], tt[3])
        return cos_w, sin_w * sign_w, cos_n, sin_n * sign_n

    def rotate_w(a, cos, sin):
        return a * cos + pltpu.roll(a, HDW // 2, 1) * sin

    def rotate_n(a, cos, sin):
        other = jnp.where(front_n, pltpu.roll(a, 128 - HDN // 2, 1), pltpu.roll(a, HDN // 2, 1))
        return a * cos + other * sin

    def ends(b):
        r = 3 * b
        now = [columns[:, r + h : r + h + 1] for h in range(3)]
        return now, [columns[BLOCK - 1 : BLOCK, r + h : r + h + 1] for h in range(3)]

    state_w = jnp.zeros((128, 128), F32)
    state_n = jnp.zeros((128, 128), F32)
    gone = [jnp.zeros((1, 1), F32)] * 3
    before_block = []
    for b in range(blocks):
        cut = pl.ds(b * BLOCK, BLOCK)
        now, last = ends(b)
        cos_w, sin_w, cos_n, sin_n = angles(b)
        st_w[b] = state_w.astype(BF16)
        st_n[b] = state_n.astype(BF16)
        before_block.append(gone)
        k = rotate_w(kw[cut, :].astype(F32), cos_w, sin_w) * HDW**-0.5
        k_w[cut, :] = k.astype(BF16)
        tail = k * jnp.exp(last[0] - now[0])
        state_w = jnp.exp(last[0]) * state_w + tdot(tail.astype(BF16), vw[cut, :])
        k = rotate_n(kn[cut, :].astype(F32), cos_n, sin_n) * HDN**-0.5
        k_n[cut, :] = k.astype(BF16)
        tail = k * jnp.where(low, jnp.exp(last[1] - now[1]), jnp.exp(last[2] - now[2]))
        keep = jnp.where(low, jnp.exp(last[1]), jnp.exp(last[2]))
        state_n = keep * state_n + jnp.where(same_head, tdot(tail.astype(BF16), vn[cut, :]), 0.0)
        gone = [g + t for g, t in zip(gone, last)]

    def outputs(b):
        cut = pl.ds(b * BLOCK, BLOCK)
        r = 3 * b
        now, last = ends(b)
        cos_w, sin_w, cos_n, sin_n = angles(b)
        gone = before_block[b]
        q = rotate_w(qw[cut, :].astype(F32), cos_w, sin_w)
        scores = dot_t(q.astype(BF16), k_w[cut, :]) * spread(r)
        out_b = dot(scores.astype(BF16), vw[cut, :])
        if b:
            out_b += dot((q * jnp.exp(now[0])).astype(BF16), st_w[b])
        o_w[cut, :] = out_b
        qe_w[cut, :] = (q * jnp.exp(now[0] + gone[0])).astype(BF16)
        q = rotate_n(qn[cut, :].astype(F32), cos_n, sin_n)
        probs = []
        for h, mask in enumerate((low, jnp.logical_not(low))):
            qh = jnp.where(mask, q, 0.0).astype(BF16)
            probs.append((dot_t(qh, k_n[cut, :]) * spread(r + 1 + h)).astype(BF16))
        v_f = vn[cut, :].astype(F32)
        v2 = jnp.concatenate(
            [jnp.where(low, v_f, 0.0).astype(BF16), jnp.where(low, 0.0, v_f).astype(BF16)], axis=0
        )
        out_b = dot(jnp.concatenate(probs, axis=1), v2)
        if b:
            seen = jnp.where(low, jnp.exp(now[1]), jnp.exp(now[2]))
            out_b += dot((q * seen).astype(BF16), st_n[b])
        o_n[cut, :] = out_b
        seen = jnp.where(low, jnp.exp(now[1] + gone[1]), jnp.exp(now[2] + gone[2]))
        qe_n[cut, :] = (q * seen).astype(BF16)

    total_w = jnp.exp(gone[0]) + jnp.zeros((1, 128), F32)
    total_n = jnp.where(low, jnp.exp(gone[1]), jnp.exp(gone[2]))
    packed_n = jnp.where(low, state_n[:HDN], state_n[HDN:])
    sw, sn = 128 // plane, HDN // plane
    part_of = lax.broadcasted_iota(jnp.int32, (8, 128), 0)

    def message(state, rate_w, rate_n):
        parts = jnp.zeros((8, 128), F32)
        for r, rate in ((0, rate_w), (2, rate_n)):
            high = rate.astype(BF16).astype(F32)
            parts = jnp.where(part_of == r, high, jnp.where(part_of == r + 1, rate - high, parts))
        return jnp.concatenate([state, parts], axis=0).astype(BF16)

    for j in range(plane):
        state = [state_w[sw * j : sw * (j + 1)], packed_n[sn * j : sn * (j + 1)]]
        msg[j] = message(jnp.concatenate(state, axis=0), total_w, total_n)
    ns = sw + sn

    def stage1(d):
        to = lax.rem(me + d, plane)
        return remote(msg.at[to], in1.at[me], left_s.at[10], s1_r, at_plane(to))

    pl.semaphore_wait(barrier, len(peers))
    for d in range(1, plane):
        stage1(d).start()
    for load in loads[4:10]:
        load.wait()
    for side in (0, 1):
        go(uz(1, side))
        go(wx(0, side))
    d_own()
    for side in (0, 1):
        go(wx(1, side))
    in1[pl.ds(me, 1)] = msg[pl.ds(me, 1)]
    for b in range(blocks // 2):
        outputs(b)

    wait_all(msg.at[pl.ds(0, plane - 1)], s1_r)
    wide_row = lax.broadcasted_iota(jnp.int32, (ns, 128), 0) < sw

    def factor(pair):
        return jnp.where(wide_row, pair[0], pair[1])

    def opened(ref, j):
        whole = ref[j].astype(F32)
        return whole[0:ns], (whole[ns : ns + 1] + whole[ns + 1 : ns + 2], whole[ns + 2 : ns + 3] + whole[ns + 3 : ns + 4])

    before = []
    held = jnp.zeros((ns, 128), F32)
    rate = (jnp.ones((1, 128), F32), jnp.ones((1, 128), F32))
    for j in range(plane):
        before.append((held, rate))
        state, mine = opened(in1, j)
        held = held * factor(mine) + state
        rate = (rate[0] * mine[0], rate[1] * mine[1])
    tot2[...] = message(held, *rate)

    def stage2(d):
        return remote(tot2, in2.at[z], left_s.at[11], s2_r, {"z": lax.rem(z + d, nz)})

    for d in range(1, nz):
        stage2(d).start()
    for side in (0, 1):
        go(uy(0, side))
    d_send(0)
    for b in range(blocks // 2, blocks):
        outputs(b)
    u_step(1)
    d_turn()
    d_send(1)
    w_turn()
    in2[pl.ds(z, 1)] = tot2[...][None]
    wait_all(in2.at[pl.ds(0, nz - 1)], s2_r)
    held = jnp.zeros((ns, 128), F32)
    for k in range(nz):
        state, mine = opened(in2, k)
        later = held * factor(mine) + state
        held = jnp.where(k < z, later, held)
    for j in range(plane):
        state, rate = before[j]
        state = held * factor(rate) + state
        msg3[j] = jnp.concatenate([state, jnp.zeros((8, 128), F32)], axis=0).astype(BF16)

    def stage3(d):
        to = lax.rem(me + d, plane)
        return remote(msg3.at[to], in3.at[me], left_s.at[12], s3_r, at_plane(to))

    for d in range(1, plane):
        stage3(d).start()
    in3[pl.ds(me, 1)] = msg3[pl.ds(me, 1)]
    u_turn(1)
    u_relay((0, 0))
    d_column()
    u_step(2)
    u_turn(2)
    d_send(2)
    w_near()
    for load in loads[10:]:
        load.wait()
    wait_all(msg.at[pl.ds(0, plane - 1)], s3_r)
    arrived = in3[...].astype(F32)
    enter_w = arrived[:, 0:sw, :].reshape(128, 128).astype(BF16)
    enter_p = arrived[:, sw:ns, :].reshape(HDN, 128)
    enter_n = jnp.concatenate(
        [jnp.where(low, enter_p, 0.0), jnp.where(low, 0.0, enter_p)], axis=0
    ).astype(BF16)

    def mixed_to(d):
        to = lax.rem(x + d, nx)
        return remote(mixed.at[to], mix_in.at[x], left_s.at[7], mx_r, {"x": to})

    def gated(o, gate):
        return (o * jax.nn.silu(gate.astype(F32))).astype(BF16)

    for d in (2, 1, 3, 0):
        i = lax.rem(x + d, nx)
        cut = pl.ds(pl.multiple_of(i * rows, rows), rows)
        o = o_w[cut, :] + dot(qe_w[cut, :], enter_w)
        o = o - jnp.mean(o, axis=-1, keepdims=True)
        o = o * lax.rsqrt(jnp.mean(o * o, axis=-1, keepdims=True) + head_eps)
        mixed[i, :, 0:128] = gated(o, gw[cut, :])
        o = o_n[cut, :] + dot(qe_n[cut, :], enter_n)

        def by_head(a):
            first = jnp.sum(jnp.where(low, a, 0.0), axis=-1, keepdims=True)
            second = jnp.sum(jnp.where(low, 0.0, a), axis=-1, keepdims=True)
            return jnp.where(low, first, second) * (1.0 / HDN)

        o = o - by_head(o)
        o = o * lax.rsqrt(by_head(o * o) + head_eps)
        mixed[i, :, 128:256] = gated(o, gn[cut, :])
        if d:
            go(mixed_to(d))

    mix_in[pl.ds(x, 1)] = mixed[pl.ds(x, 1)]

    u_relay((1, 1))
    u_step(3)
    u_turn(3)
    d_send(3)
    d_step(1, 0, 1)
    u_relay((1, 0))
    w_last()
    w_done()
    wait_all(mixed.at[pl.ds(0, nx - 1)], mx_r)

    tile = 512
    tiles = width // tile

    def project(n, squares):
        at = pl.ds(pl.multiple_of(n * tile, tile), tile)
        total = stream[:, at].astype(F32)
        for j in range(nx):
            total += dot(mix_in[j], wo[j, :, :, at].reshape(2 * deep, tile))
        total = total.astype(BF16)
        middle[:, at] = total
        total = total.astype(F32)
        return squares + jnp.sum(total * total, axis=-1, keepdims=True)

    squares = lax.fori_loop(0, tiles, project, jnp.zeros((rows, 1), F32))
    scale = lax.rsqrt(squares * (1.0 / width) + norm_eps)
    normed[pl.ds(x, 1)] = (middle[...].astype(F32) * scale * gain[...].astype(F32).reshape(1, width)).astype(BF16)[None]

    def nx_rows(piece, side):
        if piece == 4:
            return pl.ds((1 - side) * half_rows, half_rows)
        return pl.ds(side * half_rows + piece % 2 * part_rows, part_rows)

    def nm(piece, side):
        ref = normed.at[at_x(-fwd[side] if piece in (2, 3) else 0), nx_rows(piece, side)]
        return same(ref, left_s.at[8], st_r.at[side, piece], x_to[side])

    def nm_in(piece, side):
        ref = normed.at[at_x(-fwd[side] * (2 if piece in (2, 3) else 1)), nx_rows(piece, side)]
        return same(ref, left_s.at[8], st_r.at[side, piece], x_to[side])

    def nm_on(piece):
        for side in (0, 1):
            nm_in(piece, side).wait_recv()
            go(nm(piece + 2, side))

    for piece in (0, 1):
        for side in (0, 1):
            go(nm(piece, side))

    u_step(4)
    u_turn(4)
    u_relay((2, 1))
    d_step(1, 2)
    d_step(1, 3)
    d_cores(1)
    u_relay((2, 0))
    d_step(2, 0)
    u_relay((3, 1))
    d_step(2, 1)
    nm_on(0)
    u_relay((3, 0))
    d_step(2, 2)
    nm_on(1)
    u_last(0)
    for side in (0, 1):
        go(nm(4, side))
    u_relay((0, 1))
    d_step(2, 3)
    d_cores(2)
    u_rest()
    d_step(3, 0)
    u_last(1)
    d_step(3, 1)
    u_done()

    near_rows = ((xl, 0, xr, 1), (xo, 0, xo, 1), (xr, 0, xl, 1), (x, 0, x, 1))
    EARLY, FAR, LATE, OWN = range(4)

    def rise(batch):
        slot_a, half_a, slot_b, half_b = near_rows[batch]

        def one(n, _):
            at = pl.ds(pl.multiple_of(n * tile, tile), tile)
            a = normed[slot_a, half_a * half_rows : (half_a + 1) * half_rows]
            b = normed[slot_b, half_b * half_rows : (half_b + 1) * half_rows]
            h = dot(jnp.concatenate([a, b], axis=0), up[:, :, :, :, at].reshape(width, tile))
            h = jnp.maximum(h, 0.0)
            hidden[batch, :, at] = (h * h).astype(BF16)
            return 0

        lax.fori_loop(0, tiles, one, 0)

    span = width // nz
    blocks_of = (by_distance[:early], by_distance[early:])
    lanes_of = (pl.ds(0, early * span), pl.ds(early * span, width - early * span))

    first, second = slice(0, half_rows), slice(half_rows, rows)

    def fall(batch, half, put):
        for n, k in enumerate(blocks_of[half]):
            at = (half * early + n) * span
            put(slice(at, at + span), dot_t(hidden[batch], down[at_z(k)].reshape(span, width)))

    def put_far(at, piece):
        send2[:, at] = piece.astype(BF16)

    def put_early(at, piece):
        sendm[first, at] = piece[first].astype(BF16)
        send1[second, at] = piece[second].astype(BF16)

    def put_late(at, piece):
        hold[0, :, at] = piece[first]
        hold[1, :, at] = piece[second]

    def put_own(at, piece):
        own[:, at] = piece

    got_l, got_r = got_both.at[0], got_both.at[1]
    row_halves = (pl.ds(0, half_rows), pl.ds(half_rows, half_rows))

    def far(half, side):
        to = (relay_l, relay_r)[side].at[:, lanes_of[half]]
        return remote(send2.at[row_halves[side], lanes_of[half]], to, left_s.at[9], rs_r.at[2 * half + side], x_to[side])

    def near(half, side, summed):
        at = (row_halves[side if summed else 1 - side], lanes_of[half])
        source, to = ((send1, got_l), (sendm, got_r))[side]
        return remote(source.at[at], to.at[at], left_s.at[9], rs_r.at[4 + half], x_to[side])

    def add_far(half):
        at = lanes_of[half]
        far(half, 0).wait_recv()
        send1[first, at] = (hold[0, :, at] + relay_l[:, at].astype(F32)).astype(BF16)
        go(near(half, 0, 1))
        far(half, 1).wait_recv()
        sendm[second, at] = (hold[1, :, at] + relay_r[:, at].astype(F32)).astype(BF16)
        go(near(half, 1, 1))

    rise(EARLY)
    d_step(3, 2)
    wait_all(down.at[pl.ds(0, early), :, 0], core_r.at[2])
    fall(EARLY, 0, put_early)
    for side in (0, 1):
        go(near(0, side, 0))
    for side in (0, 1):
        nm_in(2, side).wait_recv()
        nm_in(3, side).wait_recv()
    d_step(3, 3)
    d_cores(3)
    rise(FAR)
    fall(FAR, 0, put_far)
    for side in (0, 1):
        go(far(0, side))
    d_step(4, 0, 1, 2, 3)
    d_cores(4)
    for side in (0, 1):
        nm_in(4, side).wait_recv()
    rise(LATE)
    fall(LATE, 0, put_late)
    wait_all(down.at[pl.ds(0, nz - early), :, 0], core_r.at[3])
    fall(EARLY, 1, put_early)
    for side in (0, 1):
        go(near(1, side, 0))
    fall(FAR, 1, put_far)
    for side in (0, 1):
        go(far(1, side))
    add_far(0)
    fall(LATE, 1, put_late)
    rise(OWN)
    add_far(1)
    fall(OWN, 0, put_own)
    fall(OWN, 1, put_own)
    for half in (0, 1):
        at = lanes_of[half]
        wait_all(got_both.at[:, :, at], rs_r.at[4 + half])
        total = own[:, at] + got_l[:, at].astype(F32) + got_r[:, at].astype(F32)
        for n, k in enumerate(blocks_of[half]):
            at = pl.ds(pl.multiple_of(at_z(k) * span, span), span)
            result[:, at] = (middle[:, at].astype(F32) + total[:, n * span : (n + 1) * span]).astype(BF16)
            go(pltpu.make_async_copy(result.at[:, at], out.at[:, at], out_s))

    totals = (
        up.at[pl.ds(0, nz - 1), 0, 0], up.at[:, pl.ds(0, 2), 0], up.at[:, 0, 0], down.at[pl.ds(0, 3), 0, 0],
        down.at[pl.ds(0, nz - 1), :, 0], wo.at[pl.ds(0, 3)], up, mixed.at[pl.ds(0, nx - 1)], normed.at[pl.ds(0, 3)],
        normed.at[pl.ds(0, 3)], msg.at[pl.ds(0, plane - 1)], in2.at[pl.ds(0, nz - 1)], msg.at[pl.ds(0, plane - 1)],
    )
    for i, total in enumerate(totals):
        wait_all(total, left_s.at[i])
    wait_all(out, out_s)


def on_device(
    sizes,
    stream_in, query_wide, key_wide, value_wide, gate_wide, decay_wide,
    query_narrow, key_narrow, value_narrow, gate_narrow, decay_narrow,
    output_wide, output_narrow, norm_gain, up_weight, down_weight,
):
    nz, ny, nc, nx = sizes
    tok = query_wide.shape[0]
    rows, width = stream_in.shape
    plane = ny * nc
    part, hid = up_weight.shape
    ns = (128 + HDN) // plane
    dma = pltpu.SemaphoreType.DMA
    vm = pltpu.VMEM
    scratch = [
        *[vm((tok, 128), BF16)] * 8, vm((rows, width), BF16),
        vm((nz, ny, nc, part, hid), BF16), vm((nz, ny, nc, part, hid), BF16), vm((nx, 2, *output_wide.shape), BF16),
        vm((tok, 128), BF16), vm((tok, 128), BF16), vm((tok, 128), F32), vm((tok, 128), F32),
        vm((128, 128), F32),
        vm((tok // BLOCK, 128, 128), BF16), vm((tok // BLOCK, 128, 128), BF16), vm((tok, 128), BF16), vm((tok, 128), BF16),
        vm((plane, ns + 8, 128), BF16), vm((plane, ns + 8, 128), BF16),
        vm((ns + 8, 128), BF16), vm((nz, ns + 8, 128), BF16),
        vm((plane, ns + 8, 128), BF16), vm((plane, ns + 8, 128), BF16),
        vm((nx, rows, 256), BF16), vm((nx, rows, 256), BF16),
        vm((rows, width), BF16), vm((nx, rows, width), BF16), vm((nx, rows, hid), BF16),
        vm((rows, width), BF16), vm((rows, width), BF16), vm((rows, width), BF16),
        vm((rows, width), F32), vm((2, rows // 2, width), F32), vm((rows, width), BF16),
        vm((rows // 2, width), BF16), vm((rows // 2, width), BF16), vm((2, rows, width), BF16),
        dma((13,)), dma((13,)), dma, dma((2, 5)), dma, dma, dma, dma, dma((6,)), dma((2, 3)), dma((2, 4)), dma((2, 5)),
        dma((2,)), dma((2, 2)), dma((2, 4, 4)), dma((4,)),
    ]
    vmem = pl.BlockSpec(memory_space=pltpu.VMEM)
    hbm = pl.BlockSpec(memory_space=pl.ANY)
    return pl.pallas_call(
        functools.partial(kernel, sizes),
        out_shape=jax.ShapeDtypeStruct((rows, width), BF16),
        in_specs=[vmem] * 6 + [hbm] * 13,
        out_specs=hbm,
        scratch_shapes=scratch,
        compiler_params=pltpu.CompilerParams(
            collective_id=0, has_side_effects=True, vmem_limit_bytes=60 * 1024 * 1024
        ),
    )(
        decay_wide, decay_narrow, norm_gain, jnp.asarray(rope_tables(BLOCK, 1)),
        jnp.asarray(rope_tables(8, BLOCK)), jnp.asarray(rope_tables(nz * plane, tok)),
        query_wide, key_wide, value_wide, query_narrow, key_narrow, value_narrow, gate_wide, gate_narrow, stream_in,
        output_wide, output_narrow, up_weight, down_weight.T,
    )


def solution(mesh):
    sizes = (8, 4, 2, mesh.shape["tp"])
    split = Mesh(mesh.devices.reshape(sizes), ("z", "y", "c", "x"))
    sp = ("z", "y", "c")
    rows, heads = P(sp, "x"), P("x", sp)
    in_specs = (
        P((*sp, "x"), None), rows, rows, rows, rows, heads, rows, rows, rows, rows, heads,
        P("x", None), P("x", None), P(), rows, heads,
    )
    return jax.shard_map(
        functools.partial(on_device, sizes), mesh=split, in_specs=in_specs,
        out_specs=P((*sp, "x"), None), check_vma=False,
    )
```

```python
import functools

import jax
import jax.numpy as jnp
import numpy as np
from jax import lax
from jax.experimental import pallas as pl
from jax.experimental.pallas import tpu as pltpu
from jax.sharding import Mesh
from jax.sharding import PartitionSpec as P

HDW = 128
HDN = 64
BLOCK = 128
head_eps = 1e-05
norm_eps = 1e-06
rope_base = 10000.0
MESH = pl.DeviceIdType.MESH
F32 = jnp.float32
BF16 = jnp.bfloat16


def rope_tables(steps, stride):
    tables = []
    for width in (HDW, HDN):
        half = width // 2
        inverse = rope_base ** (-np.arange(half, dtype=np.float64) / half)
        lanes = np.tile(inverse, 128 // half)
        angles = (stride * np.arange(steps, dtype=np.float64))[:, None] * lanes[None, :]
        tables += [np.cos(angles), np.sin(angles)]
    return np.stack(tables).astype(np.float32)


def remote(src, dst, send_sem, recv_sem, device):
    return pltpu.make_async_remote_copy(
        src_ref=src, dst_ref=dst, send_sem=send_sem, recv_sem=recv_sem, device_id=device, device_id_type=MESH
    )


def turn(cos_a, sin_a, cos_b, sin_b):
    return cos_a * cos_b - sin_a * sin_b, sin_a * cos_b + cos_a * sin_b


def dot(a, b):
    return jnp.dot(a, b, preferred_element_type=F32)


def dot_t(a, b):
    return lax.dot_general(a, b, (((1,), (1,)), ((), ())), preferred_element_type=F32)


def tdot(a, b):
    return lax.dot_general(a, b, (((0,), (0,)), ((), ())), preferred_element_type=F32)


def kernel(
    sizes,
    dw, dn, gain, tt, tb, ts,
    qw_in, kw_in, vw_in, qn_in, kn_in, vn_in, gw_in, gn_in, stream_in, ow, on, up_own, down_own,
    out,
    qw, kw, vw, qn, kn, vn, gw, gn, stream,
    up, down, wo,
    qe_w, qe_n, o_w, o_n, decays, st_w, st_n, k_w, k_n, msg, in1, tot2, in2, msg3, in3,
    mixed, mix_in, middle, normed, hidden, send2, send1, sendm, own, hold, result, relay_l, relay_r, got_both,
    left_s, in_s, out_s, st_r, s1_r, s2_r, s3_r, mx_r, rs_r, wo_r, uz_r, uy_r, ur_r, dy_r, dz_r, core_r,
):
    nz, ny, nc, nx = sizes
    z, y, c, x = (lax.axis_index(a) for a in ("z", "y", "c", "x"))
    xr, xl, xo = lax.rem(x + 1, nx), lax.rem(x + nx - 1, nx), lax.rem(x + 2, nx)
    plane = ny * nc
    me = y * nc + c
    sp = z * plane + me
    tok = qw.shape[0]
    blocks = tok // BLOCK
    rows = stream.shape[0]
    width = stream.shape[1]
    half_rows, part_rows = rows // 2, rows // 4
    right, left = {"x": xr}, {"x": xl}

    def at_plane(j):
        return {"y": j // nc, "c": lax.rem(j, nc)}

    barrier = pltpu.get_barrier_semaphore()
    peers = [right, left, {"x": xo}]
    peers += [at_plane(lax.rem(me + d, plane)) for d in range(1, plane)]
    peers += [{"z": lax.rem(z + d, nz)} for d in range(1, nz)]
    for peer in peers:
        pl.semaphore_signal(barrier, inc=1, device_id=peer, device_id_type=MESH)

    pairs = [
        (kw_in, kw), (vw_in, vw), (kn_in, kn), (vn_in, vn),
        (up_own, up.at[z, y, c]), (ow, wo.at[x, 0]), (on, wo.at[x, 1]), (down_own, down.at[z, y, c]),
        (qw_in, qw), (qn_in, qn), (gw_in, gw), (gn_in, gn), (stream_in, stream),
    ]
    loads = [pltpu.make_async_copy(a, b, in_s.at[i]) for i, (a, b) in enumerate(pairs)]
    for load in loads:
        load.start()

    lane = lax.broadcasted_iota(jnp.int32, (1, 128), 1)
    low = lane < HDN
    base = []
    for g in (0, 2):
        row = [ts[g + i, pl.ds(sp, 1), :] for i in (0, 1)]
        base.append(turn(row[0], row[1], tb[g], tb[g + 1]))
    sign_w = jnp.where(lane < HDW // 2, -1.0, 1.0)
    front_n = lax.rem(lane, HDN) < HDN // 2
    sign_n = jnp.where(front_n, -1.0, 1.0)

    def go(copy):
        copy.start()

    def wait_all(ref, sem):
        pltpu.make_async_copy(ref, ref, sem).wait()

    def same(ref, send_sem, recv_sem, device):
        return remote(ref, ref, send_sem, recv_sem, device)

    z_to = ({"z": lax.rem(z + 1, nz)}, {"z": lax.rem(z + nz - 1, nz)})
    y_to = ({"y": lax.rem(y + 1, ny)}, {"y": lax.rem(y + ny - 1, ny)})
    x_to = (right, left)
    partner = {"c": 1 - c}
    fwd = (1, -1)

    def at_z(k):
        return lax.rem(z + nz + k, nz)

    def at_y(k):
        return lax.rem(y + ny + k, ny)

    def at_x(k):
        return lax.rem(x + nx + k, nx)

    part = up.shape[3]
    halves = (pl.ds(0, part // 2), pl.ds(part // 2, part // 2))

    relayed = ((0, 1, 2, 3), (4, -1, -2, -3))

    def uz(step, side):
        ref = up.at[at_z(-fwd[side] * (step - 1)), y, c]
        if step == nz // 2:
            ref = ref.at[halves[side]]
        return same(ref, left_s.at[0], uz_r.at[side, step - 1], z_to[side])

    def uz_in(step, side):
        ref = up.at[at_z(-fwd[side] * step), y, c]
        if step == nz // 2:
            ref = ref.at[halves[side]]
        return same(ref, left_s.at[0], uz_r.at[side, step - 1], z_to[side])

    def uy(off, side):
        return same(up.at[at_z(off), y, c], left_s.at[1], uy_r.at[side, relayed[side].index(off) if off in relayed[side] else 4], y_to[side])

    def uy_in(off, side):
        ref = up.at[at_z(off), at_y(-fwd[side]), c]
        return same(ref, left_s.at[1], uy_r.at[side, relayed[side].index(off) if off in relayed[side] else 4], y_to[side])


    relays = (((0, 0), (1, 1), (1, 0), (2, 1)), ((2, 0), (3, 1), (3, 0), (0, 1)))

    def ur(i, side):
        ref = up.at[at_z(relayed[side][i]), at_y(-fwd[side]), c]
        return same(ref, left_s.at[2], ur_r.at[0 if (i, side) in relays[0] else 1], y_to[side])

    def u_core(i):
        ref = up.at[:, at_y((0, 1, -1, 2)[i]), c]
        return same(ref, left_s.at[6], core_r.at[0], partner)

    def u_step(step):
        for side in (0, 1):
            uz_in(step, side).wait_recv()
            if step < nz // 2:
                go(uz(step + 1, side))

    def u_turn(step):
        offs = (-step, step) if step < nz // 2 else (step,)
        for off in offs:
            for side in (0, 1):
                go(uy(off, side))
        if step == nz // 2:
            go(u_core(0))

    def u_relay(*which):
        for i, side in which:
            uy_in(relayed[side][i], side).wait_recv()
            go(ur(i, side))

    def u_rest():
        for side in (0, 1):
            wait_all(up.at[pl.ds(0, 4), 0, 0], uy_r.at[side, 4])
        go(u_core(1))
        go(u_core(2))

    def u_last(group):
        wait_all(up.at[pl.ds(0, 4), 0, 0], ur_r.at[group])
        for i, side in relays[group]:
            go(same(up.at[at_z(relayed[side][i]), at_y(2), c], left_s.at[6], core_r.at[0], partner))

    def u_done():
        wait_all(up.at[:, :, 0], core_r.at[0])

    by_distance = (0, 1, -1, 2, -2, 3, -3, 4)
    early = 5

    def dy(step, side):
        ref = down.at[z, at_y(-fwd[side] * (step - 1)), c]
        if step == 2:
            ref = ref.at[halves[side]]
        return same(ref, left_s.at[3], dy_r.at[side, step - 1], y_to[side])

    def dy_in(step, side):
        ref = down.at[z, at_y(-fwd[side] * step), c]
        if step == 2:
            ref = ref.at[halves[side]]
        return same(ref, left_s.at[3], dy_r.at[side, step - 1], y_to[side])

    columns_y = (0, 1, -1, 2)
    last_by = ((0, 3), (2, 1))

    def dz(step, side, g):
        ref = down.at[at_z(-fwd[side] * (step - 1)), at_y(columns_y[g]), c]
        return same(ref, left_s.at[4], dz_r.at[side, step - 1, g], z_to[side])

    def dz_in(step, side, g):
        ref = down.at[at_z(-fwd[side] * step), at_y(columns_y[g]), c]
        return same(ref, left_s.at[4], dz_r.at[side, step - 1, g], z_to[side])

    def d_core(k):
        return same(down.at[at_z(k), :, c], left_s.at[6], core_r.at[2 if k in by_distance[:early] else 3], partner)

    def d_own():
        for side in (0, 1):
            go(dy(1, side))

    def d_turn():
        for side in (0, 1):
            dy_in(1, side).wait_recv()
            go(dy(2, side))

    def d_column():
        for side in (0, 1):
            dy_in(2, side).wait_recv()
        go(d_core(0))

    def d_send(*gs):
        for side in (0, 1):
            for g in gs:
                go(dz(1, side, g))

    def d_step(step, *gs):
        for g in gs:
            for side in (0, 1):
                if step < nz // 2:
                    dz_in(step, side, g).wait_recv()
                    if step + 1 < nz // 2 or g in last_by[side]:
                        go(dz(step + 1, side, g))
                elif g in last_by[side]:
                    dz_in(step, side, g).wait_recv()

    def d_cores(step):
        go(d_core(step))
        if step < nz // 2:
            go(d_core(-step))

    deep = wo.shape[2]
    wo_halves = (pl.ds(0, deep // 2), pl.ds(deep // 2, deep // 2))

    def wx(step, side):
        ref = wo.at[at_x(-fwd[side] if step == 2 else 0), c].at[wo_halves[1 - side if step == 1 else side]]
        return same(ref, left_s.at[5], wo_r.at[side, step], x_to[side])

    def wx_in(step, side):
        ref = wo.at[at_x(-fwd[side] * (2 if step == 2 else 1)), c].at[wo_halves[1 - side if step == 1 else side]]
        return same(ref, left_s.at[5], wo_r.at[side, step], x_to[side])

    def w_core(i):
        return same(wo.at[at_x(i + 1), c], left_s.at[5], core_r.at[1], partner)

    def w_turn():
        for side in (0, 1):
            wx_in(0, side).wait_recv()
            go(wx(2, side))

    def w_near():
        for side in (0, 1):
            wx_in(1, side).wait_recv()
        go(w_core(0))
        go(w_core(2))

    def w_last():
        for side in (0, 1):
            wx_in(2, side).wait_recv()
        go(w_core(1))

    def w_done():
        wait_all(wo.at[pl.ds(0, nx - 1), 0], core_r.at[1])

    for load in loads[:4]:
        load.wait()

    decays[...] = jnp.zeros_like(decays)
    for b in range(blocks):
        cut = pl.ds(b * BLOCK, BLOCK)
        decays[pl.ds(3 * b, 1), :] = dw[:, cut]
        decays[pl.ds(3 * b + 1, 2), :] = dn[:, cut]
    running = decays[0:32, :]
    shift = 1
    while shift < BLOCK:
        running = running + jnp.where(lane >= shift, pltpu.roll(running, shift, 1), 0.0)
        shift *= 2
    decays[0:32, :] = running
    columns = jnp.transpose(decays[...])

    at_t = lax.broadcasted_iota(jnp.int32, (BLOCK, BLOCK), 0)
    at_s = lax.broadcasted_iota(jnp.int32, (BLOCK, BLOCK), 1)
    lower = at_t >= at_s
    same_head = (at_t < HDN) == (at_s < HDN)

    def spread(r):
        steps = jnp.minimum(columns[:, r : r + 1] - decays[pl.ds(r, 1), :], 0.0)
        return jnp.where(lower, jnp.exp(steps), 0.0)

    def angles(b):
        cos_w, sin_w = turn(base[0][0][b : b + 1], base[0][1][b : b + 1], tt[0], tt[1])
        cos_n, sin_n = turn(base[1][0][b : b + 1], base[1][1][b : b + 1], tt[2], tt[3])
        return cos_w, sin_w * sign_w, cos_n, sin_n * sign_n

    def rotate_w(a, cos, sin):
        return a * cos + pltpu.roll(a, HDW // 2, 1) * sin

    def rotate_n(a, cos, sin):
        other = jnp.where(front_n, pltpu.roll(a, 128 - HDN // 2, 1), pltpu.roll(a, HDN // 2, 1))
        return a * cos + other * sin

    def ends(b):
        r = 3 * b
        now = [columns[:, r + h : r + h + 1] for h in range(3)]
        return now, [columns[BLOCK - 1 : BLOCK, r + h : r + h + 1] for h in range(3)]

    state_w = jnp.zeros((128, 128), F32)
    state_n = jnp.zeros((128, 128), F32)
    gone = [jnp.zeros((1, 1), F32)] * 3
    before_block = []
    for b in range(blocks):
        cut = pl.ds(b * BLOCK, BLOCK)
        now, last = ends(b)
        cos_w, sin_w, cos_n, sin_n = angles(b)
        st_w[b] = state_w.astype(BF16)
        st_n[b] = state_n.astype(BF16)
        before_block.append(gone)
        k = rotate_w(kw[cut, :].astype(F32), cos_w, sin_w) * HDW**-0.5
        k_w[cut, :] = k.astype(BF16)
        tail = k * jnp.exp(last[0] - now[0])
        state_w = jnp.exp(last[0]) * state_w + tdot(tail.astype(BF16), vw[cut, :])
        k = rotate_n(kn[cut, :].astype(F32), cos_n, sin_n) * HDN**-0.5
        k_n[cut, :] = k.astype(BF16)
        tail = k * jnp.where(low, jnp.exp(last[1] - now[1]), jnp.exp(last[2] - now[2]))
        keep = jnp.where(low, jnp.exp(last[1]), jnp.exp(last[2]))
        state_n = keep * state_n + jnp.where(same_head, tdot(tail.astype(BF16), vn[cut, :]), 0.0)
        gone = [g + t for g, t in zip(gone, last)]

    def outputs(b):
        cut = pl.ds(b * BLOCK, BLOCK)
        r = 3 * b
        now, last = ends(b)
        cos_w, sin_w, cos_n, sin_n = angles(b)
        gone = before_block[b]
        q = rotate_w(qw[cut, :].astype(F32), cos_w, sin_w)
        scores = dot_t(q.astype(BF16), k_w[cut, :]) * spread(r)
        out_b = dot(scores.astype(BF16), vw[cut, :])
        if b:
            out_b += dot((q * jnp.exp(now[0])).astype(BF16), st_w[b])
        o_w[cut, :] = out_b
        qe_w[cut, :] = (q * jnp.exp(now[0] + gone[0])).astype(BF16)
        q = rotate_n(qn[cut, :].astype(F32), cos_n, sin_n)
        probs = []
        for h, mask in enumerate((low, jnp.logical_not(low))):
            qh = jnp.where(mask, q, 0.0).astype(BF16)
            probs.append((dot_t(qh, k_n[cut, :]) * spread(r + 1 + h)).astype(BF16))
        v_f = vn[cut, :].astype(F32)
        v2 = jnp.concatenate(
            [jnp.where(low, v_f, 0.0).astype(BF16), jnp.where(low, 0.0, v_f).astype(BF16)], axis=0
        )
        out_b = dot(jnp.concatenate(probs, axis=1), v2)
        if b:
            seen = jnp.where(low, jnp.exp(now[1]), jnp.exp(now[2]))
            out_b += dot((q * seen).astype(BF16), st_n[b])
        o_n[cut, :] = out_b
        seen = jnp.where(low, jnp.exp(now[1] + gone[1]), jnp.exp(now[2] + gone[2]))
        qe_n[cut, :] = (q * seen).astype(BF16)

    total_w = jnp.exp(gone[0]) + jnp.zeros((1, 128), F32)
    total_n = jnp.where(low, jnp.exp(gone[1]), jnp.exp(gone[2]))
    packed_n = jnp.where(low, state_n[:HDN], state_n[HDN:])
    sw, sn = 128 // plane, HDN // plane
    part_of = lax.broadcasted_iota(jnp.int32, (8, 128), 0)

    def message(state, rate_w, rate_n):
        parts = jnp.zeros((8, 128), F32)
        for r, rate in ((0, rate_w), (2, rate_n)):
            high = rate.astype(BF16).astype(F32)
            parts = jnp.where(part_of == r, high, jnp.where(part_of == r + 1, rate - high, parts))
        return jnp.concatenate([state, parts], axis=0).astype(BF16)

    for j in range(plane):
        state = [state_w[sw * j : sw * (j + 1)], packed_n[sn * j : sn * (j + 1)]]
        msg[j] = message(jnp.concatenate(state, axis=0), total_w, total_n)
    ns = sw + sn

    def stage1(d):
        to = lax.rem(me + d, plane)
        return remote(msg.at[to], in1.at[me], left_s.at[10], s1_r, at_plane(to))

    pl.semaphore_wait(barrier, len(peers))
    for d in range(1, plane):
        stage1(d).start()
    for load in loads[4:10]:
        load.wait()
    for side in (0, 1):
        go(uz(1, side))
        go(wx(0, side))
    d_own()
    for side in (0, 1):
        go(wx(1, side))
    in1[pl.ds(me, 1)] = msg[pl.ds(me, 1)]
    for b in range(blocks // 2):
        outputs(b)

    wait_all(msg.at[pl.ds(0, plane - 1)], s1_r)
    wide_row = lax.broadcasted_iota(jnp.int32, (ns, 128), 0) < sw

    def factor(pair):
        return jnp.where(wide_row, pair[0], pair[1])

    def opened(ref, j):
        whole = ref[j].astype(F32)
        return whole[0:ns], (whole[ns : ns + 1] + whole[ns + 1 : ns + 2], whole[ns + 2 : ns + 3] + whole[ns + 3 : ns + 4])

    before = []
    held = jnp.zeros((ns, 128), F32)
    rate = (jnp.ones((1, 128), F32), jnp.ones((1, 128), F32))
    for j in range(plane):
        before.append((held, rate))
        state, mine = opened(in1, j)
        held = held * factor(mine) + state
        rate = (rate[0] * mine[0], rate[1] * mine[1])
    tot2[...] = message(held, *rate)

    def stage2(d):
        return remote(tot2, in2.at[z], left_s.at[11], s2_r, {"z": lax.rem(z + d, nz)})

    for d in range(1, nz):
        stage2(d).start()
    for side in (0, 1):
        go(uy(0, side))
    d_send(0)
    for b in range(blocks // 2, blocks):
        outputs(b)
    u_step(1)
    d_turn()
    d_send(1)
    w_turn()
    in2[pl.ds(z, 1)] = tot2[...][None]
    wait_all(in2.at[pl.ds(0, nz - 1)], s2_r)
    held = jnp.zeros((ns, 128), F32)
    for k in range(nz):
        state, mine = opened(in2, k)
        later = held * factor(mine) + state
        held = jnp.where(k < z, later, held)
    for j in range(plane):
        state, rate = before[j]
        state = held * factor(rate) + state
        msg3[j] = jnp.concatenate([state, jnp.zeros((8, 128), F32)], axis=0).astype(BF16)

    def stage3(d):
        to = lax.rem(me + d, plane)
        return remote(msg3.at[to], in3.at[me], left_s.at[12], s3_r, at_plane(to))

    for d in range(1, plane):
        stage3(d).start()
    in3[pl.ds(me, 1)] = msg3[pl.ds(me, 1)]
    u_turn(1)
    u_relay((0, 0))
    d_column()
    u_step(2)
    u_turn(2)
    d_send(2)
    w_near()
    for load in loads[10:]:
        load.wait()
    wait_all(msg.at[pl.ds(0, plane - 1)], s3_r)
    arrived = in3[...].astype(F32)
    enter_w = arrived[:, 0:sw, :].reshape(128, 128).astype(BF16)
    enter_p = arrived[:, sw:ns, :].reshape(HDN, 128)
    enter_n = jnp.concatenate(
        [jnp.where(low, enter_p, 0.0), jnp.where(low, 0.0, enter_p)], axis=0
    ).astype(BF16)

    def mixed_to(d):
        to = lax.rem(x + d, nx)
        return remote(mixed.at[to], mix_in.at[x], left_s.at[7], mx_r, {"x": to})

    def gated(o, gate):
        return (o * jax.nn.silu(gate.astype(F32))).astype(BF16)

    for d in (2, 1, 3, 0):
        i = lax.rem(x + d, nx)
        cut = pl.ds(pl.multiple_of(i * rows, rows), rows)
        o = o_w[cut, :] + dot(qe_w[cut, :], enter_w)
        o = o - jnp.mean(o, axis=-1, keepdims=True)
        o = o * lax.rsqrt(jnp.mean(o * o, axis=-1, keepdims=True) + head_eps)
        mixed[i, :, 0:128] = gated(o, gw[cut, :])
        o = o_n[cut, :] + dot(qe_n[cut, :], enter_n)

        def by_head(a):
            first = jnp.sum(jnp.where(low, a, 0.0), axis=-1, keepdims=True)
            second = jnp.sum(jnp.where(low, 0.0, a), axis=-1, keepdims=True)
            return jnp.where(low, first, second) * (1.0 / HDN)

        o = o - by_head(o)
        o = o * lax.rsqrt(by_head(o * o) + head_eps)
        mixed[i, :, 128:256] = gated(o, gn[cut, :])
        if d:
            go(mixed_to(d))

    mix_in[pl.ds(x, 1)] = mixed[pl.ds(x, 1)]

    u_relay((1, 1))
    u_step(3)
    u_turn(3)
    d_send(3)
    d_step(1, 0, 1)
    u_relay((1, 0))
    w_last()
    w_done()
    wait_all(mixed.at[pl.ds(0, nx - 1)], mx_r)

    tile = 512
    tiles = width // tile

    def project(n, squares):
        at = pl.ds(pl.multiple_of(n * tile, tile), tile)
        total = stream[:, at].astype(F32)
        for j in range(nx):
            total += dot(mix_in[j], wo[j, :, :, at].reshape(2 * deep, tile))
        total = total.astype(BF16)
        middle[:, at] = total
        total = total.astype(F32)
        return squares + jnp.sum(total * total, axis=-1, keepdims=True)

    squares = lax.fori_loop(0, tiles, project, jnp.zeros((rows, 1), F32))
    scale = lax.rsqrt(squares * (1.0 / width) + norm_eps)
    normed[pl.ds(x, 1)] = (middle[...].astype(F32) * scale * gain[...].astype(F32).reshape(1, width)).astype(BF16)[None]

    def nx_rows(piece, side):
        if piece == 4:
            return pl.ds((1 - side) * half_rows, half_rows)
        return pl.ds(side * half_rows + piece % 2 * part_rows, part_rows)

    def nm(piece, side):
        ref = normed.at[at_x(-fwd[side] if piece in (2, 3) else 0), nx_rows(piece, side)]
        return same(ref, left_s.at[8], st_r.at[side, piece], x_to[side])

    def nm_in(piece, side):
        ref = normed.at[at_x(-fwd[side] * (2 if piece in (2, 3) else 1)), nx_rows(piece, side)]
        return same(ref, left_s.at[8], st_r.at[side, piece], x_to[side])

    def nm_on(piece):
        for side in (0, 1):
            nm_in(piece, side).wait_recv()
            go(nm(piece + 2, side))

    for piece in (0, 1):
        for side in (0, 1):
            go(nm(piece, side))

    u_step(4)
    u_turn(4)
    u_relay((2, 1))
    d_step(1, 2)
    d_step(1, 3)
    d_cores(1)
    u_relay((2, 0))
    d_step(2, 0)
    u_relay((3, 1))
    d_step(2, 1)
    nm_on(0)
    u_relay((3, 0))
    d_step(2, 2)
    nm_on(1)
    u_last(0)
    for side in (0, 1):
        go(nm(4, side))
    u_relay((0, 1))
    d_step(2, 3)
    d_cores(2)
    u_rest()
    d_step(3, 0)
    u_last(1)
    d_step(3, 1)
    u_done()

    near_rows = ((xl, 0, xr, 1), (xo, 0, xo, 1), (xr, 0, xl, 1), (x, 0, x, 1))
    EARLY, FAR, LATE, OWN = range(4)

    def rise(batch):
        slot_a, half_a, slot_b, half_b = near_rows[batch]

        def one(n, _):
            at = pl.ds(pl.multiple_of(n * tile, tile), tile)
            a = normed[slot_a, half_a * half_rows : (half_a + 1) * half_rows]
            b = normed[slot_b, half_b * half_rows : (half_b + 1) * half_rows]
            h = dot(jnp.concatenate([a, b], axis=0), up[:, :, :, :, at].reshape(width, tile))
            h = jnp.maximum(h, 0.0)
            hidden[batch, :, at] = (h * h).astype(BF16)
            return 0

        lax.fori_loop(0, tiles, one, 0)

    span = width // nz
    blocks_of = (by_distance[:early], by_distance[early:])
    lanes_of = (pl.ds(0, early * span), pl.ds(early * span, width - early * span))

    first, second = slice(0, half_rows), slice(half_rows, rows)

    def fall(batch, half, put):
        for n, k in enumerate(blocks_of[half]):
            at = (half * early + n) * span
            put(slice(at, at + span), dot_t(hidden[batch], down[at_z(k)].reshape(span, width)))

    def put_far(at, piece):
        send2[:, at] = piece.astype(BF16)

    def put_early(at, piece):
        sendm[first, at] = piece[first].astype(BF16)
        send1[second, at] = piece[second].astype(BF16)

    def put_late(at, piece):
        hold[0, :, at] = piece[first]
        hold[1, :, at] = piece[second]

    def put_own(at, piece):
        own[:, at] = piece

    got_l, got_r = got_both.at[0], got_both.at[1]
    row_halves = (pl.ds(0, half_rows), pl.ds(half_rows, half_rows))

    def far(half, side):
        to = (relay_l, relay_r)[side].at[:, lanes_of[half]]
        return remote(send2.at[row_halves[side], lanes_of[half]], to, left_s.at[9], rs_r.at[2 * half + side], x_to[side])

    def near(half, side, summed):
        at = (row_halves[side if summed else 1 - side], lanes_of[half])
        source, to = ((send1, got_l), (sendm, got_r))[side]
        return remote(source.at[at], to.at[at], left_s.at[9], rs_r.at[4 + half], x_to[side])

    def add_far(half):
        at = lanes_of[half]
        far(half, 0).wait_recv()
        send1[first, at] = (hold[0, :, at] + relay_l[:, at].astype(F32)).astype(BF16)
        go(near(half, 0, 1))
        far(half, 1).wait_recv()
        sendm[second, at] = (hold[1, :, at] + relay_r[:, at].astype(F32)).astype(BF16)
        go(near(half, 1, 1))

    rise(EARLY)
    d_step(3, 2)
    wait_all(down.at[pl.ds(0, early), :, 0], core_r.at[2])
    fall(EARLY, 0, put_early)
    for side in (0, 1):
        go(near(0, side, 0))
    for side in (0, 1):
        nm_in(2, side).wait_recv()
        nm_in(3, side).wait_recv()
    d_step(3, 3)
    d_cores(3)
    rise(FAR)
    fall(FAR, 0, put_far)
    for side in (0, 1):
        go(far(0, side))
    d_step(4, 0, 1, 2, 3)
    d_cores(4)
    for side in (0, 1):
        nm_in(4, side).wait_recv()
    rise(LATE)
    fall(LATE, 0, put_late)
    wait_all(down.at[pl.ds(0, nz - early), :, 0], core_r.at[3])
    fall(EARLY, 1, put_early)
    for side in (0, 1):
        go(near(1, side, 0))
    fall(FAR, 1, put_far)
    for side in (0, 1):
        go(far(1, side))
    fall(LATE, 1, put_late)
    add_far(0)
    rise(OWN)
    fall(OWN, 0, put_own)
    add_far(1)
    fall(OWN, 1, put_own)
    for half in (0, 1):
        at = lanes_of[half]
        wait_all(got_both.at[:, :, at], rs_r.at[4 + half])
        total = own[:, at] + got_l[:, at].astype(F32) + got_r[:, at].astype(F32)
        for n, k in enumerate(blocks_of[half]):
            at = pl.ds(pl.multiple_of(at_z(k) * span, span), span)
            result[:, at] = (middle[:, at].astype(F32) + total[:, n * span : (n + 1) * span]).astype(BF16)
            go(pltpu.make_async_copy(result.at[:, at], out.at[:, at], out_s))

    totals = (
        up.at[pl.ds(0, nz - 1), 0, 0], up.at[:, pl.ds(0, 2), 0], up.at[:, 0, 0], down.at[pl.ds(0, 3), 0, 0],
        down.at[pl.ds(0, nz - 1), :, 0], wo.at[pl.ds(0, 3)], up, mixed.at[pl.ds(0, nx - 1)], normed.at[pl.ds(0, 3)],
        normed.at[pl.ds(0, 3)], msg.at[pl.ds(0, plane - 1)], in2.at[pl.ds(0, nz - 1)], msg.at[pl.ds(0, plane - 1)],
    )
    for i, total in enumerate(totals):
        wait_all(total, left_s.at[i])
    wait_all(out, out_s)


def on_device(
    sizes,
    stream_in, query_wide, key_wide, value_wide, gate_wide, decay_wide,
    query_narrow, key_narrow, value_narrow, gate_narrow, decay_narrow,
    output_wide, output_narrow, norm_gain, up_weight, down_weight,
):
    nz, ny, nc, nx = sizes
    tok = query_wide.shape[0]
    rows, width = stream_in.shape
    plane = ny * nc
    part, hid = up_weight.shape
    ns = (128 + HDN) // plane
    dma = pltpu.SemaphoreType.DMA
    vm = pltpu.VMEM
    scratch = [
        *[vm((tok, 128), BF16)] * 8, vm((rows, width), BF16),
        vm((nz, ny, nc, part, hid), BF16), vm((nz, ny, nc, part, hid), BF16), vm((nx, 2, *output_wide.shape), BF16),
        vm((tok, 128), BF16), vm((tok, 128), BF16), vm((tok, 128), F32), vm((tok, 128), F32),
        vm((128, 128), F32),
        vm((tok // BLOCK, 128, 128), BF16), vm((tok // BLOCK, 128, 128), BF16), vm((tok, 128), BF16), vm((tok, 128), BF16),
        vm((plane, ns + 8, 128), BF16), vm((plane, ns + 8, 128), BF16),
        vm((ns + 8, 128), BF16), vm((nz, ns + 8, 128), BF16),
        vm((plane, ns + 8, 128), BF16), vm((plane, ns + 8, 128), BF16),
        vm((nx, rows, 256), BF16), vm((nx, rows, 256), BF16),
        vm((rows, width), BF16), vm((nx, rows, width), BF16), vm((nx, rows, hid), BF16),
        vm((rows, width), BF16), vm((rows, width), BF16), vm((rows, width), BF16),
        vm((rows, width), F32), vm((2, rows // 2, width), F32), vm((rows, width), BF16),
        vm((rows // 2, width), BF16), vm((rows // 2, width), BF16), vm((2, rows, width), BF16),
        dma((13,)), dma((13,)), dma, dma((2, 5)), dma, dma, dma, dma, dma((6,)), dma((2, 3)), dma((2, 4)), dma((2, 5)),
        dma((2,)), dma((2, 2)), dma((2, 4, 4)), dma((4,)),
    ]
    vmem = pl.BlockSpec(memory_space=pltpu.VMEM)
    hbm = pl.BlockSpec(memory_space=pl.ANY)
    return pl.pallas_call(
        functools.partial(kernel, sizes),
        out_shape=jax.ShapeDtypeStruct((rows, width), BF16),
        in_specs=[vmem] * 6 + [hbm] * 13,
        out_specs=hbm,
        scratch_shapes=scratch,
        compiler_params=pltpu.CompilerParams(
            collective_id=0, has_side_effects=True, vmem_limit_bytes=60 * 1024 * 1024
        ),
    )(
        decay_wide, decay_narrow, norm_gain, jnp.asarray(rope_tables(BLOCK, 1)),
        jnp.asarray(rope_tables(8, BLOCK)), jnp.asarray(rope_tables(nz * plane, tok)),
        query_wide, key_wide, value_wide, query_narrow, key_narrow, value_narrow, gate_wide, gate_narrow, stream_in,
        output_wide, output_narrow, up_weight, down_weight.T,
    )


def solution(mesh):
    sizes = (8, 4, 2, mesh.shape["tp"])
    split = Mesh(mesh.devices.reshape(sizes), ("z", "y", "c", "x"))
    sp = ("z", "y", "c")
    rows, heads = P(sp, "x"), P("x", sp)
    in_specs = (
        P((*sp, "x"), None), rows, rows, rows, rows, heads, rows, rows, rows, rows, heads,
        P("x", None), P("x", None), P(), rows, heads,
    )
    return jax.shard_map(
        functools.partial(on_device, sizes), mesh=split, in_specs=in_specs,
        out_specs=P((*sp, "x"), None), check_vma=False,
    )
```
